32 devices in a mesh: sp: 16 (over z, y, x), tp: 2 (over core).
Axes of the slice: x: 2, y: 2, z: 4, core: 2. Of those that a mesh axis runs over, the one named last changes fastest.
Arguments:
- residual: bfloat16 [3072, 1024], P('sp', 'tp'), may hold values from -6 to 6
- query_first: bfloat16 [3072, 1024], P('sp', 'tp'), may hold values from -64 to 64
- key_first: bfloat16 [3072, 256], P('sp', 'tp'), may hold values from -20 to 20
- value_first: bfloat16 [3072, 256], P('sp', 'tp'), may hold values from -6 to 6
- documents: int32 [3072], P('sp'), may hold values from 0 to 2, as said below
- bias_first: float32 [16, 513], P('tp'), may hold values from -4 to 4
- out_first: bfloat16 [1024, 1024], P('tp'), may hold values from -0.75 to 0.75
- norm_gain: float32 [1024], replicated, may hold values from 0.1 to 1.9
- query_w: bfloat16 [1024, 1024], P(None, 'tp'), may hold values from -0.1875 to 0.1875
- key_w: bfloat16 [1024, 256], P(None, 'tp'), may hold values from -0.1875 to 0.1875
- value_w: bfloat16 [1024, 256], P(None, 'tp'), may hold values from -0.1875 to 0.1875
- bias_second: float32 [16, 513], P('tp'), may hold values from -4 to 4
- out_second: bfloat16 [1024, 1024], P('tp'), may hold values from -0.75 to 0.75
Outputs:
- layer_two: bfloat16 [3072, 1024], P('sp', 'tp')
The draws below stay inside these ranges and needn't reach their ends.
Inputs may be any that keep to these rules, and one draw needn't show every extreme that they name: Document numbers start at 0, never fall, and rise by one at the first position of each document; there are exactly 3 documents, each of at least 896 positions.
All inputs are finite; a program needn't handle non-finite values.
Results may differ from the reference program's by a relative error of at most 0.017.
Values may be sent and summed in bfloat16 or wider, within the bound.
A program may use at most 64 MiB of HBM per device.

```python
import jax
import jax.numpy as jnp
from jax import lax

D = 1024
HEADS = 16
KV_HEADS = 4
HEAD_SIZE = 64
SEG = 64
PAST = 4
REL_CLIP = 256
TOKENS = 3072
DOC_MIN = 896
N_TP = 2


def paired_draw(key):
    base = jax.random.fold_in(key, 11)
    key_noise, query_noise = jax.random.split(base, 2)
    keys_raw = jnp.clip(jax.random.normal(key_noise, (TOKENS, KV_HEADS, HEAD_SIZE), jnp.float32), -4.0, 4.0)
    queries_raw = jnp.clip(jax.random.normal(query_noise, (TOKENS, KV_HEADS, HEADS // KV_HEADS, HEAD_SIZE), jnp.float32), -4.0, 4.0)
    keys_new = keys_raw
    queries_new = queries_raw
    return (queries_new.reshape(TOKENS, HEADS * HEAD_SIZE), keys_new.reshape(TOKENS, KV_HEADS * HEAD_SIZE))


def draw_query_first(key, part):
    return paired_draw(key)[0].astype(jnp.bfloat16)


def draw_key_first(key, part):
    return paired_draw(key)[1].astype(jnp.bfloat16)


def draw_documents(key, part):
    doc_count = TOKENS // DOC_MIN
    spare_rows = TOKENS - doc_count * DOC_MIN
    base = jax.random.fold_in(key, 23)
    cut_points = jnp.sort(jax.random.randint(base, (doc_count,), 0, spare_rows + 1))
    starts = jnp.arange(doc_count) * DOC_MIN + cut_points
    positions = jnp.arange(TOKENS)
    counted = (starts[None, 1:] <= positions[:, None]).astype(jnp.int32)
    return jnp.sum(counted, axis=1).astype(jnp.int32)


def levels(own_key, dims, shards, least, high):
    def one(dim, parts):
        draws = jax.random.uniform(jax.random.fold_in(jax.random.fold_in(own_key, 6), dim), (parts,), jnp.float32, least / len(shards), high / len(shards))
        return jnp.repeat(jnp.exp(draws), dims[dim] // parts).reshape((-1,) + (1,) * (len(dims) - dim - 1))

    loudness = one(*shards[0])
    for cut in shards[1:]:
        loudness = loudness * one(*cut)
    return loudness


def normal_values(own_key, shape, scale, most, shards=(), kind=jnp.bfloat16):
    drawn = scale * jax.random.normal(own_key, shape, jnp.float32)
    if shards:
        drawn = drawn * levels(own_key, shape, shards, -0.22, 0.18)
    return jnp.clip(drawn, -most, most).astype(kind)


def setup_inputs(seed: int = 0) -> dict:
    streams_of = jax.random.split(jax.random.key(seed), 14)
    residual = normal_values(streams_of[0], (TOKENS, D), 1.0, 6.0, ((0, 16), (1, 2)))
    query_first = draw_query_first(jax.random.fold_in(streams_of[13], 71), 0)
    key_first = draw_key_first(jax.random.fold_in(streams_of[13], 71), 0)
    value_first = normal_values(streams_of[3], (TOKENS, KV_HEADS * HEAD_SIZE), 1.0, 6.0, ((0, 16), (1, 2)))
    documents = draw_documents(jax.random.fold_in(streams_of[13], 71), 0)
    bias_first = normal_values(streams_of[5], (HEADS, 2 * REL_CLIP + 1), 1.0, 4.0, ((0, 2),), jnp.float32)
    out_first = normal_values(streams_of[6], (HEADS * HEAD_SIZE, D), (HEADS * HEAD_SIZE // 16) ** -0.5, 0.75, ((0, 2),))
    norm_gain = jnp.clip(1.0 + 0.18 * jax.random.normal(streams_of[7], (D,), jnp.float32), 0.1, 1.9)
    query_w = normal_values(streams_of[8], (D, HEADS * HEAD_SIZE), D ** -0.5, 0.1875, ((1, 2),))
    key_w = normal_values(streams_of[9], (D, KV_HEADS * HEAD_SIZE), D ** -0.5, 0.1875, ((1, 2),))
    value_w = normal_values(streams_of[10], (D, KV_HEADS * HEAD_SIZE), D ** -0.5, 0.1875, ((1, 2),))
    bias_second = normal_values(streams_of[11], (HEADS, 2 * REL_CLIP + 1), 1.0, 4.0, ((0, 2),), jnp.float32)
    out_second = normal_values(streams_of[12], (HEADS * HEAD_SIZE, D), (HEADS * HEAD_SIZE // 16) ** -0.5, 0.75, ((0, 2),))
    return dict(residual=residual, query_first=query_first, key_first=key_first, value_first=value_first, documents=documents, bias_first=bias_first, out_first=out_first, norm_gain=norm_gain, query_w=query_w, key_w=key_w, value_w=value_w, bias_second=bias_second, out_second=out_second)


eps = 1e-06

def segment_attention(queries, keys, values, documents, bias_table):
    total_rows = queries.shape[0]
    span_rows = PAST * SEG
    band_rows = span_rows + SEG
    group_size = HEADS // KV_HEADS
    keys_pad = jnp.concatenate([jnp.zeros((span_rows, keys.shape[1]), keys.dtype), keys], axis=0)
    values_pad = jnp.concatenate([jnp.zeros((span_rows, values.shape[1]), values.dtype), values], axis=0)
    docs_pad = jnp.concatenate([jnp.full((span_rows,), -1, jnp.int32), documents.astype(jnp.int32)], axis=0)
    query_pos = jnp.arange(SEG, dtype=jnp.int32)[:, None]
    key_pos = jnp.arange(band_rows, dtype=jnp.int32)[None, :]
    relative = jnp.clip(query_pos + span_rows - key_pos, -REL_CLIP, REL_CLIP) + REL_CLIP
    position_bias_grid = jnp.take(bias_table.astype(jnp.float32), relative, axis=1).reshape(KV_HEADS, group_size, SEG, band_rows)
    seg_count = total_rows // SEG

    def one_segment(segment):
        first_row = (segment * SEG).astype(jnp.int32)
        query_tile_rows = lax.dynamic_slice_in_dim(queries, first_row, SEG, 0).astype(jnp.float32).reshape(SEG, KV_HEADS, group_size, HEAD_SIZE)
        key_tile_rows = lax.dynamic_slice_in_dim(keys_pad, first_row, band_rows, 0).astype(jnp.float32).reshape(band_rows, KV_HEADS, HEAD_SIZE)
        value_tile_rows = lax.dynamic_slice_in_dim(values_pad, first_row, band_rows, 0).astype(jnp.float32).reshape(band_rows, KV_HEADS, HEAD_SIZE)
        band_docs = lax.dynamic_slice_in_dim(docs_pad, first_row, band_rows, 0)
        own_docs = lax.dynamic_slice_in_dim(documents.astype(jnp.int32), first_row, SEG, 0)
        logit_scores = jnp.einsum('yixw,ziw->ixyz', query_tile_rows, key_tile_rows) * HEAD_SIZE ** (-0.5) + position_bias_grid
        allowed = band_docs[None, :] == own_docs[:, None]
        logit_scores = jnp.where(allowed[None, None], logit_scores, -jnp.inf)
        largest = lax.optimization_barrier(jnp.max(logit_scores, axis=-1, keepdims=True))
        softmax_weight = jnp.exp(logit_scores - largest)
        softmax_weight = (softmax_weight / lax.optimization_barrier(jnp.sum(softmax_weight, axis=-1, keepdims=True))).astype(jnp.bfloat16)
        blended_output = jnp.einsum('rsvh,hru->vrsu', softmax_weight.astype(jnp.float32), value_tile_rows)
        return blended_output.astype(jnp.bfloat16).reshape(SEG, HEADS * HEAD_SIZE)
    blocks = lax.map(one_segment, jnp.arange(seg_count, dtype=jnp.int32))
    return blocks.reshape(total_rows, HEADS * HEAD_SIZE)

def project_out(mixed, weight):
    share_width = mixed.shape[1] // N_TP
    total_sum = jnp.zeros((mixed.shape[0], weight.shape[1]), jnp.float32)
    for group_index in range(N_TP):
        lower = group_index * share_width
        part_sum = jnp.dot(mixed[:, lower:lower + share_width], weight[lower:lower + share_width], preferred_element_type=jnp.float32)
        rounded = lax.optimization_barrier(part_sum.astype(jnp.bfloat16))
        total_sum = total_sum + rounded.astype(jnp.float32)
    return total_sum

def reference(residual, query_first, key_first, value_first, documents, bias_first, out_first, norm_gain, query_w, key_w, value_w, bias_second, out_second):
    mixed_one = segment_attention(query_first, key_first, value_first, documents, bias_first)
    layer_one = (residual.astype(jnp.float32) + project_out(mixed_one, out_first)).astype(jnp.bfloat16)
    rows_wide = layer_one.astype(jnp.float32)
    scale = lax.rsqrt(lax.optimization_barrier(jnp.mean(rows_wide * rows_wide, axis=1, keepdims=True)) + eps)
    normed = (rows_wide * scale * norm_gain.astype(jnp.float32)).astype(jnp.bfloat16)
    query_two = jnp.dot(normed, query_w, preferred_element_type=jnp.float32).astype(jnp.bfloat16)
    key_two = jnp.dot(normed, key_w, preferred_element_type=jnp.float32).astype(jnp.bfloat16)
    value_two = jnp.dot(normed, value_w, preferred_element_type=jnp.float32).astype(jnp.bfloat16)
    mixed_two = segment_attention(query_two, key_two, value_two, documents, bias_second)
    return (layer_one.astype(jnp.float32) + project_out(mixed_two, out_second)).astype(jnp.bfloat16)
```

```python
import functools

import jax
import jax.numpy as jnp
from jax import lax
from jax.experimental import pallas as pl
from jax.experimental.pallas import tpu as pltpu
from jax.sharding import PartitionSpec as P

HEAD_SIZE = 64
SEG = 64
PAST = 4
REL_CLIP = 256
SPAN = PAST * SEG
BAND = SPAN + SEG
LANES = 128
LOG2E = 1.4426950408889634
HIDDEN = -1e30
MESH = pl.DeviceIdType.MESH


eps = 1e-06


def hops_of(tok_rows):
    return range(1, (SPAN + tok_rows - 1) // tok_rows + 1)


def pieces_of(tok_rows):
    pieces = []
    for distance in hops_of(tok_rows):
        top = SPAN - (distance - 1) * tok_rows
        bottom = max(0, top - tok_rows)
        cuts = [cut for cut in range(SEG, tok_rows, SEG) if bottom < cut < top]
        edges = [bottom] + cuts + [top]
        for low, high in reversed(list(zip(edges[:-1], edges[1:]))):
            pieces.append((distance, tok_rows - (top - low), high - low, low))
    return pieces


def build_bias(table_ref, bias_ref):
    heads_local = table_ref.shape[0]
    group_size = bias_ref.shape[2] // SEG
    lane = lax.broadcasted_iota(jnp.int32, (SEG, LANES), 1)
    low = lane < SEG
    last = REL_CLIP + SPAN

    def tile(head, index):
        if index == 0:
            return jnp.broadcast_to(table_ref[head : head + 1, last : last + 1], (SEG, LANES))
        first = last - index * LANES
        return jnp.broadcast_to(table_ref[head : head + 1, first : first + LANES], (SEG, LANES))

    def piece(head, block, base):
        back = block // 2
        if block % 2 == 0:
            source = jnp.where(low, tile(head, back), tile(head, back + 1))
            shift = base
        else:
            source = tile(head, back + 1)
            shift = (base + SEG) % LANES
        return pltpu.roll(source, shift, 1, stride=1, stride_axis=0)

    for head in range(0, heads_local, 2):
        for block in range(PAST + 1):
            pair = jnp.where(low, piece(head, block, 0), piece(head + 1, block, SEG)) * LOG2E
            group, inner = head // group_size, head % group_size
            bias_ref[group, block * SEG : (block + 1) * SEG, inner * SEG : (inner + 2) * SEG] = pair


class Attention:
    def __init__(self, query, kv, bias, mask, mixed, padded, turned, scores, weights, stats, blend):
        self.query, self.kv, self.bias, self.mask, self.mixed = query, kv, bias, mask, mixed
        self.padded, self.turned, self.scores, self.weights = padded, turned, scores, weights
        self.stats, self.blend = stats, blend
        self.groups = bias.shape[0]
        self.group_size = bias.shape[2] // SEG
        self.kv_width = self.groups * HEAD_SIZE
        self.state = {}

    def unit(self, segment, group):
        return segment * self.groups + group

    def pad_queries(self, segment):
        lane = lax.broadcasted_iota(jnp.int32, (SEG, LANES), 1)
        rows = slice(segment * SEG, (segment + 1) * SEG)
        for group in range(self.groups):
            keep = (lane >= group * HEAD_SIZE) & (lane < (group + 1) * HEAD_SIZE)
            for inner in range(self.group_size):
                head = group * self.group_size + inner
                column = head * HEAD_SIZE // LANES * LANES
                block = self.query[rows, column : column + LANES]
                if head % 2 != group % 2:
                    block = jnp.concatenate([block[:, HEAD_SIZE:], block[:, :HEAD_SIZE]], axis=1)
                self.padded[self.unit(segment, group), inner * SEG : (inner + 1) * SEG] = jnp.where(
                    keep, block, jnp.zeros_like(block)
                )

    def turn_values(self, row):
        block = jnp.transpose(self.kv[row : row + SEG, self.kv_width : 2 * self.kv_width])
        self.turned[0, :, row : row + SEG] = block
        if row >= SEG:
            self.turned[1, :, row - SEG : row] = block

    def bounds(self, segment, local):
        first = segment * SEG
        return (max(first, SPAN), first + BAND) if local else (first, SPAN)

    def score(self, segment, group, local):
        low, high = self.bounds(segment, local)
        unit = self.unit(segment, group)
        band = slice(low - segment * SEG, high - segment * SEG)
        scores = lax.dot_general(
            self.kv[low:high, : self.kv_width],
            self.padded[unit],
            (((1,), (1,)), ((), ())),
            preferred_element_type=jnp.float32,
        )
        mask = self.mask[segment, band]
        mask = jnp.concatenate([mask] * (self.group_size * SEG // LANES), axis=1)
        scores = scores * (HEAD_SIZE ** (-0.5) * LOG2E) + self.bias[group, band] + mask
        self.scores[unit, band] = scores
        largest = jnp.max(scores, axis=0, keepdims=True)
        if local:
            self.stats[unit, 0:1] = largest
        else:
            largest = jnp.maximum(largest, self.stats[unit, 0:1])
        self.state[unit] = (largest,)

    def weigh(self, segment, group, local):
        low, high = self.bounds(segment, local)
        unit = self.unit(segment, group)
        band = slice(low - segment * SEG, high - segment * SEG)
        (largest,) = self.state[unit]
        weight = jnp.exp2(self.scores[unit, band] - largest)
        self.weights[unit, band] = weight.astype(jnp.bfloat16)
        total = jnp.sum(weight, axis=0, keepdims=True)
        if local:
            self.stats[unit, 1:2] = total
        else:
            fade = jnp.exp2(self.stats[unit, 0:1] - largest)
            inverse = 1.0 / (total + self.stats[unit, 1:2] * fade)
            self.state[unit] = (fade, inverse)

    def gather(self, segment, group, local):
        low, high = self.bounds(segment, local)
        unit = self.unit(segment, group)
        band = slice(low - segment * SEG, high - segment * SEG)
        odd = low // SEG % 2
        blended = lax.dot_general(
            self.turned[
                odd,
                group * HEAD_SIZE : (group + 1) * HEAD_SIZE,
                low - odd * SEG : high - odd * SEG,
            ],
            self.weights[unit, band],
            (((1,), (0,)), ((), ())),
            preferred_element_type=jnp.float32,
        )
        if local:
            self.blend[unit] = blended
            return
        fade, inverse = self.state[unit]
        blended = (blended + self.blend[unit] * fade) * inverse
        rows = slice(segment * SEG, (segment + 1) * SEG)
        for pair in range(self.group_size // 2):
            turned = jnp.transpose(blended[:, pair * LANES : (pair + 1) * LANES])
            both = jnp.concatenate([turned[:SEG], turned[SEG:]], axis=1)
            column = (group * self.group_size + 2 * pair) * HEAD_SIZE
            self.mixed[rows, column : column + LANES] = both.astype(jnp.bfloat16)

    def run(self, segments, local):
        units = [(segment, group) for segment in segments for group in range(self.groups)]
        self.score(*units[0], local)
        for index in range(len(units)):
            if index + 1 < len(units):
                self.score(*units[index + 1], local)
            if index > 0:
                self.gather(*units[index - 1], local)
            self.weigh(*units[index], local)
        self.gather(*units[-1], local)


def kernel(
    n_sp,
    residual_hbm,
    query_hbm,
    key_hbm,
    value_hbm,
    docs_hbm,
    bias_one_hbm,
    out_one_hbm,
    gain_hbm,
    query_w_hbm,
    key_w_hbm,
    value_w_hbm,
    bias_two_hbm,
    out_two_hbm,
    result_ref,
    w_out_one,
    w_query,
    w_kv,
    w_out_two,
    bias_one,
    bias_two,
    gain,
    docs,
    kv_one,
    kv_two,
    docs_prior,
    docs_col,
    mask,
    table_one,
    table_two,
    mixed,
    query_one,
    query_two,
    residual_full,
    part_own,
    part_in,
    last_in,
    layer,
    normed,
    padded,
    turned,
    scores,
    weights,
    stats,
    blend,
    send_sem,
    recv_sem,
    load_sem,
):
    me = lax.axis_index("sp")
    my_tp = lax.axis_index("tp")
    other = 1 - my_tp
    tok_rows, width_local = residual_hbm.shape
    kv_width = key_hbm.shape[1]
    segments = tok_rows // SEG
    hops = hops_of(tok_rows)
    pieces = pieces_of(tok_rows)
    halves = part_own.shape[0]
    blocks = [(range(segments - 1, 0, -1), SEG, tok_rows - SEG), (range(1), 0, SEG)]

    barrier = pltpu.get_barrier_semaphore()
    expected = jnp.int32(1)
    for distance in hops:
        expected = expected + (me + distance < n_sp).astype(jnp.int32)

        @pl.when(me >= distance)
        def _():
            pl.semaphore_signal(
                barrier, inc=1, device_id={"sp": me - distance}, device_id_type=MESH
            )

    pl.semaphore_signal(barrier, inc=1, device_id={"tp": other}, device_id_type=MESH)

    own = pl.ds(SPAN, tok_rows)
    transfers = dict(
        bias_one=(bias_one_hbm, bias_one),
        key=(key_hbm, kv_one.at[own, pl.ds(0, kv_width)]),
        value=(value_hbm, kv_one.at[own, pl.ds(kv_width, kv_width)]),
        docs=(docs_hbm, docs),
        query=(query_hbm, query_one),
        residual=(residual_hbm, residual_full.at[my_tp]),
        bias_two=(bias_two_hbm, bias_two),
        out_one=(out_one_hbm, w_out_one),
        gain=(gain_hbm, gain),
        key_w=(key_w_hbm, w_kv.at[:, pl.ds(0, kv_width)]),
        value_w=(value_w_hbm, w_kv.at[:, pl.ds(kv_width, kv_width)]),
        query_w=(query_w_hbm, w_query),
        out_two=(out_two_hbm, w_out_two),
    )
    loads = {
        name: pltpu.make_async_copy(src, dst, load_sem.at[index])
        for index, (name, (src, dst)) in enumerate(transfers.items())
    }
    for load in loads.values():
        load.start()

    slot = iter(range(send_sem.shape[0]))

    def remote(src, dst, target):
        index = next(slot)
        return pltpu.make_async_remote_copy(
            src_ref=src,
            dst_ref=dst,
            send_sem=send_sem.at[index],
            recv_sem=recv_sem.at[index],
            device_id=target,
            device_id_type=MESH,
        )

    def ahead(distance):
        return {"sp": lax.rem(me + distance, n_sp)}

    def start_sent(distance, copies):
        @pl.when(me + distance < n_sp)
        def _():
            for copy in copies:
                copy.start()

    def wait_arrived(distance, copies):
        @pl.when(me >= distance)
        def _():
            for copy in copies:
                copy.wait_recv()

    def wait_sent(distance, copies):
        @pl.when(me + distance < n_sp)
        def _():
            for copy in copies:
                copy.wait_send()

    for distance, _, needed, landing in pieces:

        @pl.when(me < distance)
        def _():
            empty = jnp.zeros((needed, 2 * kv_width), jnp.bfloat16)
            kv_one[landing : landing + needed] = empty
            kv_two[landing : landing + needed] = empty

    for distance in hops:

        @pl.when(me < distance)
        def _():
            docs_prior[distance - 1] = jnp.full((1, tok_rows), -1, jnp.int32)

    loads["bias_one"].wait()
    build_bias(bias_one, table_one)
    for name in ("key", "value", "docs"):
        loads[name].wait()

    pl.semaphore_wait(barrier, expected)

    def halo_copy(kv, piece):
        distance, row, needed, landing = piece
        return remote(
            kv.at[pl.ds(SPAN + row, needed)], kv.at[pl.ds(landing, needed)], ahead(distance)
        )

    docs_copies = [
        (distance, [remote(docs, docs_prior.at[distance - 1], ahead(distance))])
        for distance in hops
    ]
    first_copies = [(piece[0], [halo_copy(kv_one, piece)]) for piece in pieces]
    for distance, copies in docs_copies + first_copies:
        start_sent(distance, copies)
    loads["residual"].wait()
    residual_copy = remote(
        residual_full.at[my_tp], residual_full.at[my_tp], {"tp": other}
    )
    residual_copy.start()

    eye = lax.broadcasted_iota(jnp.int32, (SEG, SEG), 0) == lax.broadcasted_iota(
        jnp.int32, (SEG, SEG), 1
    )

    def put_column(numbers, place):
        picked = jnp.where(eye, numbers.astype(jnp.float32), 0.0)
        docs_col[place : place + SEG] = jnp.broadcast_to(
            jnp.sum(picked, axis=1, keepdims=True), (SEG, LANES)
        )

    def put_mask(segment, low, high):
        mine = docs[:, segment * SEG : (segment + 1) * SEG].astype(jnp.float32)
        mine = jnp.concatenate([mine, mine], axis=1)
        same = docs_col[low:high] == mine
        first = segment * SEG
        mask[segment, low - first : high - first] = jnp.where(same, 0.0, HIDDEN)

    shared = (mask, mixed, padded, turned, scores, weights, stats, blend)
    one = Attention(query_one, kv_one, table_one, *shared)
    two = Attention(query_two, kv_two, table_two, *shared)
    newest_first = range(segments - 1, -1, -1)

    for block in range(0, tok_rows, SEG):
        put_column(docs[:, block : block + SEG], SPAN + block)
    for segment in range(segments):
        put_mask(segment, *one.bounds(segment, True))

    loads["query"].wait()
    for row in range(SPAN, SPAN + tok_rows, SEG):
        one.turn_values(row)
    for segment in newest_first:
        one.pad_queries(segment)
    one.run(newest_first, True)

    loads["bias_two"].wait()
    build_bias(bias_two, table_two)

    for distance, copies in docs_copies:
        wait_arrived(distance, copies)
    for distance, row, needed, landing in pieces:
        for block in range(0, needed, SEG):
            put_column(
                docs_prior[distance - 1, :, row + block : row + block + SEG], landing + block
            )
    for segment in range(segments):
        put_mask(segment, *one.bounds(segment, False))

    def halo_block(layer_attention, members, waiting, done):
        for piece, (distance, copies) in zip(pieces, waiting):
            _, _, needed, landing = piece
            if landing + needed > min(members) * SEG and landing not in done:
                done.add(landing)
                wait_arrived(distance, copies)
                for row in range(landing, landing + needed, SEG):
                    layer_attention.turn_values(row)
        layer_attention.run(members, False)

    part_copies = []
    done = set()
    for members, start, count in blocks:
        halo_block(one, members, first_copies, done)
        if start > 0:
            loads["out_one"].wait()
        rows = pl.ds(start, count)
        copies = []
        for half in range(halves):
            part_own[half, start : start + count] = jnp.dot(
                mixed[start : start + count],
                w_out_one[:, half * width_local : (half + 1) * width_local],
                preferred_element_type=jnp.float32,
            ).astype(jnp.bfloat16)
            copy = remote(part_own.at[half, rows], part_in.at[half, rows], {"tp": other})
            copy.start()
            copies.append(copy)
        part_copies.append(copies)

    residual_copy.wait_recv()
    second_copies = [None] * len(pieces)
    for (_, start, count), copies in zip(blocks, part_copies):
        rows = slice(start, start + count)
        squares = jnp.zeros((count, 1), jnp.float32)
        for half in range(halves):
            copies[half].wait_recv()
            new = residual_full[half, rows].astype(jnp.float32) + (
                part_own[half, rows].astype(jnp.float32) + part_in[half, rows].astype(jnp.float32)
            )
            new = new.astype(jnp.bfloat16)
            layer[half, rows] = new
            new = new.astype(jnp.float32)
            squares = squares + jnp.sum(new * new, axis=1, keepdims=True)
        if start > 0:
            loads["gain"].wait()
        scale = lax.rsqrt(squares / (halves * width_local) + eps)
        for half in range(halves):
            columns = slice(half * width_local, (half + 1) * width_local)
            normed[rows, columns] = (
                layer[half, rows].astype(jnp.float32) * scale * gain[:, columns]
            ).astype(jnp.bfloat16)
        if start > 0:
            loads["key_w"].wait()
            loads["value_w"].wait()
        kv_two[SPAN + start : SPAN + start + count] = jnp.dot(
            normed[rows], w_kv[...], preferred_element_type=jnp.float32
        ).astype(jnp.bfloat16)
        for index, piece in enumerate(pieces):
            if start <= piece[1] < start + count:
                second_copies[index] = (piece[0], [halo_copy(kv_two, piece)])
                start_sent(*second_copies[index])
    loads["query_w"].wait()
    query_two[...] = jnp.dot(normed[...], w_query[...], preferred_element_type=jnp.float32).astype(
        jnp.bfloat16
    )
    for row in range(SPAN, SPAN + tok_rows, SEG):
        two.turn_values(row)
    for segment in newest_first:
        two.pad_queries(segment)
    two.run(newest_first, True)
    for copies in part_copies:
        for copy in copies:
            copy.wait_send()

    loads["out_two"].wait()
    theirs = pl.ds(pl.multiple_of(other * width_local, width_local), width_local)
    ours = pl.ds(pl.multiple_of(my_tp * width_local, width_local), width_local)
    last_copies = []
    done = set()
    for members, start, count in blocks:
        halo_block(two, members, second_copies, done)
        rows = pl.ds(start, count)
        part_own[0, start : start + count] = jnp.dot(
            mixed[start : start + count], w_out_two[:, theirs], preferred_element_type=jnp.float32
        ).astype(jnp.bfloat16)
        copy = remote(part_own.at[0, rows], last_in.at[rows], {"tp": other})
        copy.start()
        last_copies.append(copy)
    part_own[1] = jnp.dot(
        mixed[...], w_out_two[:, ours], preferred_element_type=jnp.float32
    ).astype(jnp.bfloat16)
    for (_, start, count), copy in zip(blocks, last_copies):
        rows = slice(start, start + count)
        copy.wait_recv()
        branch = part_own[1, rows].astype(jnp.float32) + last_in[rows].astype(jnp.float32)
        result_ref[rows] = (layer[my_tp, rows].astype(jnp.float32) + branch).astype(jnp.bfloat16)

    residual_copy.wait_send()
    for distance, copies in docs_copies + first_copies + second_copies:
        wait_sent(distance, copies)
    for copy in last_copies:
        copy.wait_send()


def body(
    residual,
    query_first,
    key_first,
    value_first,
    documents,
    bias_first,
    out_first,
    norm_gain,
    query_w,
    key_w,
    value_w,
    bias_second,
    out_second,
):
    n_sp = lax.axis_size("sp")
    tok_rows, width_local = residual.shape
    query_width = query_first.shape[1]
    kv_width = key_first.shape[1]
    kv_local = kv_width // HEAD_SIZE
    group_width = query_width // kv_local
    halves = out_first.shape[1] // width_local
    hops = len(hops_of(tok_rows))
    units = tok_rows // SEG * kv_local
    n_sems = hops + 2 * len(pieces_of(tok_rows)) + 1 + 2 * halves + 2
    vmem = pl.BlockSpec(memory_space=pltpu.VMEM)
    hbm = pl.BlockSpec(memory_space=pl.ANY)
    bf16 = jnp.bfloat16
    f32 = jnp.float32
    return pl.pallas_call(
        functools.partial(kernel, n_sp),
        name="two_layers",
        out_shape=pltpu.VMEM((tok_rows, width_local), bf16),
        in_specs=[hbm] * 13,
        out_specs=vmem,
        scratch_shapes=[
            pltpu.VMEM(out_first.shape, bf16),
            pltpu.VMEM(query_w.shape, bf16),
            pltpu.VMEM((key_w.shape[0], 2 * kv_width), bf16),
            pltpu.VMEM(out_second.shape, bf16),
            pltpu.VMEM(bias_first.shape, f32),
            pltpu.VMEM(bias_second.shape, f32),
            pltpu.VMEM((1, norm_gain.shape[0]), f32),
            pltpu.VMEM((1, tok_rows), jnp.int32),
            pltpu.VMEM((SPAN + tok_rows, 2 * kv_width), bf16),
            pltpu.VMEM((SPAN + tok_rows, 2 * kv_width), bf16),
            pltpu.VMEM((hops, 1, tok_rows), jnp.int32),
            pltpu.VMEM((SPAN + tok_rows, LANES), f32),
            pltpu.VMEM((tok_rows // SEG, BAND, LANES), f32),
            pltpu.VMEM((kv_local, BAND, group_width), f32),
            pltpu.VMEM((kv_local, BAND, group_width), f32),
            pltpu.VMEM((tok_rows, query_width), bf16),
            pltpu.VMEM((tok_rows, query_width), bf16),
            pltpu.VMEM((tok_rows, query_width), bf16),
            pltpu.VMEM((halves, tok_rows, width_local), bf16),
            pltpu.VMEM((halves, tok_rows, width_local), bf16),
            pltpu.VMEM((halves, tok_rows, width_local), bf16),
            pltpu.VMEM((tok_rows, width_local), bf16),
            pltpu.VMEM((halves, tok_rows, width_local), bf16),
            pltpu.VMEM((tok_rows, halves * width_local), bf16),
            pltpu.VMEM((units, group_width, LANES), bf16),
            pltpu.VMEM((2, kv_width, pl.cdiv(SPAN + tok_rows, LANES) * LANES), bf16),
            pltpu.VMEM((units, BAND, group_width), f32),
            pltpu.VMEM((units, BAND, group_width), bf16),
            pltpu.VMEM((units, 2, group_width), f32),
            pltpu.VMEM((units, HEAD_SIZE, group_width), f32),
            pltpu.SemaphoreType.DMA((n_sems,)),
            pltpu.SemaphoreType.DMA((n_sems,)),
            pltpu.SemaphoreType.DMA((13,)),
        ],
        compiler_params=pltpu.CompilerParams(collective_id=0, has_side_effects=True),
    )(
        residual,
        query_first,
        key_first,
        value_first,
        documents.reshape(1, tok_rows),
        bias_first,
        out_first,
        norm_gain.reshape(1, -1),
        query_w,
        key_w,
        value_w,
        bias_second,
        out_second,
    )


def solution(mesh):
    placed = (
        P("sp", "tp"),
        P("sp", "tp"),
        P("sp", "tp"),
        P("sp", "tp"),
        P("sp"),
        P("tp", None),
        P("tp", None),
        P(),
        P(None, "tp"),
        P(None, "tp"),
        P(None, "tp"),
        P("tp", None),
        P("tp", None),
    )
    return jax.shard_map(body, mesh=mesh, in_specs=placed, out_specs=P("sp", "tp"), check_vma=False)
```

```python
import functools

import jax
import jax.numpy as jnp
from jax import lax
from jax.experimental import pallas as pl
from jax.experimental.pallas import tpu as pltpu
from jax.sharding import PartitionSpec as P

HEAD_SIZE = 64
SEG = 64
PAST = 4
REL_CLIP = 256
SPAN = PAST * SEG
BAND = SPAN + SEG
LANES = 128
LOG2E = 1.4426950408889634
HIDDEN = -1e30
MESH = pl.DeviceIdType.MESH


eps = 1e-06


def hops_of(tok_rows):
    return range(1, (SPAN + tok_rows - 1) // tok_rows + 1)


def pieces_of(tok_rows):
    pieces = []
    for distance in hops_of(tok_rows):
        top = SPAN - (distance - 1) * tok_rows
        bottom = max(0, top - tok_rows)
        cuts = [cut for cut in range(SEG, tok_rows, SEG) if bottom < cut < top]
        edges = [bottom] + cuts + [top]
        for low, high in reversed(list(zip(edges[:-1], edges[1:]))):
            pieces.append((distance, tok_rows - (top - low), high - low, low))
    return pieces


def build_bias(table_ref, bias_ref):
    heads_local = table_ref.shape[0]
    group_size = bias_ref.shape[2] // SEG
    lane = lax.broadcasted_iota(jnp.int32, (SEG, LANES), 1)
    low = lane < SEG
    last = REL_CLIP + SPAN

    def tile(head, index):
        if index == 0:
            return jnp.broadcast_to(table_ref[head : head + 1, last : last + 1], (SEG, LANES))
        first = last - index * LANES
        return jnp.broadcast_to(table_ref[head : head + 1, first : first + LANES], (SEG, LANES))

    def piece(head, block, base):
        back = block // 2
        if block % 2 == 0:
            source = jnp.where(low, tile(head, back), tile(head, back + 1))
            shift = base
        else:
            source = tile(head, back + 1)
            shift = (base + SEG) % LANES
        return pltpu.roll(source, shift, 1, stride=1, stride_axis=0)

    for head in range(0, heads_local, 2):
        for block in range(PAST + 1):
            pair = jnp.where(low, piece(head, block, 0), piece(head + 1, block, SEG)) * LOG2E
            group, inner = head // group_size, head % group_size
            bias_ref[group, block * SEG : (block + 1) * SEG, inner * SEG : (inner + 2) * SEG] = pair


class Attention:
    def __init__(self, query, kv, bias, mask, mixed, padded, turned, scores, weights, stats, blend):
        self.query, self.kv, self.bias, self.mask, self.mixed = query, kv, bias, mask, mixed
        self.padded, self.turned, self.scores, self.weights = padded, turned, scores, weights
        self.stats, self.blend = stats, blend
        self.groups = bias.shape[0]
        self.group_size = bias.shape[2] // SEG
        self.kv_width = self.groups * HEAD_SIZE
        self.state = {}

    def unit(self, segment, group):
        return segment * self.groups + group

    def pad_queries(self, segment):
        lane = lax.broadcasted_iota(jnp.int32, (SEG, LANES), 1)
        rows = slice(segment * SEG, (segment + 1) * SEG)
        for group in range(self.groups):
            keep = (lane >= group * HEAD_SIZE) & (lane < (group + 1) * HEAD_SIZE)
            for inner in range(self.group_size):
                head = group * self.group_size + inner
                column = head * HEAD_SIZE // LANES * LANES
                block = self.query[rows, column : column + LANES]
                if head % 2 != group % 2:
                    block = jnp.concatenate([block[:, HEAD_SIZE:], block[:, :HEAD_SIZE]], axis=1)
                self.padded[self.unit(segment, group), inner * SEG : (inner + 1) * SEG] = jnp.where(
                    keep, block, jnp.zeros_like(block)
                )

    def turn_values(self, row):
        block = jnp.transpose(self.kv[row : row + SEG, self.kv_width : 2 * self.kv_width])
        self.turned[0, :, row : row + SEG] = block
        if row >= SEG:
            self.turned[1, :, row - SEG : row] = block

    def bounds(self, segment, local):
        first = segment * SEG
        return (max(first, SPAN), first + BAND) if local else (first, SPAN)

    def score(self, segment, group, local):
        low, high = self.bounds(segment, local)
        unit = self.unit(segment, group)
        band = slice(low - segment * SEG, high - segment * SEG)
        scores = lax.dot_general(
            self.kv[low:high, : self.kv_width],
            self.padded[unit],
            (((1,), (1,)), ((), ())),
            preferred_element_type=jnp.float32,
        )
        mask = self.mask[segment, band]
        mask = jnp.concatenate([mask] * (self.group_size * SEG // LANES), axis=1)
        scores = scores * (HEAD_SIZE ** (-0.5) * LOG2E) + self.bias[group, band] + mask
        self.scores[unit, band] = scores
        largest = jnp.max(scores, axis=0, keepdims=True)
        if local:
            self.stats[unit, 0:1] = largest
        else:
            largest = jnp.maximum(largest, self.stats[unit, 0:1])
        self.state[unit] = (largest,)

    def weigh(self, segment, group, local):
        low, high = self.bounds(segment, local)
        unit = self.unit(segment, group)
        band = slice(low - segment * SEG, high - segment * SEG)
        (largest,) = self.state[unit]
        weight = jnp.exp2(self.scores[unit, band] - largest)
        self.weights[unit, band] = weight.astype(jnp.bfloat16)
        total = jnp.sum(weight, axis=0, keepdims=True)
        if local:
            self.stats[unit, 1:2] = total
        else:
            fade = jnp.exp2(self.stats[unit, 0:1] - largest)
            inverse = 1.0 / (total + self.stats[unit, 1:2] * fade)
            self.state[unit] = (fade, inverse)

    def gather(self, segment, group, local):
        low, high = self.bounds(segment, local)
        unit = self.unit(segment, group)
        band = slice(low - segment * SEG, high - segment * SEG)
        odd = low // SEG % 2
        blended = lax.dot_general(
            self.turned[
                odd,
                group * HEAD_SIZE : (group + 1) * HEAD_SIZE,
                low - odd * SEG : high - odd * SEG,
            ],
            self.weights[unit, band],
            (((1,), (0,)), ((), ())),
            preferred_element_type=jnp.float32,
        )
        if local:
            self.blend[unit] = blended
            return
        fade, inverse = self.state[unit]
        blended = (blended + self.blend[unit] * fade) * inverse
        rows = slice(segment * SEG, (segment + 1) * SEG)
        for pair in range(self.group_size // 2):
            turned = jnp.transpose(blended[:, pair * LANES : (pair + 1) * LANES])
            both = jnp.concatenate([turned[:SEG], turned[SEG:]], axis=1)
            column = (group * self.group_size + 2 * pair) * HEAD_SIZE
            self.mixed[rows, column : column + LANES] = both.astype(jnp.bfloat16)

    def run(self, segments, local, before=None, after=None):
        units = [(segment, group) for segment in segments for group in range(self.groups)]

        def score(unit):
            if before is not None:
                before(unit[0])
            self.score(*unit, local)

        def gather(unit):
            self.gather(*unit, local)
            if after is not None and unit[1] == self.groups - 1:
                after(unit[0])

        score(units[0])
        for index, unit in enumerate(units):
            if index + 1 < len(units):
                score(units[index + 1])
            if index > 0:
                gather(units[index - 1])
            self.weigh(*unit, local)
        gather(units[-1])


def kernel(
    n_sp,
    residual_hbm,
    query_hbm,
    key_hbm,
    value_hbm,
    docs_hbm,
    bias_one_hbm,
    out_one_hbm,
    gain_hbm,
    query_w_hbm,
    key_w_hbm,
    value_w_hbm,
    bias_two_hbm,
    out_two_hbm,
    result_ref,
    w_out_one,
    w_query,
    w_kv,
    w_out_two,
    bias_one,
    bias_two,
    gain,
    docs,
    kv_one,
    kv_two,
    docs_prior,
    docs_col,
    mask,
    table_one,
    table_two,
    mixed,
    query_one,
    query_two,
    residual_full,
    part_own,
    part_in,
    last_in,
    layer,
    base,
    scaled,
    scales,
    padded,
    turned,
    scores,
    weights,
    stats,
    blend,
    send_sem,
    recv_sem,
    load_sem,
):
    me = lax.axis_index("sp")
    my_tp = lax.axis_index("tp")
    other = 1 - my_tp
    tok_rows, width_local = residual_hbm.shape
    kv_width = key_hbm.shape[1]
    segments = tok_rows // SEG
    hops = hops_of(tok_rows)
    pieces = pieces_of(tok_rows)
    halves = part_own.shape[0]
    blocks = [(range(segments - 1, 0, -1), SEG, tok_rows - SEG), (range(1), 0, SEG)]

    barrier = pltpu.get_barrier_semaphore()
    expected = jnp.int32(1)
    for distance in hops:
        expected = expected + (me + distance < n_sp).astype(jnp.int32)

        @pl.when(me >= distance)
        def _():
            pl.semaphore_signal(
                barrier, inc=1, device_id={"sp": me - distance}, device_id_type=MESH
            )

    pl.semaphore_signal(barrier, inc=1, device_id={"tp": other}, device_id_type=MESH)

    own = pl.ds(SPAN, tok_rows)
    transfers = dict(
        bias_one=(bias_one_hbm, bias_one),
        key=(key_hbm, kv_one.at[own, pl.ds(0, kv_width)]),
        value=(value_hbm, kv_one.at[own, pl.ds(kv_width, kv_width)]),
        docs=(docs_hbm, docs),
        query=(query_hbm, query_one),
        residual=(residual_hbm, residual_full.at[my_tp]),
        bias_two=(bias_two_hbm, bias_two),
        out_one=(out_one_hbm, w_out_one),
        gain=(gain_hbm, gain),
        key_w=(key_w_hbm, w_kv.at[:, pl.ds(0, kv_width)]),
        value_w=(value_w_hbm, w_kv.at[:, pl.ds(kv_width, kv_width)]),
        query_w=(query_w_hbm, w_query),
        out_two=(out_two_hbm, w_out_two),
    )
    loads = {
        name: pltpu.make_async_copy(src, dst, load_sem.at[index])
        for index, (name, (src, dst)) in enumerate(transfers.items())
    }
    for load in loads.values():
        load.start()

    slot = iter(range(send_sem.shape[0]))

    def remote(src, dst, target):
        index = next(slot)
        return pltpu.make_async_remote_copy(
            src_ref=src,
            dst_ref=dst,
            send_sem=send_sem.at[index],
            recv_sem=recv_sem.at[index],
            device_id=target,
            device_id_type=MESH,
        )

    def ahead(distance):
        return {"sp": lax.rem(me + distance, n_sp)}

    def start_sent(distance, copies):
        @pl.when(me + distance < n_sp)
        def _():
            for copy in copies:
                copy.start()

    def wait_arrived(distance, copies):
        @pl.when(me >= distance)
        def _():
            for copy in copies:
                copy.wait_recv()

    def wait_sent(distance, copies):
        @pl.when(me + distance < n_sp)
        def _():
            for copy in copies:
                copy.wait_send()

    for distance, _, needed, landing in pieces:

        @pl.when(me < distance)
        def _():
            empty = jnp.zeros((needed, 2 * kv_width), jnp.bfloat16)
            kv_one[landing : landing + needed] = empty
            kv_two[landing : landing + needed] = empty

    for distance in hops:

        @pl.when(me < distance)
        def _():
            docs_prior[distance - 1] = jnp.full((1, tok_rows), -1, jnp.int32)

    eye = lax.broadcasted_iota(jnp.int32, (SEG, SEG), 0) == lax.broadcasted_iota(
        jnp.int32, (SEG, SEG), 1
    )

    def put_column(numbers, place):
        picked = jnp.where(eye, numbers.astype(jnp.float32), 0.0)
        docs_col[place : place + SEG] = jnp.broadcast_to(
            jnp.sum(picked, axis=1, keepdims=True), (SEG, LANES)
        )

    def put_mask(segment, low, high):
        mine = docs[:, segment * SEG : (segment + 1) * SEG].astype(jnp.float32)
        mine = jnp.concatenate([mine, mine], axis=1)
        same = docs_col[low:high] == mine
        first = segment * SEG
        mask[segment, low - first : high - first] = jnp.where(same, 0.0, HIDDEN)

    shared = (mask, mixed, padded, turned, scores, weights, stats, blend)
    one = Attention(query_one, kv_one, table_one, *shared)
    two = Attention(query_two, kv_two, table_two, *shared)
    newest_first = range(segments - 1, -1, -1)

    for name in ("key", "value", "docs", "query"):
        loads[name].wait()
    for row in range(SPAN, SPAN + tok_rows, SEG):
        one.turn_values(row)
    for segment in newest_first:
        one.pad_queries(segment)
    for block in range(0, tok_rows, SEG):
        put_column(docs[:, block : block + SEG], SPAN + block)
    for segment in range(segments):
        put_mask(segment, *one.bounds(segment, True))

    pl.semaphore_wait(barrier, expected)

    def halo_copy(kv, piece):
        distance, row, needed, landing = piece
        return remote(
            kv.at[pl.ds(SPAN + row, needed)], kv.at[pl.ds(landing, needed)], ahead(distance)
        )

    docs_copies = [
        (distance, [remote(docs, docs_prior.at[distance - 1], ahead(distance))])
        for distance in hops
    ]
    first_copies = [(piece[0], [halo_copy(kv_one, piece)]) for piece in pieces]
    for distance, copies in docs_copies + first_copies:
        start_sent(distance, copies)
    loads["residual"].wait()
    residual_copy = remote(residual_full.at[my_tp], residual_full.at[my_tp], {"tp": other})
    residual_copy.start()

    loads["bias_one"].wait()
    build_bias(bias_one, table_one)
    one.run(newest_first, True)

    loads["bias_two"].wait()
    build_bias(bias_two, table_two)

    for distance, copies in docs_copies:
        wait_arrived(distance, copies)
    for distance, row, needed, landing in pieces:
        for block in range(0, needed, SEG):
            put_column(
                docs_prior[distance - 1, :, row + block : row + block + SEG], landing + block
            )
    for segment in range(segments):
        put_mask(segment, *one.bounds(segment, False))
    residual_copy.wait_recv()
    loads["out_one"].wait()

    def halo_run(attention, waiting, after):
        done = set()

        def before(segment):
            for (_, _, needed, landing), (distance, copies) in zip(pieces, waiting):
                if landing + needed > segment * SEG and landing not in done:
                    done.add(landing)
                    wait_arrived(distance, copies)
                    for row in range(landing, landing + needed, SEG):
                        attention.turn_values(row)

        attention.run(newest_first, False, before, after)

    block_after = {min(members): (start, count) for members, start, count in blocks}
    part_copies = []

    def project_one(segment):
        if segment not in block_after:
            return
        start, count = block_after[segment]
        rows = pl.ds(start, count)
        copies = []
        for half in range(halves):
            part = jnp.dot(
                mixed[start : start + count],
                w_out_one[:, half * width_local : (half + 1) * width_local],
                preferred_element_type=jnp.float32,
            ).astype(jnp.bfloat16)
            part_own[half, start : start + count] = part
            copy = remote(part_own.at[half, rows], part_in.at[half, rows], {"tp": other})
            copy.start()
            copies.append(copy)
            base[half, start : start + count] = residual_full[
                half, start : start + count
            ].astype(jnp.float32) + part.astype(jnp.float32)
        part_copies.append(copies)

    halo_run(one, first_copies, project_one)

    for name in ("gain", "key_w", "value_w", "query_w"):
        loads[name].wait()
    second_copies = [None] * len(pieces)
    for (_, start, count), copies in zip(blocks, part_copies):
        rows = slice(start, start + count)
        squares = jnp.zeros((count, LANES), jnp.float32)
        for half in range(halves):
            copies[half].wait_recv()
            new = base[half, rows] + part_in[half, rows].astype(jnp.float32)
            new = new.astype(jnp.bfloat16)
            layer[half, rows] = new
            new = new.astype(jnp.float32)
            columns = slice(half * width_local, (half + 1) * width_local)
            scaled[rows, columns] = (new * gain[:, columns]).astype(jnp.bfloat16)
            for lane in range(0, width_local, LANES):
                squares = squares + new[:, lane : lane + LANES] * new[:, lane : lane + LANES]
        scale = lax.rsqrt(
            jnp.sum(squares, axis=1, keepdims=True) / (halves * width_local) + eps
        )
        scales[rows] = jnp.broadcast_to(scale, (count, LANES))
        kv_two[SPAN + start : SPAN + start + count] = (
            jnp.dot(scaled[rows], w_kv[...], preferred_element_type=jnp.float32) * scale
        ).astype(jnp.bfloat16)
        for index, piece in enumerate(pieces):
            if start <= piece[1] < start + count:
                second_copies[index] = (piece[0], [halo_copy(kv_two, piece)])
                start_sent(*second_copies[index])
    query_two[...] = (
        jnp.dot(scaled[...], w_query[...], preferred_element_type=jnp.float32) * scales[:, 0:1]
    ).astype(jnp.bfloat16)
    for row in range(SPAN, SPAN + tok_rows, SEG):
        two.turn_values(row)
    for segment in newest_first:
        two.pad_queries(segment)
    two.run(newest_first, True)
    for copies in part_copies:
        for copy in copies:
            copy.wait_send()

    loads["out_two"].wait()
    theirs = pl.ds(pl.multiple_of(other * width_local, width_local), width_local)
    ours = pl.ds(pl.multiple_of(my_tp * width_local, width_local), width_local)
    last_copies = []

    def project_two(segment):
        if segment not in block_after:
            return
        start, count = block_after[segment]
        rows = pl.ds(start, count)
        part_own[0, start : start + count] = jnp.dot(
            mixed[start : start + count], w_out_two[:, theirs], preferred_element_type=jnp.float32
        ).astype(jnp.bfloat16)
        copy = remote(part_own.at[0, rows], last_in.at[rows], {"tp": other})
        copy.start()
        last_copies.append(copy)

    halo_run(two, second_copies, project_two)
    part_own[1] = jnp.dot(
        mixed[...], w_out_two[:, ours], preferred_element_type=jnp.float32
    ).astype(jnp.bfloat16)
    for (_, start, count), copy in zip(blocks, last_copies):
        rows = slice(start, start + count)
        copy.wait_recv()
        branch = part_own[1, rows].astype(jnp.float32) + last_in[rows].astype(jnp.float32)
        result_ref[rows] = (layer[my_tp, rows].astype(jnp.float32) + branch).astype(jnp.bfloat16)

    residual_copy.wait_send()
    for distance, copies in docs_copies + first_copies + second_copies:
        wait_sent(distance, copies)
    for copy in last_copies:
        copy.wait_send()


def body(
    residual,
    query_first,
    key_first,
    value_first,
    documents,
    bias_first,
    out_first,
    norm_gain,
    query_w,
    key_w,
    value_w,
    bias_second,
    out_second,
):
    n_sp = lax.axis_size("sp")
    tok_rows, width_local = residual.shape
    query_width = query_first.shape[1]
    kv_width = key_first.shape[1]
    kv_local = kv_width // HEAD_SIZE
    group_width = query_width // kv_local
    halves = out_first.shape[1] // width_local
    hops = len(hops_of(tok_rows))
    units = tok_rows // SEG * kv_local
    n_sems = hops + 2 * len(pieces_of(tok_rows)) + 1 + 2 * halves + 2
    vmem = pl.BlockSpec(memory_space=pltpu.VMEM)
    hbm = pl.BlockSpec(memory_space=pl.ANY)
    bf16 = jnp.bfloat16
    f32 = jnp.float32
    return pl.pallas_call(
        functools.partial(kernel, n_sp),
        name="two_layers",
        out_shape=pltpu.VMEM((tok_rows, width_local), bf16),
        in_specs=[hbm] * 13,
        out_specs=vmem,
        scratch_shapes=[
            pltpu.VMEM(out_first.shape, bf16),
            pltpu.VMEM(query_w.shape, bf16),
            pltpu.VMEM((key_w.shape[0], 2 * kv_width), bf16),
            pltpu.VMEM(out_second.shape, bf16),
            pltpu.VMEM(bias_first.shape, f32),
            pltpu.VMEM(bias_second.shape, f32),
            pltpu.VMEM((1, norm_gain.shape[0]), f32),
            pltpu.VMEM((1, tok_rows), jnp.int32),
            pltpu.VMEM((SPAN + tok_rows, 2 * kv_width), bf16),
            pltpu.VMEM((SPAN + tok_rows, 2 * kv_width), bf16),
            pltpu.VMEM((hops, 1, tok_rows), jnp.int32),
            pltpu.VMEM((SPAN + tok_rows, LANES), f32),
            pltpu.VMEM((tok_rows // SEG, BAND, LANES), f32),
            pltpu.VMEM((kv_local, BAND, group_width), f32),
            pltpu.VMEM((kv_local, BAND, group_width), f32),
            pltpu.VMEM((tok_rows, query_width), bf16),
            pltpu.VMEM((tok_rows, query_width), bf16),
            pltpu.VMEM((tok_rows, query_width), bf16),
            pltpu.VMEM((halves, tok_rows, width_local), bf16),
            pltpu.VMEM((halves, tok_rows, width_local), bf16),
            pltpu.VMEM((halves, tok_rows, width_local), bf16),
            pltpu.VMEM((tok_rows, width_local), bf16),
            pltpu.VMEM((halves, tok_rows, width_local), bf16),
            pltpu.VMEM((halves, tok_rows, width_local), f32),
            pltpu.VMEM((tok_rows, halves * width_local), bf16),
            pltpu.VMEM((tok_rows, LANES), f32),
            pltpu.VMEM((units, group_width, LANES), bf16),
            pltpu.VMEM((2, kv_width, pl.cdiv(SPAN + tok_rows, LANES) * LANES), bf16),
            pltpu.VMEM((units, BAND, group_width), f32),
            pltpu.VMEM((units, BAND, group_width), bf16),
            pltpu.VMEM((units, 2, group_width), f32),
            pltpu.VMEM((units, HEAD_SIZE, group_width), f32),
            pltpu.SemaphoreType.DMA((n_sems,)),
            pltpu.SemaphoreType.DMA((n_sems,)),
            pltpu.SemaphoreType.DMA((13,)),
        ],
        compiler_params=pltpu.CompilerParams(collective_id=0, has_side_effects=True),
    )(
        residual,
        query_first,
        key_first,
        value_first,
        documents.reshape(1, tok_rows),
        bias_first,
        out_first,
        norm_gain.reshape(1, -1),
        query_w,
        key_w,
        value_w,
        bias_second,
        out_second,
    )


def solution(mesh):
    placed = (
        P("sp", "tp"),
        P("sp", "tp"),
        P("sp", "tp"),
        P("sp", "tp"),
        P("sp"),
        P("tp", None),
        P("tp", None),
        P(),
        P(None, "tp"),
        P(None, "tp"),
        P(None, "tp"),
        P("tp", None),
        P("tp", None),
    )
    return jax.shard_map(body, mesh=mesh, in_specs=placed, out_specs=P("sp", "tp"), check_vma=False)
```

```python
import functools

import jax
import jax.numpy as jnp
from jax import lax
from jax.experimental import pallas as pl
from jax.experimental.pallas import tpu as pltpu
from jax.sharding import PartitionSpec as P

HEAD_SIZE = 64
SEG = 64
PAST = 4
REL_CLIP = 256
SPAN = PAST * SEG
BAND = SPAN + SEG
LANES = 128
LOG2E = 1.4426950408889634
HIDDEN = -1e30
MESH = pl.DeviceIdType.MESH


eps = 1e-06


def hops_of(tok_rows):
    return range(1, (SPAN + tok_rows - 1) // tok_rows + 1)


def pieces_of(tok_rows):
    pieces = []
    for distance in hops_of(tok_rows):
        top = SPAN - (distance - 1) * tok_rows
        bottom = max(0, top - tok_rows)
        cuts = [cut for cut in range(SEG, tok_rows, SEG) if bottom < cut < top]
        edges = [bottom] + cuts + [top]
        for low, high in reversed(list(zip(edges[:-1], edges[1:]))):
            pieces.append((distance, tok_rows - (top - low), high - low, low))
    return pieces


def build_bias(table_ref, bias_ref):
    heads_local = table_ref.shape[0]
    group_size = bias_ref.shape[2] // SEG
    lane = lax.broadcasted_iota(jnp.int32, (SEG, LANES), 1)
    low = lane < SEG
    last = REL_CLIP + SPAN

    def tile(head, index):
        if index == 0:
            return jnp.broadcast_to(table_ref[head : head + 1, last : last + 1], (SEG, LANES))
        first = last - index * LANES
        return jnp.broadcast_to(table_ref[head : head + 1, first : first + LANES], (SEG, LANES))

    def piece(head, block, base):
        back = block // 2
        if block % 2 == 0:
            source = jnp.where(low, tile(head, back), tile(head, back + 1))
            shift = base
        else:
            source = tile(head, back + 1)
            shift = (base + SEG) % LANES
        return pltpu.roll(source, shift, 1, stride=1, stride_axis=0)

    for head in range(0, heads_local, 2):
        for block in range(PAST + 1):
            pair = jnp.where(low, piece(head, block, 0), piece(head + 1, block, SEG)) * LOG2E
            group, inner = head // group_size, head % group_size
            bias_ref[group, block * SEG : (block + 1) * SEG, inner * SEG : (inner + 2) * SEG] = pair


class Attention:
    def __init__(self, query, kv, bias, mask, mixed, padded, turned, scores, weights, stats, blend):
        self.query, self.kv, self.bias, self.mask, self.mixed = query, kv, bias, mask, mixed
        self.padded, self.turned, self.scores, self.weights = padded, turned, scores, weights
        self.stats, self.blend = stats, blend
        self.groups = bias.shape[0]
        self.group_size = bias.shape[2] // SEG
        self.kv_width = self.groups * HEAD_SIZE
        self.state = {}

    def unit(self, segment, group):
        return segment * self.groups + group

    def pad_queries(self, segment):
        lane = lax.broadcasted_iota(jnp.int32, (SEG, LANES), 1)
        rows = slice(segment * SEG, (segment + 1) * SEG)
        for group in range(self.groups):
            keep = (lane >= group * HEAD_SIZE) & (lane < (group + 1) * HEAD_SIZE)
            for inner in range(self.group_size):
                head = group * self.group_size + inner
                column = head * HEAD_SIZE // LANES * LANES
                block = self.query[rows, column : column + LANES]
                if head % 2 != group % 2:
                    block = jnp.concatenate([block[:, HEAD_SIZE:], block[:, :HEAD_SIZE]], axis=1)
                self.padded[self.unit(segment, group), inner * SEG : (inner + 1) * SEG] = jnp.where(
                    keep, block, jnp.zeros_like(block)
                )

    def turn_values(self, row):
        block = jnp.transpose(self.kv[row : row + SEG, self.kv_width : 2 * self.kv_width])
        self.turned[0, :, row : row + SEG] = block
        if row >= SEG:
            self.turned[1, :, row - SEG : row] = block

    def bounds(self, segment, local):
        first = segment * SEG
        return (max(first, SPAN), first + BAND) if local else (first, SPAN)

    def score(self, segment, group, local):
        low, high = self.bounds(segment, local)
        unit = self.unit(segment, group)
        band = slice(low - segment * SEG, high - segment * SEG)
        scores = lax.dot_general(
            self.kv[low:high, : self.kv_width],
            self.padded[unit],
            (((1,), (1,)), ((), ())),
            preferred_element_type=jnp.float32,
        )
        mask = self.mask[segment, band]
        mask = jnp.concatenate([mask] * (self.group_size * SEG // LANES), axis=1)
        scores = scores * (HEAD_SIZE ** (-0.5) * LOG2E) + self.bias[group, band] + mask
        self.scores[unit, band] = scores
        largest = jnp.max(scores, axis=0, keepdims=True)
        if local:
            self.stats[unit, 0:1] = largest
        else:
            largest = jnp.maximum(largest, self.stats[unit, 0:1])
        self.state[unit] = (largest,)

    def weigh(self, segment, group, local):
        low, high = self.bounds(segment, local)
        unit = self.unit(segment, group)
        band = slice(low - segment * SEG, high - segment * SEG)
        (largest,) = self.state[unit]
        weight = jnp.exp2(self.scores[unit, band] - largest)
        self.weights[unit, band] = weight.astype(jnp.bfloat16)
        total = jnp.sum(weight, axis=0, keepdims=True)
        if local:
            self.stats[unit, 1:2] = total
        else:
            fade = jnp.exp2(self.stats[unit, 0:1] - largest)
            inverse = 1.0 / (total + self.stats[unit, 1:2] * fade)
            self.state[unit] = (fade, inverse)

    def gather(self, segment, group, local):
        low, high = self.bounds(segment, local)
        unit = self.unit(segment, group)
        band = slice(low - segment * SEG, high - segment * SEG)
        odd = low // SEG % 2
        blended = lax.dot_general(
            self.turned[
                odd,
                group * HEAD_SIZE : (group + 1) * HEAD_SIZE,
                low - odd * SEG : high - odd * SEG,
            ],
            self.weights[unit, band],
            (((1,), (0,)), ((), ())),
            preferred_element_type=jnp.float32,
        )
        if local:
            self.blend[unit] = blended
            return
        fade, inverse = self.state[unit]
        blended = (blended + self.blend[unit] * fade) * inverse
        rows = slice(segment * SEG, (segment + 1) * SEG)
        for pair in range(self.group_size // 2):
            turned = jnp.transpose(blended[:, pair * LANES : (pair + 1) * LANES])
            both = jnp.concatenate([turned[:SEG], turned[SEG:]], axis=1)
            column = (group * self.group_size + 2 * pair) * HEAD_SIZE
            self.mixed[rows, column : column + LANES] = both.astype(jnp.bfloat16)

    def run(self, segments, local, before=None, after=None):
        units = [(segment, group) for segment in segments for group in range(self.groups)]

        def score(unit):
            if before is not None:
                before(unit[0])
            self.score(*unit, local)

        def gather(unit):
            self.gather(*unit, local)
            if after is not None and unit[1] == self.groups - 1:
                after(unit[0])

        score(units[0])
        for index, unit in enumerate(units):
            if index + 1 < len(units):
                score(units[index + 1])
            if index > 0:
                gather(units[index - 1])
            self.weigh(*unit, local)
        gather(units[-1])


def kernel(
    n_sp,
    residual_hbm,
    query_hbm,
    key_hbm,
    value_hbm,
    docs_hbm,
    bias_one_hbm,
    out_one_hbm,
    gain_hbm,
    query_w_hbm,
    key_w_hbm,
    value_w_hbm,
    bias_two_hbm,
    out_two_hbm,
    result_ref,
    w_out_one,
    w_query,
    w_kv,
    w_out_two,
    kv_one,
    kv_two,
    docs_col,
    mask,
    table_one,
    table_two,
    mixed,
    query_one,
    query_two,
    residual_full,
    part_own,
    part_in,
    last_in,
    layer,
    base,
    scaled,
    scales,
    padded,
    turned,
    scores,
    weights,
    blend,
    bias_one,
    bias_two,
    gain,
    docs,
    docs_prior,
    stats,
    send_sem,
    recv_sem,
    load_sem,
):
    me = lax.axis_index("sp")
    my_tp = lax.axis_index("tp")
    other = 1 - my_tp
    tok_rows, width_local = residual_hbm.shape
    kv_width = key_hbm.shape[1]
    segments = tok_rows // SEG
    hops = hops_of(tok_rows)
    pieces = pieces_of(tok_rows)
    halves = part_own.shape[0]
    blocks = [(range(segments - 1, 0, -1), SEG, tok_rows - SEG), (range(1), 0, SEG)]

    barrier = pltpu.get_barrier_semaphore()
    expected = jnp.int32(1)
    for distance in hops:
        expected = expected + (me + distance < n_sp).astype(jnp.int32)

        @pl.when(me >= distance)
        def _():
            pl.semaphore_signal(
                barrier, inc=1, device_id={"sp": me - distance}, device_id_type=MESH
            )

    pl.semaphore_signal(barrier, inc=1, device_id={"tp": other}, device_id_type=MESH)

    own = pl.ds(SPAN, tok_rows)
    transfers = dict(
        key=(key_hbm, kv_one.at[own, pl.ds(0, kv_width)]),
        value=(value_hbm, kv_one.at[own, pl.ds(kv_width, kv_width)]),
        docs=(docs_hbm, docs),
        bias_one=(bias_one_hbm, bias_one),
        query=(query_hbm, query_one),
        residual=(residual_hbm, residual_full.at[my_tp]),
        bias_two=(bias_two_hbm, bias_two),
        out_one=(out_one_hbm, w_out_one),
        gain=(gain_hbm, gain),
        key_w=(key_w_hbm, w_kv.at[:, pl.ds(0, kv_width)]),
        value_w=(value_w_hbm, w_kv.at[:, pl.ds(kv_width, kv_width)]),
        query_w=(query_w_hbm, w_query),
        out_two=(out_two_hbm, w_out_two),
    )
    loads = {
        name: pltpu.make_async_copy(src, dst, load_sem.at[index])
        for index, (name, (src, dst)) in enumerate(transfers.items())
    }
    for load in loads.values():
        load.start()

    slot = iter(range(send_sem.shape[0]))

    def remote(src, dst, target):
        index = next(slot)
        return pltpu.make_async_remote_copy(
            src_ref=src,
            dst_ref=dst,
            send_sem=send_sem.at[index],
            recv_sem=recv_sem.at[index],
            device_id=target,
            device_id_type=MESH,
        )

    def ahead(distance):
        return {"sp": lax.rem(me + distance, n_sp)}

    def start_sent(distance, copies):
        @pl.when(me + distance < n_sp)
        def _():
            for copy in copies:
                copy.start()

    def wait_arrived(distance, copies):
        @pl.when(me >= distance)
        def _():
            for copy in copies:
                copy.wait_recv()

    def wait_sent(distance, copies):
        @pl.when(me + distance < n_sp)
        def _():
            for copy in copies:
                copy.wait_send()

    for distance, _, needed, landing in pieces:

        @pl.when(me < distance)
        def _():
            empty = jnp.zeros((needed, 2 * kv_width), jnp.bfloat16)
            kv_one[landing : landing + needed] = empty
            kv_two[landing : landing + needed] = empty

    for distance in hops:

        @pl.when(me < distance)
        def _():
            docs_prior[distance - 1] = jnp.full((1, tok_rows), -1, jnp.int32)

    eye = lax.broadcasted_iota(jnp.int32, (SEG, SEG), 0) == lax.broadcasted_iota(
        jnp.int32, (SEG, SEG), 1
    )

    def put_column(numbers, place):
        picked = jnp.where(eye, numbers.astype(jnp.float32), 0.0)
        docs_col[place : place + SEG] = jnp.broadcast_to(
            jnp.sum(picked, axis=1, keepdims=True), (SEG, LANES)
        )

    def put_mask(segment, low, high):
        mine = docs[:, segment * SEG : (segment + 1) * SEG].astype(jnp.float32)
        mine = jnp.concatenate([mine, mine], axis=1)
        same = docs_col[low:high] == mine
        first = segment * SEG
        mask[segment, low - first : high - first] = jnp.where(same, 0.0, HIDDEN)

    shared = (mask, mixed, padded, turned, scores, weights, stats, blend)
    one = Attention(query_one, kv_one, table_one, *shared)
    two = Attention(query_two, kv_two, table_two, *shared)
    newest_first = range(segments - 1, -1, -1)

    for name in ("key", "value", "docs"):
        loads[name].wait()
    pl.semaphore_wait(barrier, expected)

    def halo_copy(kv, piece):
        distance, row, needed, landing = piece
        return remote(
            kv.at[pl.ds(SPAN + row, needed)], kv.at[pl.ds(landing, needed)], ahead(distance)
        )

    docs_copies = [
        (distance, [remote(docs, docs_prior.at[distance - 1], ahead(distance))])
        for distance in hops
    ]
    first_copies = [(piece[0], [halo_copy(kv_one, piece)]) for piece in pieces]
    for distance, copies in docs_copies + first_copies:
        start_sent(distance, copies)
    loads["residual"].wait()
    residual_copy = remote(residual_full.at[my_tp], residual_full.at[my_tp], {"tp": other})
    residual_copy.start()

    loads["query"].wait()
    for row in range(SPAN, SPAN + tok_rows, SEG):
        one.turn_values(row)
    for segment in newest_first:
        one.pad_queries(segment)
    for block in range(0, tok_rows, SEG):
        put_column(docs[:, block : block + SEG], SPAN + block)
    for segment in range(segments):
        put_mask(segment, *one.bounds(segment, True))

    loads["bias_one"].wait()
    build_bias(bias_one, table_one)
    one.run(newest_first, True)

    for distance, copies in docs_copies:
        wait_arrived(distance, copies)
    for distance, row, needed, landing in pieces:
        for block in range(0, needed, SEG):
            put_column(
                docs_prior[distance - 1, :, row + block : row + block + SEG], landing + block
            )
    for segment in range(segments):
        put_mask(segment, *one.bounds(segment, False))
    residual_copy.wait_recv()
    loads["out_one"].wait()

    def halo_run(attention, waiting, members, done):
        def before(segment):
            if segment < segments - 1:
                segment = 0
            for (_, _, needed, landing), (distance, copies) in zip(pieces, waiting):
                if landing + needed > segment * SEG and landing not in done:
                    done.add(landing)
                    wait_arrived(distance, copies)
                    for row in range(landing, landing + needed, SEG):
                        attention.turn_values(row)

        attention.run(members, False, before)

    part_copies = []
    for _, start, count in blocks:
        rows = pl.ds(start, count)
        part_copies.append(
            [
                remote(part_own.at[half, rows], part_in.at[half, rows], {"tp": other})
                for half in range(halves)
            ]
        )

    def project_one(block):
        _, start, count = blocks[block]
        rows = slice(start, start + count)
        parts = [
            jnp.dot(
                mixed[rows],
                w_out_one[:, half * width_local : (half + 1) * width_local],
                preferred_element_type=jnp.float32,
            ).astype(jnp.bfloat16)
            for half in range(halves)
        ]
        for half, part in enumerate(parts):
            part_own[half, rows] = part
        for copy in part_copies[block]:
            copy.start()
        for half, part in enumerate(parts):
            base[half, rows] = residual_full[half, rows].astype(jnp.float32) + part.astype(
                jnp.float32
            )

    second_copies = [(piece[0], [halo_copy(kv_two, piece)]) for piece in pieces]

    def keys_two(block):
        _, start, count = blocks[block]
        rows = slice(start, start + count)
        squares = jnp.zeros((count, LANES), jnp.float32)
        for half in range(halves):
            part_copies[block][half].wait_recv()
            new = base[half, rows] + part_in[half, rows].astype(jnp.float32)
            new = new.astype(jnp.bfloat16)
            layer[half, rows] = new
            new = new.astype(jnp.float32)
            columns = slice(half * width_local, (half + 1) * width_local)
            scaled[rows, columns] = (new * gain[:, columns]).astype(jnp.bfloat16)
            for lane in range(0, width_local, LANES):
                squares = squares + new[:, lane : lane + LANES] * new[:, lane : lane + LANES]
        scale = lax.rsqrt(
            jnp.sum(squares, axis=1, keepdims=True) / (halves * width_local) + eps
        )
        scales[rows] = jnp.broadcast_to(scale, (count, LANES))
        kv_two[SPAN + start : SPAN + start + count] = (
            jnp.dot(scaled[rows], w_kv[...], preferred_element_type=jnp.float32) * scale
        ).astype(jnp.bfloat16)
        for piece, copies in zip(pieces, second_copies):
            if start <= piece[1] < start + count:
                start_sent(*copies)

    for name in ("gain", "key_w", "value_w", "query_w"):
        loads[name].wait()
    done = set()
    halo_run(one, first_copies, blocks[0][0], done)
    project_one(0)

    @pl.when(my_tp == 0)
    def _():
        keys_two(0)

    halo_run(one, first_copies, blocks[1][0], done)
    project_one(1)
    loads["bias_two"].wait()

    @pl.when(my_tp == 1)
    def _():
        build_bias(bias_two, table_two)
        keys_two(0)

    keys_two(1)
    query_two[...] = (
        jnp.dot(scaled[...], w_query[...], preferred_element_type=jnp.float32) * scales[:, 0:1]
    ).astype(jnp.bfloat16)

    @pl.when(my_tp == 0)
    def _():
        build_bias(bias_two, table_two)

    for row in range(SPAN, SPAN + tok_rows, SEG):
        two.turn_values(row)
    for segment in newest_first:
        two.pad_queries(segment)
    two.run(newest_first, True)
    for copies in part_copies:
        for copy in copies:
            copy.wait_send()

    loads["out_two"].wait()
    theirs = pl.ds(pl.multiple_of(other * width_local, width_local), width_local)
    ours = pl.ds(pl.multiple_of(my_tp * width_local, width_local), width_local)
    halo_run(two, second_copies, newest_first, set())
    part_own[0] = jnp.dot(
        mixed[...], w_out_two[:, theirs], preferred_element_type=jnp.float32
    ).astype(jnp.bfloat16)
    quarter = width_local // 2
    last_copies = []
    for part in range(2):
        place = pl.ds(part * quarter, quarter)
        last_copies.append(remote(part_own.at[0, :, place], last_in.at[:, place], {"tp": other}))
        last_copies[-1].start()
    part_own[1] = jnp.dot(
        mixed[...], w_out_two[:, ours], preferred_element_type=jnp.float32
    ).astype(jnp.bfloat16)
    branch = part_own[1].astype(jnp.float32)
    branch = branch + layer[my_tp].astype(jnp.float32)
    for part, copy in enumerate(last_copies):
        columns = slice(part * quarter, (part + 1) * quarter)
        copy.wait_recv()
        result_ref[:, columns] = (
            branch[:, columns] + last_in[:, columns].astype(jnp.float32)
        ).astype(jnp.bfloat16)

    residual_copy.wait_send()
    for distance, copies in docs_copies + first_copies + second_copies:
        wait_sent(distance, copies)
    for copy in last_copies:
        copy.wait_send()


def body(
    residual,
    query_first,
    key_first,
    value_first,
    documents,
    bias_first,
    out_first,
    norm_gain,
    query_w,
    key_w,
    value_w,
    bias_second,
    out_second,
):
    n_sp = lax.axis_size("sp")
    tok_rows, width_local = residual.shape
    query_width = query_first.shape[1]
    kv_width = key_first.shape[1]
    kv_local = kv_width // HEAD_SIZE
    group_width = query_width // kv_local
    halves = out_first.shape[1] // width_local
    hops = len(hops_of(tok_rows))
    units = tok_rows // SEG * kv_local
    n_sems = hops + 2 * len(pieces_of(tok_rows)) + 1 + 2 * halves + 2
    vmem = pl.BlockSpec(memory_space=pltpu.VMEM)
    hbm = pl.BlockSpec(memory_space=pl.ANY)
    bf16 = jnp.bfloat16
    f32 = jnp.float32
    return pl.pallas_call(
        functools.partial(kernel, n_sp),
        name="two_layers",
        out_shape=pltpu.VMEM((tok_rows, width_local), bf16),
        in_specs=[hbm] * 13,
        out_specs=vmem,
        scratch_shapes=[
            pltpu.VMEM(out_first.shape, bf16),
            pltpu.VMEM(query_w.shape, bf16),
            pltpu.VMEM((key_w.shape[0], 2 * kv_width), bf16),
            pltpu.VMEM(out_second.shape, bf16),
            pltpu.VMEM((SPAN + tok_rows, 2 * kv_width), bf16),
            pltpu.VMEM((SPAN + tok_rows, 2 * kv_width), bf16),
            pltpu.VMEM((SPAN + tok_rows, LANES), f32),
            pltpu.VMEM((tok_rows // SEG, BAND, LANES), f32),
            pltpu.VMEM((kv_local, BAND, group_width), f32),
            pltpu.VMEM((kv_local, BAND, group_width), f32),
            pltpu.VMEM((tok_rows, query_width), bf16),
            pltpu.VMEM((tok_rows, query_width), bf16),
            pltpu.VMEM((tok_rows, query_width), bf16),
            pltpu.VMEM((halves, tok_rows, width_local), bf16),
            pltpu.VMEM((halves, tok_rows, width_local), bf16),
            pltpu.VMEM((halves, tok_rows, width_local), bf16),
            pltpu.VMEM((tok_rows, width_local), bf16),
            pltpu.VMEM((halves, tok_rows, width_local), bf16),
            pltpu.VMEM((halves, tok_rows, width_local), f32),
            pltpu.VMEM((tok_rows, halves * width_local), bf16),
            pltpu.VMEM((tok_rows, LANES), f32),
            pltpu.VMEM((units, group_width, LANES), bf16),
            pltpu.VMEM((2, kv_width, pl.cdiv(SPAN + tok_rows, LANES) * LANES), bf16),
            pltpu.VMEM((units, BAND, group_width), f32),
            pltpu.VMEM((units, BAND, group_width), bf16),
            pltpu.VMEM((units, HEAD_SIZE, group_width), f32),
            pltpu.VMEM(bias_first.shape, f32),
            pltpu.VMEM(bias_second.shape, f32),
            pltpu.VMEM((1, norm_gain.shape[0]), f32),
            pltpu.VMEM((1, tok_rows), jnp.int32),
            pltpu.VMEM((hops, 1, tok_rows), jnp.int32),
            pltpu.VMEM((units, 2, group_width), f32),
            pltpu.SemaphoreType.DMA((n_sems,)),
            pltpu.SemaphoreType.DMA((n_sems,)),
            pltpu.SemaphoreType.DMA((13,)),
        ],
        compiler_params=pltpu.CompilerParams(collective_id=0, has_side_effects=True),
    )(
        residual,
        query_first,
        key_first,
        value_first,
        documents.reshape(1, tok_rows),
        bias_first,
        out_first,
        norm_gain.reshape(1, -1),
        query_w,
        key_w,
        value_w,
        bias_second,
        out_second,
    )


def solution(mesh):
    placed = (
        P("sp", "tp"),
        P("sp", "tp"),
        P("sp", "tp"),
        P("sp", "tp"),
        P("sp"),
        P("tp", None),
        P("tp", None),
        P(),
        P(None, "tp"),
        P(None, "tp"),
        P(None, "tp"),
        P("tp", None),
        P("tp", None),
    )
    return jax.shard_map(body, mesh=mesh, in_specs=placed, out_specs=P("sp", "tp"), check_vma=False)
```

```python
import functools

import jax
import jax.numpy as jnp
from jax import lax
from jax.experimental import pallas as pl
from jax.experimental.pallas import tpu as pltpu
from jax.sharding import PartitionSpec as P

HEAD_SIZE = 64
SEG = 64
PAST = 4
REL_CLIP = 256
SPAN = PAST * SEG
BAND = SPAN + SEG
LANES = 128
LOG2E = 1.4426950408889634
HIDDEN = -1e30
MESH = pl.DeviceIdType.MESH


eps = 1e-06


def hops_of(tok_rows):
    return range(1, (SPAN + tok_rows - 1) // tok_rows + 1)


def pieces_of(tok_rows):
    pieces = []
    for distance in hops_of(tok_rows):
        top = SPAN - (distance - 1) * tok_rows
        bottom = max(0, top - tok_rows)
        cuts = [cut for cut in range(SEG, tok_rows, SEG) if bottom < cut < top]
        edges = [bottom] + cuts + [top]
        for low, high in reversed(list(zip(edges[:-1], edges[1:]))):
            pieces.append((distance, tok_rows - (top - low), high - low, low))
    return pieces


def build_bias(table_ref, bias_ref):
    heads_local = table_ref.shape[0]
    group_size = bias_ref.shape[2] // SEG
    lane = lax.broadcasted_iota(jnp.int32, (SEG, LANES), 1)
    low = lane < SEG
    last = REL_CLIP + SPAN

    def tile(head, index):
        if index == 0:
            return jnp.broadcast_to(table_ref[head : head + 1, last : last + 1], (SEG, LANES))
        first = last - index * LANES
        return jnp.broadcast_to(table_ref[head : head + 1, first : first + LANES], (SEG, LANES))

    def piece(head, block, base):
        back = block // 2
        if block % 2 == 0:
            source = jnp.where(low, tile(head, back), tile(head, back + 1))
            shift = base
        else:
            source = tile(head, back + 1)
            shift = (base + SEG) % LANES
        return pltpu.roll(source, shift, 1, stride=1, stride_axis=0)

    for head in range(0, heads_local, 2):
        for block in range(PAST + 1):
            pair = jnp.where(low, piece(head, block, 0), piece(head + 1, block, SEG)) * LOG2E
            group, inner = head // group_size, head % group_size
            bias_ref[group, block * SEG : (block + 1) * SEG, inner * SEG : (inner + 2) * SEG] = pair


class Attention:
    def __init__(self, query, kv, bias, mask, mixed, padded, turned, scores, weights, stats, blend):
        self.query, self.kv, self.bias, self.mask, self.mixed = query, kv, bias, mask, mixed
        self.padded, self.turned, self.scores, self.weights = padded, turned, scores, weights
        self.stats, self.blend = stats, blend
        self.cut = SPAN
        self.groups = bias.shape[0]
        self.group_size = bias.shape[2] // SEG
        self.kv_width = self.groups * HEAD_SIZE
        self.state = {}

    def unit(self, segment, group):
        return segment * self.groups + group

    def pad_queries(self, segment):
        lane = lax.broadcasted_iota(jnp.int32, (SEG, LANES), 1)
        rows = slice(segment * SEG, (segment + 1) * SEG)
        for group in range(self.groups):
            keep = (lane >= group * HEAD_SIZE) & (lane < (group + 1) * HEAD_SIZE)
            for inner in range(self.group_size):
                head = group * self.group_size + inner
                column = head * HEAD_SIZE // LANES * LANES
                block = self.query[rows, column : column + LANES]
                if head % 2 != group % 2:
                    block = jnp.concatenate([block[:, HEAD_SIZE:], block[:, :HEAD_SIZE]], axis=1)
                self.padded[self.unit(segment, group), inner * SEG : (inner + 1) * SEG] = jnp.where(
                    keep, block, jnp.zeros_like(block)
                )

    def turn_values(self, row):
        block = jnp.transpose(self.kv[row : row + SEG, self.kv_width : 2 * self.kv_width])
        self.turned[0, :, row : row + SEG] = block
        if row >= SEG:
            self.turned[1, :, row - SEG : row] = block

    def bounds(self, segment, phase):
        first = segment * SEG
        cut = max(first, self.cut)
        return {
            "local": (max(first, SPAN), first + BAND),
            "halo": (first, SPAN),
            "near": (cut, SPAN),
            "rest": (first, cut),
        }[phase]

    def score(self, segment, group, phase):
        low, high = self.bounds(segment, phase)
        unit = self.unit(segment, group)
        band = slice(low - segment * SEG, high - segment * SEG)
        scores = lax.dot_general(
            self.kv[low:high, : self.kv_width],
            self.padded[unit],
            (((1,), (1,)), ((), ())),
            preferred_element_type=jnp.float32,
        )
        mask = self.mask[segment, band]
        mask = jnp.concatenate([mask] * (self.group_size * SEG // LANES), axis=1)
        scores = scores * (HEAD_SIZE ** (-0.5) * LOG2E) + self.bias[group, band] + mask
        self.scores[unit, band] = scores
        largest = jnp.max(scores, axis=0, keepdims=True)
        if phase != "local":
            largest = jnp.maximum(largest, self.stats[unit, 0:1])
        self.state[unit] = (largest,)

    def weigh(self, segment, group, phase):
        low, high = self.bounds(segment, phase)
        unit = self.unit(segment, group)
        band = slice(low - segment * SEG, high - segment * SEG)
        (largest,) = self.state[unit]
        weight = jnp.exp2(self.scores[unit, band] - largest)
        self.weights[unit, band] = weight.astype(jnp.bfloat16)
        total = jnp.sum(weight, axis=0, keepdims=True)
        fade = None
        if phase != "local":
            fade = jnp.exp2(self.stats[unit, 0:1] - largest)
            total = total + self.stats[unit, 1:2] * fade
        if self.ends(segment, phase):
            self.state[unit] = (fade, 1.0 / total)
        else:
            self.stats[unit, 0:1] = largest
            self.stats[unit, 1:2] = total
            self.state[unit] = (fade,)

    def ends(self, segment, phase):
        return phase != "local" and self.bounds(segment, phase)[0] == segment * SEG

    def gather(self, segment, group, phase):
        low, high = self.bounds(segment, phase)
        unit = self.unit(segment, group)
        band = slice(low - segment * SEG, high - segment * SEG)
        odd = low // SEG % 2
        blended = lax.dot_general(
            self.turned[
                odd,
                group * HEAD_SIZE : (group + 1) * HEAD_SIZE,
                low - odd * SEG : high - odd * SEG,
            ],
            self.weights[unit, band],
            (((1,), (0,)), ((), ())),
            preferred_element_type=jnp.float32,
        )
        if phase != "local":
            blended = blended + self.blend[unit] * self.state[unit][0]
        if not self.ends(segment, phase):
            self.blend[unit] = blended
            return
        blended = (blended * self.state[unit][1]).astype(jnp.bfloat16)
        rows = slice(segment * SEG, (segment + 1) * SEG)
        for pair in range(self.group_size // 2):
            turned = jnp.transpose(blended[:, pair * LANES : (pair + 1) * LANES])
            both = jnp.concatenate([turned[:SEG], turned[SEG:]], axis=1)
            column = (group * self.group_size + 2 * pair) * HEAD_SIZE
            self.mixed[rows, column : column + LANES] = both

    def steps(self, segments, phase, arrivals=()):
        units = [(segment, group) for segment in segments for group in range(self.groups)]
        waits = {segment: wait for segment, wait, _ in arrivals}
        turns = {segment: rows for segment, _, rows in arrivals}

        def score(unit):
            segment, group = unit
            if group == 0 and segment in waits:
                waits[segment]()
            self.score(segment, group, phase)
            if group == self.groups - 1 and segment in turns:
                for row in turns[segment]:
                    self.turn_values(row)

        def weigh(unit):
            self.weigh(*unit, phase)

        def gather(unit):
            self.gather(*unit, phase)

        plan = [(score, units[0])]
        for index, unit in enumerate(units):
            if index + 1 < len(units):
                plan.append((score, units[index + 1]))
            if index > 0:
                plan.append((gather, units[index - 1]))
            plan.append((weigh, unit))
        plan.append((gather, units[-1]))
        return [functools.partial(step, unit) for step, unit in plan]

    def run(self, segments, phase, arrivals=()):
        for step in self.steps(segments, phase, arrivals):
            step()


def kernel(
    n_sp,
    residual_hbm,
    query_hbm,
    key_hbm,
    value_hbm,
    docs_hbm,
    bias_one_hbm,
    out_one_hbm,
    gain_hbm,
    query_w_hbm,
    key_w_hbm,
    value_w_hbm,
    bias_two_hbm,
    out_two_hbm,
    result_ref,
    w_out_one,
    w_query,
    w_kv,
    w_out_two,
    kv_one,
    kv_two,
    docs_col,
    mask,
    table_one,
    table_two,
    mixed,
    query_one,
    query_two,
    residual_full,
    part_own,
    part_in,
    last_in,
    layer,
    base,
    scaled,
    scales,
    padded,
    turned,
    scores,
    weights,
    blend,
    bias_one,
    bias_two,
    gain,
    docs,
    docs_prior,
    stats,
    send_sem,
    recv_sem,
    load_sem,
):
    me = lax.axis_index("sp")
    my_tp = lax.axis_index("tp")
    other = 1 - my_tp
    tok_rows, width_local = residual_hbm.shape
    kv_width = key_hbm.shape[1]
    segments = tok_rows // SEG
    hops = hops_of(tok_rows)
    pieces = pieces_of(tok_rows)
    halves = part_own.shape[0]
    blocks = [(range(segments - 1, 0, -1), SEG, tok_rows - SEG), (range(1), 0, SEG)]

    barrier = pltpu.get_barrier_semaphore()
    expected = jnp.int32(1)
    for distance in hops:
        expected = expected + (me + distance < n_sp).astype(jnp.int32)

        @pl.when(me >= distance)
        def _():
            pl.semaphore_signal(
                barrier, inc=1, device_id={"sp": me - distance}, device_id_type=MESH
            )

    pl.semaphore_signal(barrier, inc=1, device_id={"tp": other}, device_id_type=MESH)

    own = pl.ds(SPAN, tok_rows)
    transfers = dict(
        key=(key_hbm, kv_one.at[own, pl.ds(0, kv_width)]),
        value=(value_hbm, kv_one.at[own, pl.ds(kv_width, kv_width)]),
        docs=(docs_hbm, docs),
        bias_one=(bias_one_hbm, bias_one),
        query=(query_hbm, query_one),
        residual=(residual_hbm, residual_full.at[my_tp]),
        bias_two=(bias_two_hbm, bias_two),
        out_one=(out_one_hbm, w_out_one),
        gain=(gain_hbm, gain),
        key_w=(key_w_hbm, w_kv.at[:, pl.ds(0, kv_width)]),
        value_w=(value_w_hbm, w_kv.at[:, pl.ds(kv_width, kv_width)]),
        query_w=(query_w_hbm, w_query),
        out_two=(out_two_hbm, w_out_two),
    )
    loads = {
        name: pltpu.make_async_copy(src, dst, load_sem.at[index])
        for index, (name, (src, dst)) in enumerate(transfers.items())
    }
    for load in loads.values():
        load.start()

    slot = iter(range(send_sem.shape[0]))

    def remote(src, dst, target):
        index = next(slot)
        return pltpu.make_async_remote_copy(
            src_ref=src,
            dst_ref=dst,
            send_sem=send_sem.at[index],
            recv_sem=recv_sem.at[index],
            device_id=target,
            device_id_type=MESH,
        )

    def ahead(distance):
        return {"sp": lax.rem(me + distance, n_sp)}

    def start_sent(distance, copies):
        @pl.when(me + distance < n_sp)
        def _():
            for copy in copies:
                copy.start()

    def wait_arrived(distance, copies):
        @pl.when(me >= distance)
        def _():
            for copy in copies:
                copy.wait_recv()

    def wait_sent(distance, copies):
        @pl.when(me + distance < n_sp)
        def _():
            for copy in copies:
                copy.wait_send()

    for distance, _, needed, landing in pieces:

        @pl.when(me < distance)
        def _():
            empty = jnp.zeros((needed, 2 * kv_width), jnp.bfloat16)
            kv_one[landing : landing + needed] = empty
            kv_two[landing : landing + needed] = empty

    for distance in hops:

        @pl.when(me < distance)
        def _():
            docs_prior[distance - 1] = jnp.full((1, tok_rows), -1, jnp.int32)

    eye = lax.broadcasted_iota(jnp.int32, (SEG, SEG), 0) == lax.broadcasted_iota(
        jnp.int32, (SEG, SEG), 1
    )

    def put_column(numbers, place):
        picked = jnp.where(eye, numbers.astype(jnp.float32), 0.0)
        docs_col[place : place + SEG] = jnp.broadcast_to(
            jnp.sum(picked, axis=1, keepdims=True), (SEG, LANES)
        )

    def put_mask(segment, low, high):
        mine = docs[:, segment * SEG : (segment + 1) * SEG].astype(jnp.float32)
        mine = jnp.concatenate([mine, mine], axis=1)
        same = docs_col[low:high] == mine
        first = segment * SEG
        mask[segment, low - first : high - first] = jnp.where(same, 0.0, HIDDEN)

    shared = (mask, mixed, padded, turned, scores, weights, stats, blend)
    one = Attention(query_one, kv_one, table_one, *shared)
    two = Attention(query_two, kv_two, table_two, *shared)
    newest_first = range(segments - 1, -1, -1)
    two.cut = pieces[0][3]

    for name in ("key", "value", "docs"):
        loads[name].wait()
    pl.semaphore_wait(barrier, expected)

    def halo_copy(kv, piece):
        distance, row, needed, landing = piece
        return remote(
            kv.at[pl.ds(SPAN + row, needed)], kv.at[pl.ds(landing, needed)], ahead(distance)
        )

    docs_copies = [
        (distance, [remote(docs, docs_prior.at[distance - 1], ahead(distance))])
        for distance in hops
    ]
    first_copies = [(piece[0], [halo_copy(kv_one, piece)]) for piece in pieces]
    for distance, copies in docs_copies + first_copies:
        start_sent(distance, copies)
    loads["residual"].wait()
    residual_copy = remote(residual_full.at[my_tp], residual_full.at[my_tp], {"tp": other})
    residual_copy.start()

    loads["query"].wait()
    for row in range(SPAN, SPAN + tok_rows, SEG):
        one.turn_values(row)
    for segment in newest_first:
        one.pad_queries(segment)
    for block in range(0, tok_rows, SEG):
        put_column(docs[:, block : block + SEG], SPAN + block)
    for segment in range(segments):
        put_mask(segment, *one.bounds(segment, "local"))

    loads["bias_one"].wait()
    build_bias(bias_one, table_one)
    one.run(newest_first, "local")

    for distance, copies in docs_copies:
        wait_arrived(distance, copies)
    for distance, row, needed, landing in pieces:
        for block in range(0, needed, SEG):
            put_column(
                docs_prior[distance - 1, :, row + block : row + block + SEG], landing + block
            )
    for segment in range(segments):
        put_mask(segment, *one.bounds(segment, "halo"))
    residual_copy.wait_recv()
    loads["out_one"].wait()

    def arrival(segment, waiting, which):
        members = list(zip(pieces, waiting))[which]

        def wait():
            for _, (distance, copies) in members:
                wait_arrived(distance, copies)

        rows = [
            row
            for (_, _, needed, landing), _ in members
            for row in range(landing, landing + needed, SEG)
        ]
        return segment, wait, rows

    newest, older = newest_first[0], newest_first[1]

    part_copies = []
    for _, start, count in blocks:
        rows = pl.ds(start, count)
        part_copies.append(
            [
                remote(part_own.at[half, rows], part_in.at[half, rows], {"tp": other})
                for half in range(halves)
            ]
        )

    def project_one(block, beside=()):
        _, start, count = blocks[block]
        rows = slice(start, start + count)
        parts = [
            jnp.dot(
                mixed[rows],
                w_out_one[:, half * width_local : (half + 1) * width_local],
                preferred_element_type=jnp.float32,
            ).astype(jnp.bfloat16)
            for half in range(halves)
        ]
        for step in beside:
            step()
        for half, part in enumerate(parts):
            part_own[half, rows] = part
        for copy in part_copies[block]:
            copy.start()
        for half, part in enumerate(parts):
            base[half, rows] = residual_full[half, rows].astype(jnp.float32) + part.astype(
                jnp.float32
            )

    second_copies = [(piece[0], [halo_copy(kv_two, piece)]) for piece in pieces]

    def keys_two(block):
        _, start, count = blocks[block]
        rows = slice(start, start + count)
        squares = jnp.zeros((count, LANES), jnp.float32)
        for half in range(halves):
            part_copies[block][half].wait_recv()
            new = base[half, rows] + part_in[half, rows].astype(jnp.float32)
            new = new.astype(jnp.bfloat16)
            layer[half, rows] = new
            new = new.astype(jnp.float32)
            columns = slice(half * width_local, (half + 1) * width_local)
            scaled[rows, columns] = (new * gain[:, columns]).astype(jnp.bfloat16)
            for lane in range(0, width_local, LANES):
                squares = squares + new[:, lane : lane + LANES] * new[:, lane : lane + LANES]
        scale = lax.rsqrt(
            jnp.sum(squares, axis=1, keepdims=True) / (halves * width_local) + eps
        )
        scales[rows] = jnp.broadcast_to(scale, (count, LANES))
        kv_two[SPAN + start : SPAN + start + count] = (
            jnp.dot(scaled[rows], w_kv[...], preferred_element_type=jnp.float32) * scale
        ).astype(jnp.bfloat16)
        for piece, copies in zip(pieces, second_copies):
            if start <= piece[1] < start + count:
                start_sent(*copies)

    for name in ("gain", "key_w", "value_w", "query_w"):
        loads[name].wait()
    plan = one.steps(
        newest_first,
        "halo",
        (
            arrival(newest, first_copies, slice(0, 1)),
            arrival(older, first_copies, slice(1, None)),
        ),
    )
    tail = 2 * one.groups
    for step in plan[:-tail]:
        step()
    weighs, gathers = plan[-tail::2], plan[1 - tail :: 2]
    project_one(0, weighs)

    @pl.when(my_tp == 0)
    def _():
        keys_two(0)

    for step in gathers:
        step()
    project_one(1)
    loads["bias_two"].wait()

    @pl.when(my_tp == 1)
    def _():
        build_bias(bias_two, table_two)
        keys_two(0)

    keys_two(1)
    query_two[...] = (
        jnp.dot(scaled[...], w_query[...], preferred_element_type=jnp.float32) * scales[:, 0:1]
    ).astype(jnp.bfloat16)

    @pl.when(my_tp == 0)
    def _():
        build_bias(bias_two, table_two)

    for row in range(SPAN, SPAN + tok_rows, SEG):
        two.turn_values(row)
    for segment in newest_first:
        two.pad_queries(segment)
    two.run(newest_first, "local")
    for copies in part_copies:
        for copy in copies:
            copy.wait_send()

    loads["out_two"].wait()
    theirs = pl.ds(pl.multiple_of(other * width_local, width_local), width_local)
    ours = pl.ds(pl.multiple_of(my_tp * width_local, width_local), width_local)
    two.run(newest_first, "near", (arrival(newest, second_copies, slice(0, 1)),))
    two.run(
        [segment for segment in newest_first if segment * SEG < two.cut],
        "rest",
        (arrival(older, second_copies, slice(1, None)),),
    )
    part_own[0] = jnp.dot(
        mixed[...], w_out_two[:, theirs], preferred_element_type=jnp.float32
    ).astype(jnp.bfloat16)
    quarter = width_local // 2
    last_copies = []
    for part in range(2):
        place = pl.ds(part * quarter, quarter)
        last_copies.append(remote(part_own.at[0, :, place], last_in.at[:, place], {"tp": other}))
        last_copies[-1].start()
    part_own[1] = jnp.dot(
        mixed[...], w_out_two[:, ours], preferred_element_type=jnp.float32
    ).astype(jnp.bfloat16)
    branch = part_own[1].astype(jnp.float32)
    branch = branch + layer[my_tp].astype(jnp.float32)
    for part, copy in enumerate(last_copies):
        columns = slice(part * quarter, (part + 1) * quarter)
        copy.wait_recv()
        result_ref[:, columns] = (
            branch[:, columns] + last_in[:, columns].astype(jnp.float32)
        ).astype(jnp.bfloat16)

    residual_copy.wait_send()
    for distance, copies in docs_copies + first_copies + second_copies:
        wait_sent(distance, copies)
    for copy in last_copies:
        copy.wait_send()


def body(
    residual,
    query_first,
    key_first,
    value_first,
    documents,
    bias_first,
    out_first,
    norm_gain,
    query_w,
    key_w,
    value_w,
    bias_second,
    out_second,
):
    n_sp = lax.axis_size("sp")
    tok_rows, width_local = residual.shape
    query_width = query_first.shape[1]
    kv_width = key_first.shape[1]
    kv_local = kv_width // HEAD_SIZE
    group_width = query_width // kv_local
    halves = out_first.shape[1] // width_local
    hops = len(hops_of(tok_rows))
    units = tok_rows // SEG * kv_local
    n_sems = hops + 2 * len(pieces_of(tok_rows)) + 1 + 2 * halves + 2
    vmem = pl.BlockSpec(memory_space=pltpu.VMEM)
    hbm = pl.BlockSpec(memory_space=pl.ANY)
    bf16 = jnp.bfloat16
    f32 = jnp.float32
    return pl.pallas_call(
        functools.partial(kernel, n_sp),
        name="two_layers",
        out_shape=pltpu.VMEM((tok_rows, width_local), bf16),
        in_specs=[hbm] * 13,
        out_specs=vmem,
        scratch_shapes=[
            pltpu.VMEM(out_first.shape, bf16),
            pltpu.VMEM(query_w.shape, bf16),
            pltpu.VMEM((key_w.shape[0], 2 * kv_width), bf16),
            pltpu.VMEM(out_second.shape, bf16),
            pltpu.VMEM((SPAN + tok_rows, 2 * kv_width), bf16),
            pltpu.VMEM((SPAN + tok_rows, 2 * kv_width), bf16),
            pltpu.VMEM((SPAN + tok_rows, LANES), f32),
            pltpu.VMEM((tok_rows // SEG, BAND, LANES), f32),
            pltpu.VMEM((kv_local, BAND, group_width), f32),
            pltpu.VMEM((kv_local, BAND, group_width), f32),
            pltpu.VMEM((tok_rows, query_width), bf16),
            pltpu.VMEM((tok_rows, query_width), bf16),
            pltpu.VMEM((tok_rows, query_width), bf16),
            pltpu.VMEM((halves, tok_rows, width_local), bf16),
            pltpu.VMEM((halves, tok_rows, width_local), bf16),
            pltpu.VMEM((halves, tok_rows, width_local), bf16),
            pltpu.VMEM((tok_rows, width_local), bf16),
            pltpu.VMEM((halves, tok_rows, width_local), bf16),
            pltpu.VMEM((halves, tok_rows, width_local), f32),
            pltpu.VMEM((tok_rows, halves * width_local), bf16),
            pltpu.VMEM((tok_rows, LANES), f32),
            pltpu.VMEM((units, group_width, LANES), bf16),
            pltpu.VMEM((2, kv_width, pl.cdiv(SPAN + tok_rows, LANES) * LANES), bf16),
            pltpu.VMEM((units, BAND, group_width), f32),
            pltpu.VMEM((units, BAND, group_width), bf16),
            pltpu.VMEM((units, HEAD_SIZE, group_width), f32),
            pltpu.VMEM(bias_first.shape, f32),
            pltpu.VMEM(bias_second.shape, f32),
            pltpu.VMEM((1, norm_gain.shape[0]), f32),
            pltpu.VMEM((1, tok_rows), jnp.int32),
            pltpu.VMEM((hops, 1, tok_rows), jnp.int32),
            pltpu.VMEM((units, 2, group_width), f32),
            pltpu.SemaphoreType.DMA((n_sems,)),
            pltpu.SemaphoreType.DMA((n_sems,)),
            pltpu.SemaphoreType.DMA((13,)),
        ],
        compiler_params=pltpu.CompilerParams(collective_id=0, has_side_effects=True),
    )(
        residual,
        query_first,
        key_first,
        value_first,
        documents.reshape(1, tok_rows),
        bias_first,
        out_first,
        norm_gain.reshape(1, -1),
        query_w,
        key_w,
        value_w,
        bias_second,
        out_second,
    )


def solution(mesh):
    placed = (
        P("sp", "tp"),
        P("sp", "tp"),
        P("sp", "tp"),
        P("sp", "tp"),
        P("sp"),
        P("tp", None),
        P("tp", None),
        P(),
        P(None, "tp"),
        P(None, "tp"),
        P(None, "tp"),
        P("tp", None),
        P("tp", None),
    )
    return jax.shard_map(body, mesh=mesh, in_specs=placed, out_specs=P("sp", "tp"), check_vma=False)
```

```python
import functools

import jax
import jax.numpy as jnp
from jax import lax
from jax.experimental import pallas as pl
from jax.experimental.pallas import tpu as pltpu
from jax.sharding import PartitionSpec as P

HEAD_SIZE = 64
SEG = 64
PAST = 4
REL_CLIP = 256
SPAN = PAST * SEG
BAND = SPAN + SEG
LANES = 128
LOG2E = 1.4426950408889634
HIDDEN = -1e30
MESH = pl.DeviceIdType.MESH


eps = 1e-06


def hops_of(tok_rows):
    return range(1, (SPAN + tok_rows - 1) // tok_rows + 1)


def pieces_of(tok_rows):
    pieces = []
    for distance in hops_of(tok_rows):
        top = SPAN - (distance - 1) * tok_rows
        bottom = max(0, top - tok_rows)
        cuts = [cut for cut in range(SEG, tok_rows, SEG) if bottom < cut < top]
        edges = [bottom] + cuts + [top]
        for low, high in reversed(list(zip(edges[:-1], edges[1:]))):
            pieces.append((distance, tok_rows - (top - low), high - low, low))
    return pieces


def build_bias(table_ref, bias_ref):
    heads_local = table_ref.shape[0]
    group_size = bias_ref.shape[2] // SEG
    lane = lax.broadcasted_iota(jnp.int32, (SEG, LANES), 1)
    low = lane < SEG
    last = REL_CLIP + SPAN

    def tile(head, index):
        if index == 0:
            return jnp.broadcast_to(table_ref[head : head + 1, last : last + 1], (SEG, LANES))
        first = last - index * LANES
        return jnp.broadcast_to(table_ref[head : head + 1, first : first + LANES], (SEG, LANES))

    def piece(head, block, base):
        back = block // 2
        if block % 2 == 0:
            source = jnp.where(low, tile(head, back), tile(head, back + 1))
            shift = base
        else:
            source = tile(head, back + 1)
            shift = (base + SEG) % LANES
        return pltpu.roll(source, shift, 1, stride=1, stride_axis=0)

    for head in range(0, heads_local, 2):
        for block in range(PAST + 1):
            pair = jnp.where(low, piece(head, block, 0), piece(head + 1, block, SEG)) * LOG2E
            group, inner = head // group_size, head % group_size
            bias_ref[group, block * SEG : (block + 1) * SEG, inner * SEG : (inner + 2) * SEG] = pair


class Attention:
    def __init__(self, query, kv, bias, mask, mixed, padded, turned, scores, weights, stats, blend):
        self.query, self.kv, self.bias, self.mask, self.mixed = query, kv, bias, mask, mixed
        self.padded, self.turned, self.scores, self.weights = padded, turned, scores, weights
        self.stats, self.blend = stats, blend
        self.cut = SPAN
        self.groups = bias.shape[0]
        self.group_size = bias.shape[2] // SEG
        self.kv_width = self.groups * HEAD_SIZE
        self.state = {}

    def unit(self, segment, group):
        return segment * self.groups + group

    def pad_queries(self, segment):
        lane = lax.broadcasted_iota(jnp.int32, (SEG, LANES), 1)
        rows = slice(segment * SEG, (segment + 1) * SEG)
        for group in range(self.groups):
            keep = (lane >= group * HEAD_SIZE) & (lane < (group + 1) * HEAD_SIZE)
            for inner in range(self.group_size):
                head = group * self.group_size + inner
                column = head * HEAD_SIZE // LANES * LANES
                block = self.query[rows, column : column + LANES]
                if head % 2 != group % 2:
                    block = jnp.concatenate([block[:, HEAD_SIZE:], block[:, :HEAD_SIZE]], axis=1)
                self.padded[self.unit(segment, group), inner * SEG : (inner + 1) * SEG] = jnp.where(
                    keep, block, jnp.zeros_like(block)
                )

    def turn_values(self, row):
        block = jnp.transpose(self.kv[row : row + SEG, self.kv_width : 2 * self.kv_width])
        self.turned[0, :, row : row + SEG] = block
        if row >= SEG:
            self.turned[1, :, row - SEG : row] = block

    def bounds(self, segment, phase):
        first = segment * SEG
        cut = max(first, self.cut)
        return {
            "local": (max(first, SPAN), first + BAND),
            "halo": (first, SPAN),
            "near": (cut, SPAN),
            "rest": (first, cut),
        }[phase]

    def score(self, segment, group, phase):
        low, high = self.bounds(segment, phase)
        unit = self.unit(segment, group)
        band = slice(low - segment * SEG, high - segment * SEG)
        scores = lax.dot_general(
            self.kv[low:high, : self.kv_width],
            self.padded[unit],
            (((1,), (1,)), ((), ())),
            preferred_element_type=jnp.float32,
        )
        mask = self.mask[segment, band]
        mask = jnp.concatenate([mask] * (self.group_size * SEG // LANES), axis=1)
        scores = scores * (HEAD_SIZE ** (-0.5) * LOG2E) + self.bias[group, band] + mask
        self.scores[unit, band] = scores
        largest = jnp.max(scores, axis=0, keepdims=True)
        if phase != "local":
            largest = jnp.maximum(largest, self.stats[unit, 0:1])
        self.state[unit] = (largest,)

    def weigh(self, segment, group, phase):
        low, high = self.bounds(segment, phase)
        unit = self.unit(segment, group)
        band = slice(low - segment * SEG, high - segment * SEG)
        (largest,) = self.state[unit]
        weight = jnp.exp2(self.scores[unit, band] - largest)
        self.weights[unit, band] = weight.astype(jnp.bfloat16)
        total = jnp.sum(weight, axis=0, keepdims=True)
        fade = None
        if phase != "local":
            fade = jnp.exp2(self.stats[unit, 0:1] - largest)
            total = total + self.stats[unit, 1:2] * fade
        if self.ends(segment, phase):
            self.state[unit] = (fade, 1.0 / total)
        else:
            self.stats[unit, 0:1] = largest
            self.stats[unit, 1:2] = total
            self.state[unit] = (fade,)

    def ends(self, segment, phase):
        return phase != "local" and self.bounds(segment, phase)[0] == segment * SEG

    def gather(self, segment, group, phase):
        low, high = self.bounds(segment, phase)
        unit = self.unit(segment, group)
        band = slice(low - segment * SEG, high - segment * SEG)
        odd = low // SEG % 2
        blended = lax.dot_general(
            self.turned[
                odd,
                group * HEAD_SIZE : (group + 1) * HEAD_SIZE,
                low - odd * SEG : high - odd * SEG,
            ],
            self.weights[unit, band],
            (((1,), (0,)), ((), ())),
            preferred_element_type=jnp.float32,
        )
        if phase != "local":
            blended = blended + self.blend[unit] * self.state[unit][0]
        if not self.ends(segment, phase):
            self.blend[unit] = blended
            return
        blended = (blended * self.state[unit][1]).astype(jnp.bfloat16)
        rows = slice(segment * SEG, (segment + 1) * SEG)
        for pair in range(self.group_size // 2):
            turned = jnp.transpose(blended[:, pair * LANES : (pair + 1) * LANES])
            both = jnp.concatenate([turned[:SEG], turned[SEG:]], axis=1)
            column = (group * self.group_size + 2 * pair) * HEAD_SIZE
            self.mixed[rows, column : column + LANES] = both

    def steps(self, segments, phase, arrivals=()):
        units = [(segment, group) for segment in segments for group in range(self.groups)]
        waits = {segment: wait for segment, wait, _ in arrivals}
        turns = {segment: rows for segment, _, rows in arrivals}

        def score(unit):
            segment, group = unit
            if group == 0 and segment in waits:
                waits[segment]()
            self.score(segment, group, phase)
            if group == self.groups - 1 and segment in turns:
                for row in turns[segment]:
                    self.turn_values(row)

        def weigh(unit):
            self.weigh(*unit, phase)

        def gather(unit):
            self.gather(*unit, phase)

        plan = [(score, units[0])]
        for index, unit in enumerate(units):
            if index + 1 < len(units):
                plan.append((score, units[index + 1]))
            if index > 0:
                plan.append((gather, units[index - 1]))
            plan.append((weigh, unit))
        plan.append((gather, units[-1]))
        return [functools.partial(step, unit) for step, unit in plan]

    def run(self, segments, phase, arrivals=()):
        for step in self.steps(segments, phase, arrivals):
            step()


def kernel(
    n_sp,
    residual_hbm,
    query_hbm,
    key_hbm,
    value_hbm,
    docs_hbm,
    bias_one_hbm,
    out_one_hbm,
    gain_hbm,
    query_w_hbm,
    key_w_hbm,
    value_w_hbm,
    bias_two_hbm,
    out_two_hbm,
    result_ref,
    w_out_one,
    w_query,
    w_kv,
    w_out_two,
    kv_one,
    kv_two,
    docs_col,
    mask,
    table_one,
    table_two,
    mixed,
    query_one,
    query_two,
    residual_full,
    part_own,
    part_in,
    last_in,
    layer,
    base,
    scaled,
    scales,
    padded,
    turned,
    scores,
    weights,
    blend,
    bias_one,
    bias_two,
    gain,
    docs,
    docs_prior,
    stats,
    send_sem,
    recv_sem,
    load_sem,
):
    me = lax.axis_index("sp")
    my_tp = lax.axis_index("tp")
    other = 1 - my_tp
    tok_rows, width_local = residual_hbm.shape
    kv_width = key_hbm.shape[1]
    segments = tok_rows // SEG
    hops = hops_of(tok_rows)
    pieces = pieces_of(tok_rows)
    halves = part_own.shape[0]
    blocks = [(range(segments - 1, 0, -1), SEG, tok_rows - SEG), (range(1), 0, SEG)]

    barrier = pltpu.get_barrier_semaphore()
    expected = jnp.int32(1)
    for distance in hops:
        expected = expected + (me + distance < n_sp).astype(jnp.int32)

        @pl.when(me >= distance)
        def _():
            pl.semaphore_signal(
                barrier, inc=1, device_id={"sp": me - distance}, device_id_type=MESH
            )

    pl.semaphore_signal(barrier, inc=1, device_id={"tp": other}, device_id_type=MESH)

    own = pl.ds(SPAN, tok_rows)
    transfers = dict(
        key=(key_hbm, kv_one.at[own, pl.ds(0, kv_width)]),
        value=(value_hbm, kv_one.at[own, pl.ds(kv_width, kv_width)]),
        docs=(docs_hbm, docs),
        bias_one=(bias_one_hbm, bias_one),
        query=(query_hbm, query_one),
        residual=(residual_hbm, residual_full.at[my_tp]),
        bias_two=(bias_two_hbm, bias_two),
        out_one=(out_one_hbm, w_out_one),
        gain=(gain_hbm, gain),
        key_w=(key_w_hbm, w_kv.at[:, pl.ds(0, kv_width)]),
        value_w=(value_w_hbm, w_kv.at[:, pl.ds(kv_width, kv_width)]),
        query_w=(query_w_hbm, w_query),
        out_two=(out_two_hbm, w_out_two),
    )
    loads = {
        name: pltpu.make_async_copy(src, dst, load_sem.at[index])
        for index, (name, (src, dst)) in enumerate(transfers.items())
    }
    for load in loads.values():
        load.start()

    slot = iter(range(send_sem.shape[0]))

    def remote(src, dst, target):
        index = next(slot)
        return pltpu.make_async_remote_copy(
            src_ref=src,
            dst_ref=dst,
            send_sem=send_sem.at[index],
            recv_sem=recv_sem.at[index],
            device_id=target,
            device_id_type=MESH,
        )

    def ahead(distance):
        return {"sp": lax.rem(me + distance, n_sp)}

    def start_sent(distance, copies):
        @pl.when(me + distance < n_sp)
        def _():
            for copy in copies:
                copy.start()

    def wait_arrived(distance, copies):
        @pl.when(me >= distance)
        def _():
            for copy in copies:
                copy.wait_recv()

    def wait_sent(distance, copies):
        @pl.when(me + distance < n_sp)
        def _():
            for copy in copies:
                copy.wait_send()

    for distance, _, needed, landing in pieces:

        @pl.when(me < distance)
        def _():
            empty = jnp.zeros((needed, 2 * kv_width), jnp.bfloat16)
            kv_one[landing : landing + needed] = empty
            kv_two[landing : landing + needed] = empty

    for distance in hops:

        @pl.when(me < distance)
        def _():
            docs_prior[distance - 1] = jnp.full((1, tok_rows), -1, jnp.int32)

    eye = lax.broadcasted_iota(jnp.int32, (SEG, SEG), 0) == lax.broadcasted_iota(
        jnp.int32, (SEG, SEG), 1
    )

    def put_column(numbers, place):
        picked = jnp.where(eye, numbers.astype(jnp.float32), 0.0)
        docs_col[place : place + SEG] = jnp.broadcast_to(
            jnp.sum(picked, axis=1, keepdims=True), (SEG, LANES)
        )

    def put_mask(segment, low, high):
        mine = docs[:, segment * SEG : (segment + 1) * SEG].astype(jnp.float32)
        mine = jnp.concatenate([mine, mine], axis=1)
        same = docs_col[low:high] == mine
        first = segment * SEG
        mask[segment, low - first : high - first] = jnp.where(same, 0.0, HIDDEN)

    shared = (mask, mixed, padded, turned, scores, weights, stats, blend)
    one = Attention(query_one, kv_one, table_one, *shared)
    two = Attention(query_two, kv_two, table_two, *shared)
    newest_first = range(segments - 1, -1, -1)
    two.cut = pieces[0][3]

    for name in ("key", "value", "docs"):
        loads[name].wait()
    pl.semaphore_wait(barrier, expected)

    def halo_copy(kv, piece):
        distance, row, needed, landing = piece
        return remote(
            kv.at[pl.ds(SPAN + row, needed)], kv.at[pl.ds(landing, needed)], ahead(distance)
        )

    docs_copies = [
        (distance, [remote(docs, docs_prior.at[distance - 1], ahead(distance))])
        for distance in hops
    ]
    first_copies = [(piece[0], [halo_copy(kv_one, piece)]) for piece in pieces]
    for distance, copies in docs_copies + first_copies:
        start_sent(distance, copies)
    loads["residual"].wait()
    residual_copy = remote(residual_full.at[my_tp], residual_full.at[my_tp], {"tp": other})
    residual_copy.start()

    loads["query"].wait()
    for row in range(SPAN, SPAN + tok_rows, SEG):
        one.turn_values(row)
    for segment in newest_first:
        one.pad_queries(segment)
    for block in range(0, tok_rows, SEG):
        put_column(docs[:, block : block + SEG], SPAN + block)
    for segment in range(segments):
        put_mask(segment, *one.bounds(segment, "local"))

    loads["bias_one"].wait()
    build_bias(bias_one, table_one)
    one.run(newest_first, "local")

    for distance, copies in docs_copies:
        wait_arrived(distance, copies)
    for distance, row, needed, landing in pieces:
        for block in range(0, needed, SEG):
            put_column(
                docs_prior[distance - 1, :, row + block : row + block + SEG], landing + block
            )
    for segment in range(segments):
        put_mask(segment, *one.bounds(segment, "halo"))
    residual_copy.wait_recv()
    loads["out_one"].wait()

    def arrival(segment, waiting, which):
        members = list(zip(pieces, waiting))[which]

        def wait():
            for _, (distance, copies) in members:
                wait_arrived(distance, copies)

        rows = [
            row
            for (_, _, needed, landing), _ in members
            for row in range(landing, landing + needed, SEG)
        ]
        return segment, wait, rows

    newest, older = newest_first[0], newest_first[1]

    part_copies = []
    for _, start, count in blocks:
        rows = pl.ds(start, count)
        part_copies.append(
            [
                remote(part_own.at[half, rows], part_in.at[half, rows], {"tp": other})
                for half in range(halves)
            ]
        )

    def project_one(block, beside=()):
        _, start, count = blocks[block]
        rows = slice(start, start + count)
        parts = [
            jnp.dot(
                mixed[rows],
                w_out_one[:, half * width_local : (half + 1) * width_local],
                preferred_element_type=jnp.float32,
            ).astype(jnp.bfloat16)
            for half in range(halves)
        ]
        for step in beside:
            step()
        for half, part in enumerate(parts):
            part_own[half, rows] = part
        for copy in part_copies[block]:
            copy.start()
        for half, part in enumerate(parts):
            base[half, rows] = residual_full[half, rows].astype(jnp.float32) + part.astype(
                jnp.float32
            )

    second_copies = [(piece[0], [halo_copy(kv_two, piece)]) for piece in pieces]

    def keys_two(block):
        _, start, count = blocks[block]
        rows = slice(start, start + count)
        squares = jnp.zeros((count, LANES), jnp.float32)
        for copy in part_copies[block]:
            copy.wait_recv()
        for half in range(halves):
            new = base[half, rows] + part_in[half, rows].astype(jnp.float32)
            new = new.astype(jnp.bfloat16)
            layer[half, rows] = new
            new = new.astype(jnp.float32)
            columns = slice(half * width_local, (half + 1) * width_local)
            scaled[rows, columns] = (new * gain[:, columns]).astype(jnp.bfloat16)
            for lane in range(0, width_local, LANES):
                squares = squares + new[:, lane : lane + LANES] * new[:, lane : lane + LANES]
        scale = lax.rsqrt(
            jnp.sum(squares, axis=1, keepdims=True) / (halves * width_local) + eps
        )
        scales[rows] = jnp.broadcast_to(scale, (count, LANES))
        kv_two[SPAN + start : SPAN + start + count] = (
            jnp.dot(scaled[rows], w_kv[...], preferred_element_type=jnp.float32) * scale
        ).astype(jnp.bfloat16)
        for piece, copies in zip(pieces, second_copies):
            if start <= piece[1] < start + count:
                start_sent(*copies)

    for name in ("gain", "key_w", "value_w", "query_w"):
        loads[name].wait()
    for step in one.steps(
        newest_first[:-1],
        "halo",
        (
            arrival(newest, first_copies, slice(0, 1)),
            arrival(older, first_copies, slice(1, 2)),
        ),
    ):
        step()
    project_one(0)
    plan = one.steps(
        newest_first[-1:], "halo", (arrival(newest_first[-1], first_copies, slice(2, None)),)
    )

    @pl.when(my_tp == 0)
    def _():
        keys_two(0)

    for step in plan:
        step()
    project_one(1)
    loads["bias_two"].wait()

    @pl.when(my_tp == 1)
    def _():
        build_bias(bias_two, table_two)
        keys_two(0)

    keys_two(1)
    query_two[...] = (
        jnp.dot(scaled[...], w_query[...], preferred_element_type=jnp.float32) * scales[:, 0:1]
    ).astype(jnp.bfloat16)

    @pl.when(my_tp == 0)
    def _():
        build_bias(bias_two, table_two)

    for row in range(SPAN, SPAN + tok_rows, SEG):
        two.turn_values(row)
    for segment in newest_first:
        two.pad_queries(segment)
    two.run(newest_first, "local")
    for copies in part_copies:
        for copy in copies:
            copy.wait_send()

    loads["out_two"].wait()
    theirs = pl.ds(pl.multiple_of(other * width_local, width_local), width_local)
    ours = pl.ds(pl.multiple_of(my_tp * width_local, width_local), width_local)
    two.run(newest_first, "near", (arrival(newest, second_copies, slice(0, 1)),))
    two.run(
        [segment for segment in newest_first if segment * SEG < two.cut],
        "rest",
        (arrival(older, second_copies, slice(1, None)),),
    )
    part_own[0] = jnp.dot(
        mixed[...], w_out_two[:, theirs], preferred_element_type=jnp.float32
    ).astype(jnp.bfloat16)
    quarter = width_local // 2
    last_copies = []
    for part in range(2):
        place = pl.ds(part * quarter, quarter)
        last_copies.append(remote(part_own.at[0, :, place], last_in.at[:, place], {"tp": other}))
        last_copies[-1].start()
    part_own[1] = jnp.dot(
        mixed[...], w_out_two[:, ours], preferred_element_type=jnp.float32
    ).astype(jnp.bfloat16)
    branch = part_own[1].astype(jnp.float32)
    branch = branch + layer[my_tp].astype(jnp.float32)
    for part, copy in enumerate(last_copies):
        columns = slice(part * quarter, (part + 1) * quarter)
        copy.wait_recv()
        result_ref[:, columns] = (
            branch[:, columns] + last_in[:, columns].astype(jnp.float32)
        ).astype(jnp.bfloat16)

    residual_copy.wait_send()
    for distance, copies in docs_copies + first_copies + second_copies:
        wait_sent(distance, copies)
    for copy in last_copies:
        copy.wait_send()


def body(
    residual,
    query_first,
    key_first,
    value_first,
    documents,
    bias_first,
    out_first,
    norm_gain,
    query_w,
    key_w,
    value_w,
    bias_second,
    out_second,
):
    n_sp = lax.axis_size("sp")
    tok_rows, width_local = residual.shape
    query_width = query_first.shape[1]
    kv_width = key_first.shape[1]
    kv_local = kv_width // HEAD_SIZE
    group_width = query_width // kv_local
    halves = out_first.shape[1] // width_local
    hops = len(hops_of(tok_rows))
    units = tok_rows // SEG * kv_local
    n_sems = hops + 2 * len(pieces_of(tok_rows)) + 1 + 2 * halves + 2
    vmem = pl.BlockSpec(memory_space=pltpu.VMEM)
    hbm = pl.BlockSpec(memory_space=pl.ANY)
    bf16 = jnp.bfloat16
    f32 = jnp.float32
    return pl.pallas_call(
        functools.partial(kernel, n_sp),
        name="two_layers",
        out_shape=pltpu.VMEM((tok_rows, width_local), bf16),
        in_specs=[hbm] * 13,
        out_specs=vmem,
        scratch_shapes=[
            pltpu.VMEM(out_first.shape, bf16),
            pltpu.VMEM(query_w.shape, bf16),
            pltpu.VMEM((key_w.shape[0], 2 * kv_width), bf16),
            pltpu.VMEM(out_second.shape, bf16),
            pltpu.VMEM((SPAN + tok_rows, 2 * kv_width), bf16),
            pltpu.VMEM((SPAN + tok_rows, 2 * kv_width), bf16),
            pltpu.VMEM((SPAN + tok_rows, LANES), f32),
            pltpu.VMEM((tok_rows // SEG, BAND, LANES), f32),
            pltpu.VMEM((kv_local, BAND, group_width), f32),
            pltpu.VMEM((kv_local, BAND, group_width), f32),
            pltpu.VMEM((tok_rows, query_width), bf16),
            pltpu.VMEM((tok_rows, query_width), bf16),
            pltpu.VMEM((tok_rows, query_width), bf16),
            pltpu.VMEM((halves, tok_rows, width_local), bf16),
            pltpu.VMEM((halves, tok_rows, width_local), bf16),
            pltpu.VMEM((halves, tok_rows, width_local), bf16),
            pltpu.VMEM((tok_rows, width_local), bf16),
            pltpu.VMEM((halves, tok_rows, width_local), bf16),
            pltpu.VMEM((halves, tok_rows, width_local), f32),
            pltpu.VMEM((tok_rows, halves * width_local), bf16),
            pltpu.VMEM((tok_rows, LANES), f32),
            pltpu.VMEM((units, group_width, LANES), bf16),
            pltpu.VMEM((2, kv_width, pl.cdiv(SPAN + tok_rows, LANES) * LANES), bf16),
            pltpu.VMEM((units, BAND, group_width), f32),
            pltpu.VMEM((units, BAND, group_width), bf16),
            pltpu.VMEM((units, HEAD_SIZE, group_width), f32),
            pltpu.VMEM(bias_first.shape, f32),
            pltpu.VMEM(bias_second.shape, f32),
            pltpu.VMEM((1, norm_gain.shape[0]), f32),
            pltpu.VMEM((1, tok_rows), jnp.int32),
            pltpu.VMEM((hops, 1, tok_rows), jnp.int32),
            pltpu.VMEM((units, 2, group_width), f32),
            pltpu.SemaphoreType.DMA((n_sems,)),
            pltpu.SemaphoreType.DMA((n_sems,)),
            pltpu.SemaphoreType.DMA((13,)),
        ],
        compiler_params=pltpu.CompilerParams(collective_id=0, has_side_effects=True),
    )(
        residual,
        query_first,
        key_first,
        value_first,
        documents.reshape(1, tok_rows),
        bias_first,
        out_first,
        norm_gain.reshape(1, -1),
        query_w,
        key_w,
        value_w,
        bias_second,
        out_second,
    )


def solution(mesh):
    placed = (
        P("sp", "tp"),
        P("sp", "tp"),
        P("sp", "tp"),
        P("sp", "tp"),
        P("sp"),
        P("tp", None),
        P("tp", None),
        P(),
        P(None, "tp"),
        P(None, "tp"),
        P(None, "tp"),
        P("tp", None),
        P("tp", None),
    )
    return jax.shard_map(body, mesh=mesh, in_specs=placed, out_specs=P("sp", "tp"), check_vma=False)
```

```python
import functools

import jax
import jax.numpy as jnp
from jax import lax
from jax.experimental import pallas as pl
from jax.experimental.pallas import tpu as pltpu
from jax.sharding import PartitionSpec as P

HEAD_SIZE = 64
SEG = 64
PAST = 4
REL_CLIP = 256
SPAN = PAST * SEG
BAND = SPAN + SEG
LANES = 128
LOG2E = 1.4426950408889634
HIDDEN = -1e30
MESH = pl.DeviceIdType.MESH


eps = 1e-06


def hops_of(tok_rows):
    return range(1, (SPAN + tok_rows - 1) // tok_rows + 1)


def pieces_of(tok_rows):
    pieces = []
    for distance in hops_of(tok_rows):
        top = SPAN - (distance - 1) * tok_rows
        bottom = max(0, top - tok_rows)
        cuts = [cut for cut in range(SEG, tok_rows, SEG) if bottom < cut < top]
        edges = [bottom] + cuts + [top]
        for low, high in reversed(list(zip(edges[:-1], edges[1:]))):
            pieces.append((distance, tok_rows - (top - low), high - low, low))
    return pieces


def build_bias(table_ref, bias_ref):
    heads_local = table_ref.shape[0]
    group_size = bias_ref.shape[2] // SEG
    lane = lax.broadcasted_iota(jnp.int32, (SEG, LANES), 1)
    low = lane < SEG
    last = REL_CLIP + SPAN

    def tile(head, index):
        if index == 0:
            return jnp.broadcast_to(table_ref[head : head + 1, last : last + 1], (SEG, LANES))
        first = last - index * LANES
        return jnp.broadcast_to(table_ref[head : head + 1, first : first + LANES], (SEG, LANES))

    def piece(head, block, base):
        back = block // 2
        if block % 2 == 0:
            source = jnp.where(low, tile(head, back), tile(head, back + 1))
            shift = base
        else:
            source = tile(head, back + 1)
            shift = (base + SEG) % LANES
        return pltpu.roll(source, shift, 1, stride=1, stride_axis=0)

    for head in range(0, heads_local, 2):
        for block in range(PAST + 1):
            pair = jnp.where(low, piece(head, block, 0), piece(head + 1, block, SEG)) * LOG2E
            group, inner = head // group_size, head % group_size
            bias_ref[group, block * SEG : (block + 1) * SEG, inner * SEG : (inner + 2) * SEG] = pair


class Attention:
    def __init__(self, query, kv, bias, mask, mixed, padded, turned, scores, weights, stats, blend):
        self.query, self.kv, self.bias, self.mask, self.mixed = query, kv, bias, mask, mixed
        self.padded, self.turned, self.scores, self.weights = padded, turned, scores, weights
        self.stats, self.blend = stats, blend
        self.cut = SPAN
        self.groups = bias.shape[0]
        self.group_size = bias.shape[2] // SEG
        self.kv_width = self.groups * HEAD_SIZE
        self.state = {}

    def unit(self, segment, group):
        return segment * self.groups + group

    def pad_queries(self, segment):
        lane = lax.broadcasted_iota(jnp.int32, (SEG, LANES), 1)
        rows = slice(segment * SEG, (segment + 1) * SEG)
        for group in range(self.groups):
            keep = (lane >= group * HEAD_SIZE) & (lane < (group + 1) * HEAD_SIZE)
            for inner in range(self.group_size):
                head = group * self.group_size + inner
                column = head * HEAD_SIZE // LANES * LANES
                block = self.query[rows, column : column + LANES]
                if head % 2 != group % 2:
                    block = jnp.concatenate([block[:, HEAD_SIZE:], block[:, :HEAD_SIZE]], axis=1)
                self.padded[self.unit(segment, group), inner * SEG : (inner + 1) * SEG] = jnp.where(
                    keep, block, jnp.zeros_like(block)
                )

    def turn_values(self, row):
        block = jnp.transpose(self.kv[row : row + SEG, self.kv_width : 2 * self.kv_width])
        self.turned[0, :, row : row + SEG] = block
        if row >= SEG:
            self.turned[1, :, row - SEG : row] = block

    def bounds(self, segment, phase):
        first = segment * SEG
        cut = max(first, self.cut)
        return {
            "local": (max(first, SPAN), first + BAND),
            "halo": (first, SPAN),
            "near": (cut, SPAN),
            "rest": (first, cut),
        }[phase]

    def score(self, segment, group, phase):
        low, high = self.bounds(segment, phase)
        unit = self.unit(segment, group)
        band = slice(low - segment * SEG, high - segment * SEG)
        scores = lax.dot_general(
            self.kv[low:high, : self.kv_width],
            self.padded[unit],
            (((1,), (1,)), ((), ())),
            preferred_element_type=jnp.float32,
        )
        mask = self.mask[segment, band]
        mask = jnp.concatenate([mask] * (self.group_size * SEG // LANES), axis=1)
        scores = scores * (HEAD_SIZE ** (-0.5) * LOG2E) + self.bias[group, band] + mask
        self.scores[unit, band] = scores
        largest = jnp.max(scores, axis=0, keepdims=True)
        if phase != "local":
            largest = jnp.maximum(largest, self.stats[unit, 0:1])
        self.state[unit] = (largest,)

    def weigh(self, segment, group, phase):
        low, high = self.bounds(segment, phase)
        unit = self.unit(segment, group)
        band = slice(low - segment * SEG, high - segment * SEG)
        (largest,) = self.state[unit]
        weight = jnp.exp2(self.scores[unit, band] - largest)
        self.weights[unit, band] = weight.astype(jnp.bfloat16)
        total = jnp.sum(weight, axis=0, keepdims=True)
        fade = None
        if phase != "local":
            fade = jnp.exp2(self.stats[unit, 0:1] - largest)
            total = total + self.stats[unit, 1:2] * fade
        if self.ends(segment, phase):
            self.state[unit] = (fade, 1.0 / total)
        else:
            self.stats[unit, 0:1] = largest
            self.stats[unit, 1:2] = total
            self.state[unit] = (fade,)

    def ends(self, segment, phase):
        return phase != "local" and self.bounds(segment, phase)[0] == segment * SEG

    def gather(self, segment, group, phase):
        low, high = self.bounds(segment, phase)
        unit = self.unit(segment, group)
        band = slice(low - segment * SEG, high - segment * SEG)
        odd = low // SEG % 2
        blended = lax.dot_general(
            self.turned[
                odd,
                group * HEAD_SIZE : (group + 1) * HEAD_SIZE,
                low - odd * SEG : high - odd * SEG,
            ],
            self.weights[unit, band],
            (((1,), (0,)), ((), ())),
            preferred_element_type=jnp.float32,
        )
        if phase != "local":
            blended = blended + self.blend[unit] * self.state[unit][0]
        if not self.ends(segment, phase):
            self.blend[unit] = blended
            return
        blended = (blended * self.state[unit][1]).astype(jnp.bfloat16)
        rows = slice(segment * SEG, (segment + 1) * SEG)
        for pair in range(self.group_size // 2):
            turned = jnp.transpose(blended[:, pair * LANES : (pair + 1) * LANES])
            both = jnp.concatenate([turned[:SEG], turned[SEG:]], axis=1)
            column = (group * self.group_size + 2 * pair) * HEAD_SIZE
            self.mixed[rows, column : column + LANES] = both

    def steps(self, segments, phase, arrivals=()):
        units = [(segment, group) for segment in segments for group in range(self.groups)]
        waits = {segment: wait for segment, wait, _ in arrivals}
        turns = {segment: rows for segment, _, rows in arrivals}

        def score(unit):
            segment, group = unit
            if group == 0 and segment in waits:
                waits[segment]()
            self.score(segment, group, phase)
            if group == self.groups - 1 and segment in turns:
                for row in turns[segment]:
                    self.turn_values(row)

        def weigh(unit):
            self.weigh(*unit, phase)

        def gather(unit):
            self.gather(*unit, phase)

        plan = [(score, units[0])]
        for index, unit in enumerate(units):
            if index + 1 < len(units):
                plan.append((score, units[index + 1]))
            if index > 0:
                plan.append((gather, units[index - 1]))
            plan.append((weigh, unit))
        plan.append((gather, units[-1]))
        return [functools.partial(step, unit) for step, unit in plan]

    def run(self, segments, phase, arrivals=()):
        for step in self.steps(segments, phase, arrivals):
            step()


def kernel(
    n_sp,
    residual_hbm,
    query_hbm,
    key_hbm,
    value_hbm,
    docs_hbm,
    bias_one_hbm,
    out_one_hbm,
    gain_hbm,
    query_w_hbm,
    key_w_hbm,
    value_w_hbm,
    bias_two_hbm,
    out_two_hbm,
    result_ref,
    w_out_one,
    w_query,
    w_kv,
    w_out_two,
    kv_one,
    kv_two,
    docs_col,
    mask,
    table_one,
    table_two,
    mixed,
    query_one,
    query_two,
    residual_full,
    part_own,
    part_in,
    layer,
    base,
    scaled,
    scales,
    mixed_in,
    w_other,
    last_mixed,
    w_last,
    padded,
    turned,
    scores,
    weights,
    blend,
    bias_one,
    bias_two,
    gain,
    docs,
    docs_prior,
    stats,
    send_sem,
    recv_sem,
    load_sem,
):
    me = lax.axis_index("sp")
    my_tp = lax.axis_index("tp")
    other = 1 - my_tp
    tok_rows, width_local = residual_hbm.shape
    kv_width = key_hbm.shape[1]
    segments = tok_rows // SEG
    hops = hops_of(tok_rows)
    pieces = pieces_of(tok_rows)
    halves = part_own.shape[0]
    blocks = [(range(segments - 1, 0, -1), SEG, tok_rows - SEG), (range(1), 0, SEG)]

    barrier = pltpu.get_barrier_semaphore()
    expected = jnp.int32(1)
    for distance in hops:
        expected = expected + (me + distance < n_sp).astype(jnp.int32)

        @pl.when(me >= distance)
        def _():
            pl.semaphore_signal(
                barrier, inc=1, device_id={"sp": me - distance}, device_id_type=MESH
            )

    pl.semaphore_signal(barrier, inc=1, device_id={"tp": other}, device_id_type=MESH)

    own = pl.ds(SPAN, tok_rows)
    transfers = dict(
        key=(key_hbm, kv_one.at[own, pl.ds(0, kv_width)]),
        value=(value_hbm, kv_one.at[own, pl.ds(kv_width, kv_width)]),
        docs=(docs_hbm, docs),
        bias_one=(bias_one_hbm, bias_one),
        query=(query_hbm, query_one),
        residual=(residual_hbm, residual_full.at[my_tp]),
        bias_two=(bias_two_hbm, bias_two),
        out_one=(out_one_hbm, w_out_one),
        gain=(gain_hbm, gain),
        key_w=(key_w_hbm, w_kv.at[:, pl.ds(0, kv_width)]),
        value_w=(value_w_hbm, w_kv.at[:, pl.ds(kv_width, kv_width)]),
        query_w=(query_w_hbm, w_query),
        out_two=(out_two_hbm, w_out_two),
    )
    loads = {
        name: pltpu.make_async_copy(src, dst, load_sem.at[index])
        for index, (name, (src, dst)) in enumerate(transfers.items())
    }
    for load in loads.values():
        load.start()

    slot = iter(range(send_sem.shape[0]))

    def remote(src, dst, target):
        index = next(slot)
        return pltpu.make_async_remote_copy(
            src_ref=src,
            dst_ref=dst,
            send_sem=send_sem.at[index],
            recv_sem=recv_sem.at[index],
            device_id=target,
            device_id_type=MESH,
        )

    def ahead(distance):
        return {"sp": lax.rem(me + distance, n_sp)}

    def start_sent(distance, copies):
        @pl.when(me + distance < n_sp)
        def _():
            for copy in copies:
                copy.start()

    def wait_arrived(distance, copies):
        @pl.when(me >= distance)
        def _():
            for copy in copies:
                copy.wait_recv()

    def wait_sent(distance, copies):
        @pl.when(me + distance < n_sp)
        def _():
            for copy in copies:
                copy.wait_send()

    for distance, _, needed, landing in pieces:

        @pl.when(me < distance)
        def _():
            empty = jnp.zeros((needed, 2 * kv_width), jnp.bfloat16)
            kv_one[landing : landing + needed] = empty
            kv_two[landing : landing + needed] = empty

    for distance in hops:

        @pl.when(me < distance)
        def _():
            docs_prior[distance - 1] = jnp.full((1, tok_rows), -1, jnp.int32)

    eye = lax.broadcasted_iota(jnp.int32, (SEG, SEG), 0) == lax.broadcasted_iota(
        jnp.int32, (SEG, SEG), 1
    )

    def put_column(numbers, place):
        picked = jnp.where(eye, numbers.astype(jnp.float32), 0.0)
        docs_col[place : place + SEG] = jnp.broadcast_to(
            jnp.sum(picked, axis=1, keepdims=True), (SEG, LANES)
        )

    def put_mask(segment, low, high):
        mine = docs[:, segment * SEG : (segment + 1) * SEG].astype(jnp.float32)
        mine = jnp.concatenate([mine, mine], axis=1)
        same = docs_col[low:high] == mine
        first = segment * SEG
        mask[segment, low - first : high - first] = jnp.where(same, 0.0, HIDDEN)

    shared = (mask, mixed, padded, turned, scores, weights, stats, blend)
    one = Attention(query_one, kv_one, table_one, *shared)
    two = Attention(query_two, kv_two, table_two, *shared)
    newest_first = range(segments - 1, -1, -1)
    two.cut = pieces[0][3]

    for name in ("key", "value", "docs"):
        loads[name].wait()
    pl.semaphore_wait(barrier, expected)

    def halo_copy(kv, piece):
        distance, row, needed, landing = piece
        return remote(
            kv.at[pl.ds(SPAN + row, needed)], kv.at[pl.ds(landing, needed)], ahead(distance)
        )

    docs_copies = [
        (distance, [remote(docs, docs_prior.at[distance - 1], ahead(distance))])
        for distance in hops
    ]
    first_copies = [(piece[0], [halo_copy(kv_one, piece)]) for piece in pieces]
    for distance, copies in docs_copies + first_copies:
        start_sent(distance, copies)
    loads["residual"].wait()
    residual_copy = remote(residual_full.at[my_tp], residual_full.at[my_tp], {"tp": other})
    residual_copy.start()

    loads["query"].wait()
    for row in range(SPAN, SPAN + tok_rows, SEG):
        one.turn_values(row)
    for segment in newest_first:
        one.pad_queries(segment)
    for block in range(0, tok_rows, SEG):
        put_column(docs[:, block : block + SEG], SPAN + block)
    for segment in range(segments):
        put_mask(segment, *one.bounds(segment, "local"))

    loads["bias_one"].wait()
    build_bias(bias_one, table_one)
    loads["out_one"].wait()
    weight_copy = remote(w_out_one, w_other, {"tp": other})

    @pl.when(my_tp == 0)
    def _():
        weight_copy.start()

    one.run(newest_first, "local")

    for distance, copies in docs_copies:
        wait_arrived(distance, copies)
    for distance, row, needed, landing in pieces:
        for block in range(0, needed, SEG):
            put_column(
                docs_prior[distance - 1, :, row + block : row + block + SEG], landing + block
            )
    for segment in range(segments):
        put_mask(segment, *one.bounds(segment, "halo"))
    residual_copy.wait_recv()

    def arrival(segment, waiting, which):
        members = list(zip(pieces, waiting))[which]

        def wait():
            for _, (distance, copies) in members:
                wait_arrived(distance, copies)

        rows = [
            row
            for (_, _, needed, landing), _ in members
            for row in range(landing, landing + needed, SEG)
        ]
        return segment, wait, rows

    newest, older = newest_first[0], newest_first[1]

    part_copies = []
    for _, start, count in blocks:
        rows = pl.ds(start, count)
        part_copies.append(
            [
                remote(part_own.at[half, rows], part_in.at[half, rows], {"tp": other})
                for half in range(halves)
            ]
        )

    mixed_copies = []
    for members, _, _ in blocks:
        mixed_copies.append([])
        for segment in members:
            rows = pl.ds(segment * SEG, SEG)
            mixed_copies[-1].append(remote(mixed.at[rows], mixed_in.at[rows], {"tp": other}))

    def start_mixed(block):
        @pl.when(my_tp == 0)
        def _():
            for copy in mixed_copies[block]:
                copy.start()

    def project(source, weight, rows):
        return [
            jnp.dot(
                source[rows],
                weight[:, half * width_local : (half + 1) * width_local],
                preferred_element_type=jnp.float32,
            ).astype(jnp.bfloat16)
            for half in range(halves)
        ]

    def project_one(block):
        _, start, count = blocks[block]
        rows = slice(start, start + count)
        parts = project(mixed, w_out_one, rows)
        for half, part in enumerate(parts):
            part_own[half, rows] = part

        @pl.when(my_tp == 1)
        def _():
            for copy in part_copies[block]:
                copy.start()

        for half, part in enumerate(parts):
            base[half, rows] = residual_full[half, rows].astype(jnp.float32) + part.astype(
                jnp.float32
            )

    second_copies = [(piece[0], [halo_copy(kv_two, piece)]) for piece in pieces]

    def keys_two(block, core):
        _, start, count = blocks[block]
        rows = slice(start, start + count)
        squares = jnp.zeros((count, LANES), jnp.float32)
        if core == 0:
            for copy in part_copies[block]:
                copy.wait_recv()
            parts = [part_in[half, rows] for half in range(halves)]
        else:
            if block == 0:
                weight_copy.wait_recv()
            for copy in mixed_copies[block]:
                copy.wait_recv()
            parts = project(mixed_in, w_other, rows)
        for half in range(halves):
            new = base[half, rows] + parts[half].astype(jnp.float32)
            new = new.astype(jnp.bfloat16)
            layer[half, rows] = new
            new = new.astype(jnp.float32)
            columns = slice(half * width_local, (half + 1) * width_local)
            scaled[rows, columns] = (new * gain[:, columns]).astype(jnp.bfloat16)
            for lane in range(0, width_local, LANES):
                squares = squares + new[:, lane : lane + LANES] * new[:, lane : lane + LANES]
        scale = lax.rsqrt(
            jnp.sum(squares, axis=1, keepdims=True) / (halves * width_local) + eps
        )
        scales[rows] = jnp.broadcast_to(scale, (count, LANES))
        kv_two[SPAN + start : SPAN + start + count] = (
            jnp.dot(scaled[rows], w_kv[...], preferred_element_type=jnp.float32) * scale
        ).astype(jnp.bfloat16)
        for piece, copies in zip(pieces, second_copies):
            if start <= piece[1] < start + count:
                start_sent(*copies)

    for name in ("gain", "key_w", "value_w", "query_w"):
        loads[name].wait()
    for step in one.steps(
        newest_first[:-1],
        "halo",
        (
            arrival(newest, first_copies, slice(0, 1)),
            arrival(older, first_copies, slice(1, 2)),
        ),
    ):
        step()
    start_mixed(0)
    project_one(0)
    plan = one.steps(
        newest_first[-1:], "halo", (arrival(newest_first[-1], first_copies, slice(2, None)),)
    )

    @pl.when(my_tp == 0)
    def _():
        keys_two(0, 0)

    for step in plan:
        step()
    start_mixed(1)
    project_one(1)
    loads["bias_two"].wait()

    @pl.when(my_tp == 1)
    def _():
        build_bias(bias_two, table_two)
        keys_two(0, 1)
        keys_two(1, 1)

    @pl.when(my_tp == 0)
    def _():
        keys_two(1, 0)

    query_two[...] = (
        jnp.dot(scaled[...], w_query[...], preferred_element_type=jnp.float32) * scales[:, 0:1]
    ).astype(jnp.bfloat16)

    @pl.when(my_tp == 0)
    def _():
        build_bias(bias_two, table_two)

    for row in range(SPAN, SPAN + tok_rows, SEG):
        two.turn_values(row)
    for segment in newest_first:
        two.pad_queries(segment)
    loads["out_two"].wait()
    theirs = pl.ds(pl.multiple_of(other * width_local, width_local), width_local)
    ours = pl.ds(pl.multiple_of(my_tp * width_local, width_local), width_local)
    last_weight = remote(w_out_two.at[:, theirs], w_last, {"tp": other})
    last_weight.start()
    two.run(newest_first, "local")

    @pl.when(my_tp == 1)
    def _():
        for copies in part_copies:
            for copy in copies:
                copy.wait_send()

    @pl.when(my_tp == 0)
    def _():
        weight_copy.wait_send()
        for copies in mixed_copies:
            for copy in copies:
                copy.wait_send()


    finished = (pl.ds(two.cut, tok_rows - two.cut), pl.ds(0, two.cut))
    mixed_last = [
        remote(mixed.at[rows], last_mixed.at[rows], {"tp": other}) for rows in finished
    ]
    two.run(newest_first, "near", (arrival(newest, second_copies, slice(0, 1)),))

    mixed_last[0].start()
    two.run(
        [segment for segment in newest_first if segment * SEG < two.cut],
        "rest",
        (arrival(older, second_copies, slice(1, None)),),
    )
    mixed_last[1].start()
    branch = jnp.dot(mixed[...], w_out_two[:, ours], preferred_element_type=jnp.float32).astype(
        jnp.bfloat16
    )
    base[0] = layer[my_tp].astype(jnp.float32) + branch.astype(jnp.float32)
    last_weight.wait_recv()
    for copy in mixed_last:
        copy.wait_recv()
    branch = jnp.dot(last_mixed[...], w_last[...], preferred_element_type=jnp.float32).astype(
        jnp.bfloat16
    )
    result_ref[...] = (base[0] + branch.astype(jnp.float32)).astype(jnp.bfloat16)

    last_weight.wait_send()
    for copy in mixed_last:
        copy.wait_send()
    residual_copy.wait_send()
    for distance, copies in docs_copies + first_copies + second_copies:
        wait_sent(distance, copies)


def body(
    residual,
    query_first,
    key_first,
    value_first,
    documents,
    bias_first,
    out_first,
    norm_gain,
    query_w,
    key_w,
    value_w,
    bias_second,
    out_second,
):
    n_sp = lax.axis_size("sp")
    tok_rows, width_local = residual.shape
    query_width = query_first.shape[1]
    kv_width = key_first.shape[1]
    kv_local = kv_width // HEAD_SIZE
    group_width = query_width // kv_local
    halves = out_first.shape[1] // width_local
    hops = len(hops_of(tok_rows))
    units = tok_rows // SEG * kv_local
    n_sems = hops + 2 * len(pieces_of(tok_rows)) + 1 + 2 * halves
    n_sems += tok_rows // SEG + 1 + 3
    vmem = pl.BlockSpec(memory_space=pltpu.VMEM)
    hbm = pl.BlockSpec(memory_space=pl.ANY)
    bf16 = jnp.bfloat16
    f32 = jnp.float32
    return pl.pallas_call(
        functools.partial(kernel, n_sp),
        name="two_layers",
        out_shape=pltpu.VMEM((tok_rows, width_local), bf16),
        in_specs=[hbm] * 13,
        out_specs=vmem,
        scratch_shapes=[
            pltpu.VMEM(out_first.shape, bf16),
            pltpu.VMEM(query_w.shape, bf16),
            pltpu.VMEM((key_w.shape[0], 2 * kv_width), bf16),
            pltpu.VMEM(out_second.shape, bf16),
            pltpu.VMEM((SPAN + tok_rows, 2 * kv_width), bf16),
            pltpu.VMEM((SPAN + tok_rows, 2 * kv_width), bf16),
            pltpu.VMEM((SPAN + tok_rows, LANES), f32),
            pltpu.VMEM((tok_rows // SEG, BAND, LANES), f32),
            pltpu.VMEM((kv_local, BAND, group_width), f32),
            pltpu.VMEM((kv_local, BAND, group_width), f32),
            pltpu.VMEM((tok_rows, query_width), bf16),
            pltpu.VMEM((tok_rows, query_width), bf16),
            pltpu.VMEM((tok_rows, query_width), bf16),
            pltpu.VMEM((halves, tok_rows, width_local), bf16),
            pltpu.VMEM((halves, tok_rows, width_local), bf16),
            pltpu.VMEM((halves, tok_rows, width_local), bf16),
            pltpu.VMEM((halves, tok_rows, width_local), bf16),
            pltpu.VMEM((halves, tok_rows, width_local), f32),
            pltpu.VMEM((tok_rows, halves * width_local), bf16),
            pltpu.VMEM((tok_rows, LANES), f32),
            pltpu.VMEM((tok_rows, query_width), bf16),
            pltpu.VMEM(out_first.shape, bf16),
            pltpu.VMEM((tok_rows, query_width), bf16),
            pltpu.VMEM((out_second.shape[0], width_local), bf16),
            pltpu.VMEM((units, group_width, LANES), bf16),
            pltpu.VMEM((2, kv_width, pl.cdiv(SPAN + tok_rows, LANES) * LANES), bf16),
            pltpu.VMEM((units, BAND, group_width), f32),
            pltpu.VMEM((units, BAND, group_width), bf16),
            pltpu.VMEM((units, HEAD_SIZE, group_width), f32),
            pltpu.VMEM(bias_first.shape, f32),
            pltpu.VMEM(bias_second.shape, f32),
            pltpu.VMEM((1, norm_gain.shape[0]), f32),
            pltpu.VMEM((1, tok_rows), jnp.int32),
            pltpu.VMEM((hops, 1, tok_rows), jnp.int32),
            pltpu.VMEM((units, 2, group_width), f32),
            pltpu.SemaphoreType.DMA((n_sems,)),
            pltpu.SemaphoreType.DMA((n_sems,)),
            pltpu.SemaphoreType.DMA((13,)),
        ],
        compiler_params=pltpu.CompilerParams(collective_id=0, has_side_effects=True),
    )(
        residual,
        query_first,
        key_first,
        value_first,
        documents.reshape(1, tok_rows),
        bias_first,
        out_first,
        norm_gain.reshape(1, -1),
        query_w,
        key_w,
        value_w,
        bias_second,
        out_second,
    )


def solution(mesh):
    placed = (
        P("sp", "tp"),
        P("sp", "tp"),
        P("sp", "tp"),
        P("sp", "tp"),
        P("sp"),
        P("tp", None),
        P("tp", None),
        P(),
        P(None, "tp"),
        P(None, "tp"),
        P(None, "tp"),
        P("tp", None),
        P("tp", None),
    )
    return jax.shard_map(body, mesh=mesh, in_specs=placed, out_specs=P("sp", "tp"), check_vma=False)
```

```python
import functools

import jax
import jax.numpy as jnp
from jax import lax
from jax.experimental import pallas as pl
from jax.experimental.pallas import tpu as pltpu
from jax.sharding import PartitionSpec as P

HEAD_SIZE = 64
SEG = 64
PAST = 4
REL_CLIP = 256
SPAN = PAST * SEG
BAND = SPAN + SEG
LANES = 128
LOG2E = 1.4426950408889634
HIDDEN = -1e30
MESH = pl.DeviceIdType.MESH


eps = 1e-06


def hops_of(tok_rows):
    return range(1, (SPAN + tok_rows - 1) // tok_rows + 1)


def pieces_of(tok_rows):
    pieces = []
    for distance in hops_of(tok_rows):
        top = SPAN - (distance - 1) * tok_rows
        bottom = max(0, top - tok_rows)
        cuts = [cut for cut in range(SEG, tok_rows, SEG) if bottom < cut < top]
        edges = [bottom] + cuts + [top]
        for low, high in reversed(list(zip(edges[:-1], edges[1:]))):
            pieces.append((distance, tok_rows - (top - low), high - low, low))
    return pieces


def build_bias(table_ref, bias_ref):
    heads_local = table_ref.shape[0]
    group_size = bias_ref.shape[2] // SEG
    lane = lax.broadcasted_iota(jnp.int32, (SEG, LANES), 1)
    low = lane < SEG
    last = REL_CLIP + SPAN

    def tile(head, index):
        if index == 0:
            return jnp.broadcast_to(table_ref[head : head + 1, last : last + 1], (SEG, LANES))
        first = last - index * LANES
        return jnp.broadcast_to(table_ref[head : head + 1, first : first + LANES], (SEG, LANES))

    def piece(head, block, base):
        back = block // 2
        if block % 2 == 0:
            source = jnp.where(low, tile(head, back), tile(head, back + 1))
            shift = base
        else:
            source = tile(head, back + 1)
            shift = (base + SEG) % LANES
        return pltpu.roll(source, shift, 1, stride=1, stride_axis=0)

    for head in range(0, heads_local, 2):
        for block in range(PAST + 1):
            pair = jnp.where(low, piece(head, block, 0), piece(head + 1, block, SEG)) * LOG2E
            group, inner = head // group_size, head % group_size
            bias_ref[group, block * SEG : (block + 1) * SEG, inner * SEG : (inner + 2) * SEG] = pair


class Attention:
    def __init__(self, query, kv, bias, mask, mixed, padded, turned, scores, weights, stats, blend):
        self.query, self.kv, self.bias, self.mask, self.mixed = query, kv, bias, mask, mixed
        self.padded, self.turned, self.scores, self.weights = padded, turned, scores, weights
        self.stats, self.blend = stats, blend
        self.cut = SPAN
        self.groups = bias.shape[0]
        self.group_size = bias.shape[2] // SEG
        self.kv_width = self.groups * HEAD_SIZE
        self.state = {}

    def unit(self, segment, group):
        return segment * self.groups + group

    def pad_queries(self, segment):
        lane = lax.broadcasted_iota(jnp.int32, (SEG, LANES), 1)
        rows = slice(segment * SEG, (segment + 1) * SEG)
        for group in range(self.groups):
            keep = (lane >= group * HEAD_SIZE) & (lane < (group + 1) * HEAD_SIZE)
            for inner in range(self.group_size):
                head = group * self.group_size + inner
                column = head * HEAD_SIZE // LANES * LANES
                block = self.query[rows, column : column + LANES]
                if head % 2 != group % 2:
                    block = jnp.concatenate([block[:, HEAD_SIZE:], block[:, :HEAD_SIZE]], axis=1)
                self.padded[self.unit(segment, group), inner * SEG : (inner + 1) * SEG] = jnp.where(
                    keep, block, jnp.zeros_like(block)
                )

    def turn_values(self, row):
        block = jnp.transpose(self.kv[row : row + SEG, self.kv_width : 2 * self.kv_width])
        self.turned[0, :, row : row + SEG] = block
        if row >= SEG:
            self.turned[1, :, row - SEG : row] = block

    def bounds(self, segment, phase):
        first = segment * SEG
        cut = max(first, self.cut)
        return {
            "local": (max(first, SPAN), first + BAND),
            "halo": (first, SPAN),
            "near": (cut, SPAN),
            "rest": (first, cut),
        }[phase]

    def score(self, segment, group, phase):
        low, high = self.bounds(segment, phase)
        unit = self.unit(segment, group)
        band = slice(low - segment * SEG, high - segment * SEG)
        scores = lax.dot_general(
            self.kv[low:high, : self.kv_width],
            self.padded[unit],
            (((1,), (1,)), ((), ())),
            preferred_element_type=jnp.float32,
        )
        mask = self.mask[segment, band]
        mask = jnp.concatenate([mask] * (self.group_size * SEG // LANES), axis=1)
        scores = scores * (HEAD_SIZE ** (-0.5) * LOG2E) + self.bias[group, band] + mask
        self.scores[unit, band] = scores
        largest = jnp.max(scores, axis=0, keepdims=True)
        if phase != "local":
            largest = jnp.maximum(largest, self.stats[unit, 0:1])
        self.state[unit] = (largest,)

    def weigh(self, segment, group, phase):
        low, high = self.bounds(segment, phase)
        unit = self.unit(segment, group)
        band = slice(low - segment * SEG, high - segment * SEG)
        (largest,) = self.state[unit]
        weight = jnp.exp2(self.scores[unit, band] - largest)
        self.weights[unit, band] = weight.astype(jnp.bfloat16)
        total = jnp.sum(weight, axis=0, keepdims=True)
        fade = None
        if phase != "local":
            fade = jnp.exp2(self.stats[unit, 0:1] - largest)
            total = total + self.stats[unit, 1:2] * fade
        if self.ends(segment, phase):
            self.state[unit] = (fade, 1.0 / total)
        else:
            self.stats[unit, 0:1] = largest
            self.stats[unit, 1:2] = total
            self.state[unit] = (fade,)

    def ends(self, segment, phase):
        return phase != "local" and self.bounds(segment, phase)[0] == segment * SEG

    def gather(self, segment, group, phase):
        low, high = self.bounds(segment, phase)
        unit = self.unit(segment, group)
        band = slice(low - segment * SEG, high - segment * SEG)
        odd = low // SEG % 2
        blended = lax.dot_general(
            self.turned[
                odd,
                group * HEAD_SIZE : (group + 1) * HEAD_SIZE,
                low - odd * SEG : high - odd * SEG,
            ],
            self.weights[unit, band],
            (((1,), (0,)), ((), ())),
            preferred_element_type=jnp.float32,
        )
        if phase != "local":
            blended = blended + self.blend[unit] * self.state[unit][0]
        if not self.ends(segment, phase):
            self.blend[unit] = blended
            return
        blended = (blended * self.state[unit][1]).astype(jnp.bfloat16)
        rows = slice(segment * SEG, (segment + 1) * SEG)
        for pair in range(self.group_size // 2):
            turned = jnp.transpose(blended[:, pair * LANES : (pair + 1) * LANES])
            both = jnp.concatenate([turned[:SEG], turned[SEG:]], axis=1)
            column = (group * self.group_size + 2 * pair) * HEAD_SIZE
            self.mixed[rows, column : column + LANES] = both

    def steps(self, segments, phase, arrivals=()):
        units = [(segment, group) for segment in segments for group in range(self.groups)]
        waits = {segment: wait for segment, wait, _ in arrivals}
        turns = {segment: rows for segment, _, rows in arrivals}

        def score(unit):
            segment, group = unit
            if group == 0 and segment in waits:
                waits[segment]()
            self.score(segment, group, phase)
            if group == self.groups - 1 and segment in turns:
                for row in turns[segment]:
                    self.turn_values(row)

        def weigh(unit):
            self.weigh(*unit, phase)

        def gather(unit):
            self.gather(*unit, phase)

        plan = [(score, units[0])]
        for index, unit in enumerate(units):
            if index + 1 < len(units):
                plan.append((score, units[index + 1]))
            if index > 0:
                plan.append((gather, units[index - 1]))
            plan.append((weigh, unit))
        plan.append((gather, units[-1]))
        return [functools.partial(step, unit) for step, unit in plan]

    def run(self, segments, phase, arrivals=()):
        for step in self.steps(segments, phase, arrivals):
            step()


def kernel(
    n_sp,
    residual_hbm,
    query_hbm,
    key_hbm,
    value_hbm,
    docs_hbm,
    bias_one_hbm,
    out_one_hbm,
    gain_hbm,
    query_w_hbm,
    key_w_hbm,
    value_w_hbm,
    bias_two_hbm,
    out_two_hbm,
    result_ref,
    w_out_one,
    w_query,
    w_kv,
    w_out_two,
    kv_one,
    kv_two,
    docs_col,
    mask,
    table_one,
    table_two,
    mixed,
    query_one,
    query_two,
    residual_full,
    part_own,
    part_in,
    layer,
    base,
    scaled,
    scales,
    mixed_in,
    w_other,
    last_mixed,
    w_last,
    padded,
    turned,
    scores,
    weights,
    blend,
    bias_one,
    bias_two,
    gain,
    docs,
    docs_prior,
    stats,
    send_sem,
    recv_sem,
    load_sem,
):
    me = lax.axis_index("sp")
    my_tp = lax.axis_index("tp")
    other = 1 - my_tp
    tok_rows, width_local = residual_hbm.shape
    kv_width = key_hbm.shape[1]
    segments = tok_rows // SEG
    hops = hops_of(tok_rows)
    pieces = pieces_of(tok_rows)
    halves = part_own.shape[0]
    blocks = [(range(segments - 1, 0, -1), SEG, tok_rows - SEG), (range(1), 0, SEG)]

    barrier = pltpu.get_barrier_semaphore()
    expected = jnp.int32(1)
    for distance in hops:
        expected = expected + (me + distance < n_sp).astype(jnp.int32)

        @pl.when(me >= distance)
        def _():
            pl.semaphore_signal(
                barrier, inc=1, device_id={"sp": me - distance}, device_id_type=MESH
            )

    pl.semaphore_signal(barrier, inc=1, device_id={"tp": other}, device_id_type=MESH)

    own = pl.ds(SPAN, tok_rows)
    transfers = dict(
        key=(key_hbm, kv_one.at[own, pl.ds(0, kv_width)]),
        value=(value_hbm, kv_one.at[own, pl.ds(kv_width, kv_width)]),
        docs=(docs_hbm, docs),
        bias_one=(bias_one_hbm, bias_one),
        query=(query_hbm, query_one),
        residual=(residual_hbm, residual_full.at[my_tp]),
        bias_two=(bias_two_hbm, bias_two),
        out_one=(out_one_hbm, w_out_one),
        gain=(gain_hbm, gain),
        key_w=(key_w_hbm, w_kv.at[:, pl.ds(0, kv_width)]),
        value_w=(value_w_hbm, w_kv.at[:, pl.ds(kv_width, kv_width)]),
        query_w=(query_w_hbm, w_query),
        out_two=(out_two_hbm, w_out_two),
    )
    loads = {
        name: pltpu.make_async_copy(src, dst, load_sem.at[index])
        for index, (name, (src, dst)) in enumerate(transfers.items())
    }
    for load in loads.values():
        load.start()

    slot = iter(range(send_sem.shape[0]))

    def remote(src, dst, target):
        index = next(slot)
        return pltpu.make_async_remote_copy(
            src_ref=src,
            dst_ref=dst,
            send_sem=send_sem.at[index],
            recv_sem=recv_sem.at[index],
            device_id=target,
            device_id_type=MESH,
        )

    def ahead(distance):
        return {"sp": lax.rem(me + distance, n_sp)}

    def start_sent(distance, copies):
        @pl.when(me + distance < n_sp)
        def _():
            for copy in copies:
                copy.start()

    def wait_arrived(distance, copies):
        @pl.when(me >= distance)
        def _():
            for copy in copies:
                copy.wait_recv()

    def wait_sent(distance, copies):
        @pl.when(me + distance < n_sp)
        def _():
            for copy in copies:
                copy.wait_send()

    for distance, _, needed, landing in pieces:

        @pl.when(me < distance)
        def _():
            empty = jnp.zeros((needed, 2 * kv_width), jnp.bfloat16)
            kv_one[landing : landing + needed] = empty
            kv_two[landing : landing + needed] = empty

    for distance in hops:

        @pl.when(me < distance)
        def _():
            docs_prior[distance - 1] = jnp.full((1, tok_rows), -1, jnp.int32)

    eye = lax.broadcasted_iota(jnp.int32, (SEG, SEG), 0) == lax.broadcasted_iota(
        jnp.int32, (SEG, SEG), 1
    )

    def put_column(numbers, place):
        picked = jnp.where(eye, numbers.astype(jnp.float32), 0.0)
        docs_col[place : place + SEG] = jnp.broadcast_to(
            jnp.sum(picked, axis=1, keepdims=True), (SEG, LANES)
        )

    def put_mask(segment, low, high):
        mine = docs[:, segment * SEG : (segment + 1) * SEG].astype(jnp.float32)
        mine = jnp.concatenate([mine, mine], axis=1)
        same = docs_col[low:high] == mine
        first = segment * SEG
        mask[segment, low - first : high - first] = jnp.where(same, 0.0, HIDDEN)

    shared = (mask, mixed, padded, turned, scores, weights, stats, blend)
    one = Attention(query_one, kv_one, table_one, *shared)
    two = Attention(query_two, kv_two, table_two, *shared)
    newest_first = range(segments - 1, -1, -1)
    two.cut = pieces[0][3]

    for name in ("key", "value", "docs"):
        loads[name].wait()
    pl.semaphore_wait(barrier, expected)

    def halo_copy(kv, piece):
        distance, row, needed, landing = piece
        return remote(
            kv.at[pl.ds(SPAN + row, needed)], kv.at[pl.ds(landing, needed)], ahead(distance)
        )

    docs_copies = [
        (distance, [remote(docs, docs_prior.at[distance - 1], ahead(distance))])
        for distance in hops
    ]
    first_copies = [(piece[0], [halo_copy(kv_one, piece)]) for piece in pieces]
    for distance, copies in docs_copies + first_copies:
        start_sent(distance, copies)
    loads["residual"].wait()
    residual_copy = remote(residual_full.at[my_tp], residual_full.at[my_tp], {"tp": other})
    residual_copy.start()

    loads["query"].wait()
    for row in range(SPAN, SPAN + tok_rows, SEG):
        one.turn_values(row)
    for segment in newest_first:
        one.pad_queries(segment)
    for block in range(0, tok_rows, SEG):
        put_column(docs[:, block : block + SEG], SPAN + block)
    for segment in range(segments):
        put_mask(segment, *one.bounds(segment, "local"))

    loads["bias_one"].wait()
    build_bias(bias_one, table_one)
    loads["out_one"].wait()
    weight_copy = remote(w_out_one, w_other, {"tp": other})

    @pl.when(my_tp == 0)
    def _():
        weight_copy.start()

    loads["out_two"].wait()
    theirs = pl.ds(pl.multiple_of(other * width_local, width_local), width_local)
    ours = pl.ds(pl.multiple_of(my_tp * width_local, width_local), width_local)
    last_weight = remote(w_out_two.at[:, theirs], w_last, {"tp": other})
    last_weight.start()
    one.run(newest_first, "local")

    for distance, copies in docs_copies:
        wait_arrived(distance, copies)
    for distance, row, needed, landing in pieces:
        for block in range(0, needed, SEG):
            put_column(
                docs_prior[distance - 1, :, row + block : row + block + SEG], landing + block
            )
    for segment in range(segments):
        put_mask(segment, *one.bounds(segment, "halo"))
    residual_copy.wait_recv()

    def arrival(segment, waiting, which):
        members = list(zip(pieces, waiting))[which]

        def wait():
            for _, (distance, copies) in members:
                wait_arrived(distance, copies)

        rows = [
            row
            for (_, _, needed, landing), _ in members
            for row in range(landing, landing + needed, SEG)
        ]
        return segment, wait, rows

    newest, older = newest_first[0], newest_first[1]

    part_copies = []
    for _, start, count in blocks:
        rows = pl.ds(start, count)
        part_copies.append(
            [
                remote(part_own.at[half, rows], part_in.at[half, rows], {"tp": other})
                for half in range(halves)
            ]
        )

    mixed_copies = []
    for members, _, _ in blocks:
        mixed_copies.append([])
        for segment in members:
            rows = pl.ds(segment * SEG, SEG)
            mixed_copies[-1].append(remote(mixed.at[rows], mixed_in.at[rows], {"tp": other}))

    def start_mixed(block):
        @pl.when(my_tp == 0)
        def _():
            for copy in mixed_copies[block]:
                copy.start()

    def project(source, weight, rows):
        return [
            jnp.dot(
                source[rows],
                weight[:, half * width_local : (half + 1) * width_local],
                preferred_element_type=jnp.float32,
            ).astype(jnp.bfloat16)
            for half in range(halves)
        ]

    def project_one(block):
        _, start, count = blocks[block]
        rows = slice(start, start + count)
        parts = project(mixed, w_out_one, rows)
        for half, part in enumerate(parts):
            part_own[half, rows] = part

        @pl.when(my_tp == 1)
        def _():
            for copy in part_copies[block]:
                copy.start()

        for half, part in enumerate(parts):
            base[half, rows] = residual_full[half, rows].astype(jnp.float32) + part.astype(
                jnp.float32
            )

    second_copies = [(piece[0], [halo_copy(kv_two, piece)]) for piece in pieces]

    def keys_two(block, core):
        _, start, count = blocks[block]
        rows = slice(start, start + count)
        squares = jnp.zeros((count, LANES), jnp.float32)
        if core == 0:
            for copy in part_copies[block]:
                copy.wait_recv()
            parts = [part_in[half, rows] for half in range(halves)]
        else:
            if block == 0:
                weight_copy.wait_recv()
            for copy in mixed_copies[block]:
                copy.wait_recv()
            parts = project(mixed_in, w_other, rows)
        for half in range(halves):
            new = base[half, rows] + parts[half].astype(jnp.float32)
            new = new.astype(jnp.bfloat16)
            layer[half, rows] = new
            new = new.astype(jnp.float32)
            columns = slice(half * width_local, (half + 1) * width_local)
            scaled[rows, columns] = (new * gain[:, columns]).astype(jnp.bfloat16)
            for lane in range(0, width_local, LANES):
                squares = squares + new[:, lane : lane + LANES] * new[:, lane : lane + LANES]
        scale = lax.rsqrt(
            jnp.sum(squares, axis=1, keepdims=True) / (halves * width_local) + eps
        )
        scales[rows] = jnp.broadcast_to(scale, (count, LANES))
        kv_two[SPAN + start : SPAN + start + count] = (
            jnp.dot(scaled[rows], w_kv[...], preferred_element_type=jnp.float32) * scale
        ).astype(jnp.bfloat16)
        for piece, copies in reversed(list(zip(pieces, second_copies))):
            late = core == 1 and piece[0] != pieces[0][0]
            if block == 1 if late else start <= piece[1] < start + count:
                start_sent(*copies)

    for name in ("gain", "key_w", "value_w", "query_w"):
        loads[name].wait()
    for step in one.steps(
        newest_first[:-1],
        "halo",
        (
            arrival(newest, first_copies, slice(0, 1)),
            arrival(older, first_copies, slice(1, 2)),
        ),
    ):
        step()
    start_mixed(0)
    project_one(0)
    plan = one.steps(
        newest_first[-1:], "halo", (arrival(newest_first[-1], first_copies, slice(2, None)),)
    )

    @pl.when(my_tp == 0)
    def _():
        keys_two(0, 0)

    for step in plan:
        step()
    start_mixed(1)
    project_one(1)
    loads["bias_two"].wait()

    @pl.when(my_tp == 1)
    def _():
        build_bias(bias_two, table_two)
        keys_two(0, 1)
        keys_two(1, 1)

    @pl.when(my_tp == 0)
    def _():
        keys_two(1, 0)

    query_two[...] = (
        jnp.dot(scaled[...], w_query[...], preferred_element_type=jnp.float32) * scales[:, 0:1]
    ).astype(jnp.bfloat16)

    @pl.when(my_tp == 0)
    def _():
        build_bias(bias_two, table_two)

    for row in range(SPAN, SPAN + tok_rows, SEG):
        two.turn_values(row)
    for segment in newest_first:
        two.pad_queries(segment)
    two.run(newest_first, "local")

    @pl.when(my_tp == 1)
    def _():
        for copies in part_copies:
            for copy in copies:
                copy.wait_send()

    @pl.when(my_tp == 0)
    def _():
        weight_copy.wait_send()
        for copies in mixed_copies:
            for copy in copies:
                copy.wait_send()


    finished = (pl.ds(two.cut, tok_rows - two.cut), pl.ds(0, two.cut))
    mixed_last = [
        remote(mixed.at[rows], last_mixed.at[rows], {"tp": other}) for rows in finished
    ]
    two.run(newest_first, "near", (arrival(newest, second_copies, slice(0, 1)),))

    mixed_last[0].start()
    two.run(
        [segment for segment in newest_first if segment * SEG < two.cut],
        "rest",
        (arrival(older, second_copies, slice(1, None)),),
    )
    mixed_last[1].start()
    branch = jnp.dot(mixed[...], w_out_two[:, ours], preferred_element_type=jnp.float32).astype(
        jnp.bfloat16
    )
    base[0] = layer[my_tp].astype(jnp.float32) + branch.astype(jnp.float32)
    last_weight.wait_recv()
    for copy in mixed_last:
        copy.wait_recv()
    branch = jnp.dot(last_mixed[...], w_last[...], preferred_element_type=jnp.float32).astype(
        jnp.bfloat16
    )
    result_ref[...] = (base[0] + branch.astype(jnp.float32)).astype(jnp.bfloat16)

    last_weight.wait_send()
    for copy in mixed_last:
        copy.wait_send()
    residual_copy.wait_send()
    for distance, copies in docs_copies + first_copies + second_copies:
        wait_sent(distance, copies)


def body(
    residual,
    query_first,
    key_first,
    value_first,
    documents,
    bias_first,
    out_first,
    norm_gain,
    query_w,
    key_w,
    value_w,
    bias_second,
    out_second,
):
    n_sp = lax.axis_size("sp")
    tok_rows, width_local = residual.shape
    query_width = query_first.shape[1]
    kv_width = key_first.shape[1]
    kv_local = kv_width // HEAD_SIZE
    group_width = query_width // kv_local
    halves = out_first.shape[1] // width_local
    hops = len(hops_of(tok_rows))
    units = tok_rows // SEG * kv_local
    n_sems = hops + 2 * len(pieces_of(tok_rows)) + 1 + 2 * halves
    n_sems += tok_rows // SEG + 1 + 3
    vmem = pl.BlockSpec(memory_space=pltpu.VMEM)
    hbm = pl.BlockSpec(memory_space=pl.ANY)
    bf16 = jnp.bfloat16
    f32 = jnp.float32
    return pl.pallas_call(
        functools.partial(kernel, n_sp),
        name="two_layers",
        out_shape=pltpu.VMEM((tok_rows, width_local), bf16),
        in_specs=[hbm] * 13,
        out_specs=vmem,
        scratch_shapes=[
            pltpu.VMEM(out_first.shape, bf16),
            pltpu.VMEM(query_w.shape, bf16),
            pltpu.VMEM((key_w.shape[0], 2 * kv_width), bf16),
            pltpu.VMEM(out_second.shape, bf16),
            pltpu.VMEM((SPAN + tok_rows, 2 * kv_width), bf16),
            pltpu.VMEM((SPAN + tok_rows, 2 * kv_width), bf16),
            pltpu.VMEM((SPAN + tok_rows, LANES), f32),
            pltpu.VMEM((tok_rows // SEG, BAND, LANES), f32),
            pltpu.VMEM((kv_local, BAND, group_width), f32),
            pltpu.VMEM((kv_local, BAND, group_width), f32),
            pltpu.VMEM((tok_rows, query_width), bf16),
            pltpu.VMEM((tok_rows, query_width), bf16),
            pltpu.VMEM((tok_rows, query_width), bf16),
            pltpu.VMEM((halves, tok_rows, width_local), bf16),
            pltpu.VMEM((halves, tok_rows, width_local), bf16),
            pltpu.VMEM((halves, tok_rows, width_local), bf16),
            pltpu.VMEM((halves, tok_rows, width_local), bf16),
            pltpu.VMEM((halves, tok_rows, width_local), f32),
            pltpu.VMEM((tok_rows, halves * width_local), bf16),
            pltpu.VMEM((tok_rows, LANES), f32),
            pltpu.VMEM((tok_rows, query_width), bf16),
            pltpu.VMEM(out_first.shape, bf16),
            pltpu.VMEM((tok_rows, query_width), bf16),
            pltpu.VMEM((out_second.shape[0], width_local), bf16),
            pltpu.VMEM((units, group_width, LANES), bf16),
            pltpu.VMEM((2, kv_width, pl.cdiv(SPAN + tok_rows, LANES) * LANES), bf16),
            pltpu.VMEM((units, BAND, group_width), f32),
            pltpu.VMEM((units, BAND, group_width), bf16),
            pltpu.VMEM((units, HEAD_SIZE, group_width), f32),
            pltpu.VMEM(bias_first.shape, f32),
            pltpu.VMEM(bias_second.shape, f32),
            pltpu.VMEM((1, norm_gain.shape[0]), f32),
            pltpu.VMEM((1, tok_rows), jnp.int32),
            pltpu.VMEM((hops, 1, tok_rows), jnp.int32),
            pltpu.VMEM((units, 2, group_width), f32),
            pltpu.SemaphoreType.DMA((n_sems,)),
            pltpu.SemaphoreType.DMA((n_sems,)),
            pltpu.SemaphoreType.DMA((13,)),
        ],
        compiler_params=pltpu.CompilerParams(collective_id=0, has_side_effects=True),
    )(
        residual,
        query_first,
        key_first,
        value_first,
        documents.reshape(1, tok_rows),
        bias_first,
        out_first,
        norm_gain.reshape(1, -1),
        query_w,
        key_w,
        value_w,
        bias_second,
        out_second,
    )


def solution(mesh):
    placed = (
        P("sp", "tp"),
        P("sp", "tp"),
        P("sp", "tp"),
        P("sp", "tp"),
        P("sp"),
        P("tp", None),
        P("tp", None),
        P(),
        P(None, "tp"),
        P(None, "tp"),
        P(None, "tp"),
        P("tp", None),
        P("tp", None),
    )
    return jax.shard_map(body, mesh=mesh, in_specs=placed, out_specs=P("sp", "tp"), check_vma=False)
```

```python
import functools

import jax
import jax.numpy as jnp
from jax import lax
from jax.experimental import pallas as pl
from jax.experimental.pallas import tpu as pltpu
from jax.sharding import PartitionSpec as P

HEAD_SIZE = 64
SEG = 64
PAST = 4
REL_CLIP = 256
SPAN = PAST * SEG
BAND = SPAN + SEG
LANES = 128
LOG2E = 1.4426950408889634
HIDDEN = -1e30
MESH = pl.DeviceIdType.MESH


eps = 1e-06


def hops_of(tok_rows):
    return range(1, (SPAN + tok_rows - 1) // tok_rows + 1)


def pieces_of(tok_rows):
    pieces = []
    for distance in hops_of(tok_rows):
        top = SPAN - (distance - 1) * tok_rows
        bottom = max(0, top - tok_rows)
        cuts = [cut for cut in range(SEG, tok_rows, SEG) if bottom < cut < top]
        edges = [bottom] + cuts + [top]
        for low, high in reversed(list(zip(edges[:-1], edges[1:]))):
            pieces.append((distance, tok_rows - (top - low), high - low, low))
    return pieces


def build_bias(table_ref, bias_ref):
    heads_local = table_ref.shape[0]
    group_size = bias_ref.shape[2] // SEG
    lane = lax.broadcasted_iota(jnp.int32, (SEG, LANES), 1)
    low = lane < SEG
    last = REL_CLIP + SPAN

    def tile(head, index):
        if index == 0:
            return jnp.broadcast_to(table_ref[head : head + 1, last : last + 1], (SEG, LANES))
        first = last - index * LANES
        return jnp.broadcast_to(table_ref[head : head + 1, first : first + LANES], (SEG, LANES))

    def piece(head, block, base):
        back = block // 2
        if block % 2 == 0:
            source = jnp.where(low, tile(head, back), tile(head, back + 1))
            shift = base
        else:
            source = tile(head, back + 1)
            shift = (base + SEG) % LANES
        return pltpu.roll(source, shift, 1, stride=1, stride_axis=0)

    for head in range(0, heads_local, 2):
        for block in range(PAST + 1):
            pair = jnp.where(low, piece(head, block, 0), piece(head + 1, block, SEG)) * LOG2E
            group, inner = head // group_size, head % group_size
            bias_ref[group, block * SEG : (block + 1) * SEG, inner * SEG : (inner + 2) * SEG] = pair


class Attention:
    def __init__(self, query, kv, bias, mask, mixed, padded, turned, scores, weights, stats, blend):
        self.query, self.kv, self.bias, self.mask, self.mixed = query, kv, bias, mask, mixed
        self.padded, self.turned, self.scores, self.weights = padded, turned, scores, weights
        self.stats, self.blend = stats, blend
        self.cut = SPAN
        self.groups = bias.shape[0]
        self.group_size = bias.shape[2] // SEG
        self.kv_width = self.groups * HEAD_SIZE
        self.state = {}

    def unit(self, segment, group):
        return segment * self.groups + group

    def pad_queries(self, segment):
        lane = lax.broadcasted_iota(jnp.int32, (SEG, LANES), 1)
        rows = slice(segment * SEG, (segment + 1) * SEG)
        for group in range(self.groups):
            keep = (lane >= group * HEAD_SIZE) & (lane < (group + 1) * HEAD_SIZE)
            for inner in range(self.group_size):
                head = group * self.group_size + inner
                column = head * HEAD_SIZE // LANES * LANES
                block = self.query[rows, column : column + LANES]
                if head % 2 != group % 2:
                    block = jnp.concatenate([block[:, HEAD_SIZE:], block[:, :HEAD_SIZE]], axis=1)
                self.padded[self.unit(segment, group), inner * SEG : (inner + 1) * SEG] = jnp.where(
                    keep, block, jnp.zeros_like(block)
                )

    def turn_values(self, row):
        block = jnp.transpose(self.kv[row : row + SEG, self.kv_width : 2 * self.kv_width])
        self.turned[0, :, row : row + SEG] = block
        if row >= SEG:
            self.turned[1, :, row - SEG : row] = block

    def bounds(self, segment, phase):
        first = segment * SEG
        cut = max(first, self.cut)
        return {
            "local": (max(first, SPAN), first + BAND),
            "halo": (first, SPAN),
            "near": (cut, SPAN),
            "rest": (first, cut),
        }[phase]

    def score(self, segment, group, phase):
        low, high = self.bounds(segment, phase)
        unit = self.unit(segment, group)
        band = slice(low - segment * SEG, high - segment * SEG)
        scores = lax.dot_general(
            self.kv[low:high, : self.kv_width],
            self.padded[unit],
            (((1,), (1,)), ((), ())),
            preferred_element_type=jnp.float32,
        )
        mask = self.mask[segment, band]
        mask = jnp.concatenate([mask] * (self.group_size * SEG // LANES), axis=1)
        scores = scores * (HEAD_SIZE ** (-0.5) * LOG2E) + self.bias[group, band] + mask
        self.scores[unit, band] = scores
        largest = jnp.max(scores, axis=0, keepdims=True)
        if phase != "local":
            largest = jnp.maximum(largest, self.stats[unit, 0:1])
        self.state[unit] = (largest,)

    def weigh(self, segment, group, phase):
        low, high = self.bounds(segment, phase)
        unit = self.unit(segment, group)
        band = slice(low - segment * SEG, high - segment * SEG)
        (largest,) = self.state[unit]
        weight = jnp.exp2(self.scores[unit, band] - largest)
        self.weights[unit, band] = weight.astype(jnp.bfloat16)
        total = jnp.sum(weight, axis=0, keepdims=True)
        fade = None
        if phase != "local":
            fade = jnp.exp2(self.stats[unit, 0:1] - largest)
            total = total + self.stats[unit, 1:2] * fade
        if self.ends(segment, phase):
            self.state[unit] = (fade, 1.0 / total)
        else:
            self.stats[unit, 0:1] = largest
            self.stats[unit, 1:2] = total
            self.state[unit] = (fade,)

    def ends(self, segment, phase):
        return phase != "local" and self.bounds(segment, phase)[0] == segment * SEG

    def gather(self, segment, group, phase):
        low, high = self.bounds(segment, phase)
        unit = self.unit(segment, group)
        band = slice(low - segment * SEG, high - segment * SEG)
        odd = low // SEG % 2
        blended = lax.dot_general(
            self.turned[
                odd,
                group * HEAD_SIZE : (group + 1) * HEAD_SIZE,
                low - odd * SEG : high - odd * SEG,
            ],
            self.weights[unit, band],
            (((1,), (0,)), ((), ())),
            preferred_element_type=jnp.float32,
        )
        if phase != "local":
            blended = blended + self.blend[unit] * self.state[unit][0]
        if not self.ends(segment, phase):
            self.blend[unit] = blended
            return
        blended = (blended * self.state[unit][1]).astype(jnp.bfloat16)
        rows = slice(segment * SEG, (segment + 1) * SEG)
        for pair in range(self.group_size // 2):
            turned = jnp.transpose(blended[:, pair * LANES : (pair + 1) * LANES])
            both = jnp.concatenate([turned[:SEG], turned[SEG:]], axis=1)
            column = (group * self.group_size + 2 * pair) * HEAD_SIZE
            self.mixed[rows, column : column + LANES] = both

    def steps(self, segments, phase, arrivals=()):
        units = [(segment, group) for segment in segments for group in range(self.groups)]
        waits = {segment: wait for segment, wait, _ in arrivals}
        turns = {segment: rows for segment, _, rows in arrivals}

        def score(unit):
            segment, group = unit
            if group == 0 and segment in waits:
                waits[segment]()
            self.score(segment, group, phase)
            if group == self.groups - 1 and segment in turns:
                for row in turns[segment]:
                    self.turn_values(row)

        def weigh(unit):
            self.weigh(*unit, phase)

        def gather(unit):
            self.gather(*unit, phase)

        plan = [(score, units[0])]
        for index, unit in enumerate(units):
            if index + 1 < len(units):
                plan.append((score, units[index + 1]))
            if index > 0:
                plan.append((gather, units[index - 1]))
            plan.append((weigh, unit))
        plan.append((gather, units[-1]))
        return [functools.partial(step, unit) for step, unit in plan]

    def run(self, segments, phase, arrivals=()):
        for step in self.steps(segments, phase, arrivals):
            step()


    def run_keys_first(self, segments, phase, values):
        units = [(segment, group) for segment in segments for group in range(self.groups)]
        for unit in units:
            self.score(*unit, phase)
        for unit in units[:2]:
            self.weigh(*unit, phase)
        values()
        for index, unit in enumerate(units):
            self.gather(*unit, phase)
            if index + 2 < len(units):
                self.weigh(*units[index + 2], phase)


def kernel(
    n_sp,
    residual_hbm,
    query_hbm,
    key_hbm,
    value_hbm,
    docs_hbm,
    bias_one_hbm,
    out_one_hbm,
    gain_hbm,
    query_w_hbm,
    key_w_hbm,
    value_w_hbm,
    bias_two_hbm,
    out_two_hbm,
    result_ref,
    w_out_one,
    w_query,
    w_kv,
    w_out_two,
    kv_one,
    kv_two,
    docs_col,
    mask,
    table_one,
    table_two,
    mixed,
    query_one,
    query_two,
    residual_full,
    part_own,
    part_in,
    layer,
    base,
    scaled,
    scales,
    mixed_in,
    w_other,
    last_mixed,
    w_last,
    padded,
    turned,
    scores,
    weights,
    blend,
    bias_one,
    bias_two,
    gain,
    docs,
    docs_prior,
    stats,
    send_sem,
    recv_sem,
    load_sem,
):
    me = lax.axis_index("sp")
    my_tp = lax.axis_index("tp")
    other = 1 - my_tp
    tok_rows, width_local = residual_hbm.shape
    kv_width = key_hbm.shape[1]
    segments = tok_rows // SEG
    hops = hops_of(tok_rows)
    pieces = pieces_of(tok_rows)
    halves = part_own.shape[0]
    blocks = [(range(segments - 1, 0, -1), SEG, tok_rows - SEG), (range(1), 0, SEG)]

    barrier = pltpu.get_barrier_semaphore()
    expected = jnp.int32(1)
    for distance in hops:
        expected = expected + (me + distance < n_sp).astype(jnp.int32)

        @pl.when(me >= distance)
        def _():
            pl.semaphore_signal(
                barrier, inc=1, device_id={"sp": me - distance}, device_id_type=MESH
            )

    pl.semaphore_signal(barrier, inc=1, device_id={"tp": other}, device_id_type=MESH)

    own = pl.ds(SPAN, tok_rows)
    transfers = dict(
        key=(key_hbm, kv_one.at[own, pl.ds(0, kv_width)]),
        value=(value_hbm, kv_one.at[own, pl.ds(kv_width, kv_width)]),
        docs=(docs_hbm, docs),
        bias_one=(bias_one_hbm, bias_one),
        query=(query_hbm, query_one),
        residual=(residual_hbm, residual_full.at[my_tp]),
        bias_two=(bias_two_hbm, bias_two),
        out_one=(out_one_hbm, w_out_one),
        gain=(gain_hbm, gain),
        key_w=(key_w_hbm, w_kv.at[:, pl.ds(0, kv_width)]),
        value_w=(value_w_hbm, w_kv.at[:, pl.ds(kv_width, kv_width)]),
        query_w=(query_w_hbm, w_query),
        out_two=(out_two_hbm, w_out_two),
    )
    loads = {
        name: pltpu.make_async_copy(src, dst, load_sem.at[index])
        for index, (name, (src, dst)) in enumerate(transfers.items())
    }
    for load in loads.values():
        load.start()

    slot = iter(range(send_sem.shape[0]))

    def remote(src, dst, target):
        index = next(slot)
        return pltpu.make_async_remote_copy(
            src_ref=src,
            dst_ref=dst,
            send_sem=send_sem.at[index],
            recv_sem=recv_sem.at[index],
            device_id=target,
            device_id_type=MESH,
        )

    def ahead(distance):
        return {"sp": lax.rem(me + distance, n_sp)}

    def start_sent(distance, copies):
        @pl.when(me + distance < n_sp)
        def _():
            for copy in copies:
                copy.start()

    def wait_arrived(distance, copies):
        @pl.when(me >= distance)
        def _():
            for copy in copies:
                copy.wait_recv()

    def wait_sent(distance, copies):
        @pl.when(me + distance < n_sp)
        def _():
            for copy in copies:
                copy.wait_send()

    for distance, _, needed, landing in pieces:

        @pl.when(me < distance)
        def _():
            empty = jnp.zeros((needed, 2 * kv_width), jnp.bfloat16)
            kv_one[landing : landing + needed] = empty
            kv_two[landing : landing + needed] = empty

    for distance in hops:

        @pl.when(me < distance)
        def _():
            docs_prior[distance - 1] = jnp.full((1, tok_rows), -1, jnp.int32)

    eye = lax.broadcasted_iota(jnp.int32, (SEG, SEG), 0) == lax.broadcasted_iota(
        jnp.int32, (SEG, SEG), 1
    )

    def put_column(numbers, place):
        picked = jnp.where(eye, numbers.astype(jnp.float32), 0.0)
        docs_col[place : place + SEG] = jnp.broadcast_to(
            jnp.sum(picked, axis=1, keepdims=True), (SEG, LANES)
        )

    def put_mask(segment, low, high):
        mine = docs[:, segment * SEG : (segment + 1) * SEG].astype(jnp.float32)
        mine = jnp.concatenate([mine, mine], axis=1)
        same = docs_col[low:high] == mine
        first = segment * SEG
        mask[segment, low - first : high - first] = jnp.where(same, 0.0, HIDDEN)

    shared = (mask, mixed, padded, turned, scores, weights, stats, blend)
    one = Attention(query_one, kv_one, table_one, *shared)
    two = Attention(query_two, kv_two, table_two, *shared)
    newest_first = range(segments - 1, -1, -1)
    two.cut = pieces[0][3]

    for name in ("key", "value", "docs"):
        loads[name].wait()
    pl.semaphore_wait(barrier, expected)

    def halo_copy(kv, piece, column=0, width=2 * kv_width):
        distance, row, needed, landing = piece
        columns = pl.ds(column, width)
        return remote(
            kv.at[pl.ds(SPAN + row, needed), columns],
            kv.at[pl.ds(landing, needed), columns],
            ahead(distance),
        )

    docs_copies = [
        (distance, [remote(docs, docs_prior.at[distance - 1], ahead(distance))])
        for distance in hops
    ]
    first_copies = [(piece[0], [halo_copy(kv_one, piece)]) for piece in pieces]
    for distance, copies in docs_copies + first_copies:
        start_sent(distance, copies)
    loads["residual"].wait()
    residual_copy = remote(residual_full.at[my_tp], residual_full.at[my_tp], {"tp": other})
    residual_copy.start()

    loads["query"].wait()
    for row in range(SPAN, SPAN + tok_rows, SEG):
        one.turn_values(row)
    for segment in newest_first:
        one.pad_queries(segment)
    for block in range(0, tok_rows, SEG):
        put_column(docs[:, block : block + SEG], SPAN + block)
    for segment in range(segments):
        put_mask(segment, *one.bounds(segment, "local"))

    loads["bias_one"].wait()
    build_bias(bias_one, table_one)
    loads["out_one"].wait()
    weight_copy = remote(w_out_one, w_other, {"tp": other})

    @pl.when(my_tp == 0)
    def _():
        weight_copy.start()

    loads["out_two"].wait()
    theirs = pl.ds(pl.multiple_of(other * width_local, width_local), width_local)
    ours = pl.ds(pl.multiple_of(my_tp * width_local, width_local), width_local)
    last_weight = remote(w_out_two.at[:, theirs], w_last, {"tp": other})
    last_weight.start()
    one.run(newest_first, "local")

    for distance, copies in docs_copies:
        wait_arrived(distance, copies)
    for distance, row, needed, landing in pieces:
        for block in range(0, needed, SEG):
            put_column(
                docs_prior[distance - 1, :, row + block : row + block + SEG], landing + block
            )
    for segment in range(segments):
        put_mask(segment, *one.bounds(segment, "halo"))
    residual_copy.wait_recv()

    def arrival(segment, waiting, which):
        members = list(zip(pieces, waiting))[which]

        def wait():
            for _, (distance, copies) in members:
                wait_arrived(distance, copies)

        rows = [
            row
            for (_, _, needed, landing), _ in members
            for row in range(landing, landing + needed, SEG)
        ]
        return segment, wait, rows

    newest, older = newest_first[0], newest_first[1]

    part_copies = []
    for _, start, count in blocks:
        rows = pl.ds(start, count)
        part_copies.append(
            [
                remote(part_own.at[half, rows], part_in.at[half, rows], {"tp": other})
                for half in range(halves)
            ]
        )

    mixed_copies = []
    for members, _, _ in blocks:
        mixed_copies.append([])
        for segment in members:
            rows = pl.ds(segment * SEG, SEG)
            mixed_copies[-1].append(remote(mixed.at[rows], mixed_in.at[rows], {"tp": other}))

    def start_mixed(block):
        @pl.when(my_tp == 0)
        def _():
            for copy in mixed_copies[block]:
                copy.start()

    def project(source, weight, rows):
        return [
            jnp.dot(
                source[rows],
                weight[:, half * width_local : (half + 1) * width_local],
                preferred_element_type=jnp.float32,
            ).astype(jnp.bfloat16)
            for half in range(halves)
        ]

    def project_one(block):
        _, start, count = blocks[block]
        rows = slice(start, start + count)
        parts = project(mixed, w_out_one, rows)
        for half, part in enumerate(parts):
            part_own[half, rows] = part

        @pl.when(my_tp == 1)
        def _():
            for copy in part_copies[block]:
                copy.start()

        for half, part in enumerate(parts):
            base[half, rows] = residual_full[half, rows].astype(jnp.float32) + part.astype(
                jnp.float32
            )

    second_copies = [
        (piece[0], [halo_copy(kv_two, piece, part * kv_width, kv_width) for part in range(2)])
        for piece in pieces
    ]

    def keys_two(block, core):
        _, start, count = blocks[block]
        rows = slice(start, start + count)
        squares = jnp.zeros((count, LANES), jnp.float32)
        if core == 0:
            for copy in part_copies[block]:
                copy.wait_recv()
            parts = [part_in[half, rows] for half in range(halves)]
        else:
            if block == 0:
                weight_copy.wait_recv()
            for copy in mixed_copies[block]:
                copy.wait_recv()
            parts = project(mixed_in, w_other, rows)
        for half in range(halves):
            new = base[half, rows] + parts[half].astype(jnp.float32)
            new = new.astype(jnp.bfloat16)
            layer[half, rows] = new
            new = new.astype(jnp.float32)
            columns = slice(half * width_local, (half + 1) * width_local)
            scaled[rows, columns] = (new * gain[:, columns]).astype(jnp.bfloat16)
            for lane in range(0, width_local, LANES):
                squares = squares + new[:, lane : lane + LANES] * new[:, lane : lane + LANES]
        scale = lax.rsqrt(
            jnp.sum(squares, axis=1, keepdims=True) / (halves * width_local) + eps
        )
        scales[rows] = jnp.broadcast_to(scale, (count, LANES))
        kv_two[SPAN + start : SPAN + start + count] = (
            jnp.dot(scaled[rows], w_kv[...], preferred_element_type=jnp.float32) * scale
        ).astype(jnp.bfloat16)
        for piece, copies in reversed(list(zip(pieces, second_copies))):
            late = core == 1 and piece[0] != pieces[0][0]
            if block == 1 if late else start <= piece[1] < start + count:
                start_sent(*copies)

    for name in ("gain", "key_w", "value_w", "query_w"):
        loads[name].wait()
    for step in one.steps(
        newest_first[:-1],
        "halo",
        (
            arrival(newest, first_copies, slice(0, 1)),
            arrival(older, first_copies, slice(1, 2)),
        ),
    ):
        step()
    start_mixed(0)
    project_one(0)
    plan = one.steps(
        newest_first[-1:], "halo", (arrival(newest_first[-1], first_copies, slice(2, None)),)
    )

    @pl.when(my_tp == 0)
    def _():
        keys_two(0, 0)

    for step in plan:
        step()
    start_mixed(1)
    project_one(1)
    loads["bias_two"].wait()

    @pl.when(my_tp == 1)
    def _():
        build_bias(bias_two, table_two)
        keys_two(0, 1)
        keys_two(1, 1)

    @pl.when(my_tp == 0)
    def _():
        keys_two(1, 0)

    query_two[...] = (
        jnp.dot(scaled[...], w_query[...], preferred_element_type=jnp.float32) * scales[:, 0:1]
    ).astype(jnp.bfloat16)

    @pl.when(my_tp == 0)
    def _():
        build_bias(bias_two, table_two)

    for row in range(SPAN, SPAN + tok_rows, SEG):
        two.turn_values(row)
    for segment in newest_first:
        two.pad_queries(segment)
    two.run(newest_first, "local")

    @pl.when(my_tp == 1)
    def _():
        for copies in part_copies:
            for copy in copies:
                copy.wait_send()

    @pl.when(my_tp == 0)
    def _():
        weight_copy.wait_send()
        for copies in mixed_copies:
            for copy in copies:
                copy.wait_send()


    finished = (pl.ds(two.cut, tok_rows - two.cut), pl.ds(0, two.cut))
    mixed_last = [
        remote(mixed.at[rows], last_mixed.at[rows], {"tp": other}) for rows in finished
    ]
    def attend_two(members, phase, which):
        landed = list(zip(pieces, second_copies))[which]
        for _, (distance, copies) in landed:
            wait_arrived(distance, copies[:1])

        def values():
            for _, (distance, copies) in landed:
                wait_arrived(distance, copies[1:])
            for (_, _, needed, landing), _ in landed:
                for row in range(landing, landing + needed, SEG):
                    two.turn_values(row)

        two.run_keys_first(members, phase, values)

    attend_two(newest_first, "near", slice(0, 1))
    mixed_last[0].start()
    older_two = [segment for segment in newest_first if segment * SEG < two.cut]
    attend_two(older_two, "rest", slice(1, None))
    mixed_last[1].start()
    branch = jnp.dot(mixed[...], w_out_two[:, ours], preferred_element_type=jnp.float32).astype(
        jnp.bfloat16
    )
    base[0] = layer[my_tp].astype(jnp.float32) + branch.astype(jnp.float32)
    last_weight.wait_recv()
    for copy in mixed_last:
        copy.wait_recv()
    branch = jnp.dot(last_mixed[...], w_last[...], preferred_element_type=jnp.float32).astype(
        jnp.bfloat16
    )
    result_ref[...] = (base[0] + branch.astype(jnp.float32)).astype(jnp.bfloat16)

    last_weight.wait_send()
    for copy in mixed_last:
        copy.wait_send()
    residual_copy.wait_send()
    for distance, copies in docs_copies + first_copies + second_copies:
        wait_sent(distance, copies)


def body(
    residual,
    query_first,
    key_first,
    value_first,
    documents,
    bias_first,
    out_first,
    norm_gain,
    query_w,
    key_w,
    value_w,
    bias_second,
    out_second,
):
    n_sp = lax.axis_size("sp")
    tok_rows, width_local = residual.shape
    query_width = query_first.shape[1]
    kv_width = key_first.shape[1]
    kv_local = kv_width // HEAD_SIZE
    group_width = query_width // kv_local
    halves = out_first.shape[1] // width_local
    hops = len(hops_of(tok_rows))
    units = tok_rows // SEG * kv_local
    n_sems = hops + 3 * len(pieces_of(tok_rows)) + 1 + 2 * halves
    n_sems += tok_rows // SEG + 1 + 3
    vmem = pl.BlockSpec(memory_space=pltpu.VMEM)
    hbm = pl.BlockSpec(memory_space=pl.ANY)
    bf16 = jnp.bfloat16
    f32 = jnp.float32
    return pl.pallas_call(
        functools.partial(kernel, n_sp),
        name="two_layers",
        out_shape=pltpu.VMEM((tok_rows, width_local), bf16),
        in_specs=[hbm] * 13,
        out_specs=vmem,
        scratch_shapes=[
            pltpu.VMEM(out_first.shape, bf16),
            pltpu.VMEM(query_w.shape, bf16),
            pltpu.VMEM((key_w.shape[0], 2 * kv_width), bf16),
            pltpu.VMEM(out_second.shape, bf16),
            pltpu.VMEM((SPAN + tok_rows, 2 * kv_width), bf16),
            pltpu.VMEM((SPAN + tok_rows, 2 * kv_width), bf16),
            pltpu.VMEM((SPAN + tok_rows, LANES), f32),
            pltpu.VMEM((tok_rows // SEG, BAND, LANES), f32),
            pltpu.VMEM((kv_local, BAND, group_width), f32),
            pltpu.VMEM((kv_local, BAND, group_width), f32),
            pltpu.VMEM((tok_rows, query_width), bf16),
            pltpu.VMEM((tok_rows, query_width), bf16),
            pltpu.VMEM((tok_rows, query_width), bf16),
            pltpu.VMEM((halves, tok_rows, width_local), bf16),
            pltpu.VMEM((halves, tok_rows, width_local), bf16),
            pltpu.VMEM((halves, tok_rows, width_local), bf16),
            pltpu.VMEM((halves, tok_rows, width_local), bf16),
            pltpu.VMEM((halves, tok_rows, width_local), f32),
            pltpu.VMEM((tok_rows, halves * width_local), bf16),
            pltpu.VMEM((tok_rows, LANES), f32),
            pltpu.VMEM((tok_rows, query_width), bf16),
            pltpu.VMEM(out_first.shape, bf16),
            pltpu.VMEM((tok_rows, query_width), bf16),
            pltpu.VMEM((out_second.shape[0], width_local), bf16),
            pltpu.VMEM((units, group_width, LANES), bf16),
            pltpu.VMEM((2, kv_width, pl.cdiv(SPAN + tok_rows, LANES) * LANES), bf16),
            pltpu.VMEM((units, BAND, group_width), f32),
            pltpu.VMEM((units, BAND, group_width), bf16),
            pltpu.VMEM((units, HEAD_SIZE, group_width), f32),
            pltpu.VMEM(bias_first.shape, f32),
            pltpu.VMEM(bias_second.shape, f32),
            pltpu.VMEM((1, norm_gain.shape[0]), f32),
            pltpu.VMEM((1, tok_rows), jnp.int32),
            pltpu.VMEM((hops, 1, tok_rows), jnp.int32),
            pltpu.VMEM((units, 2, group_width), f32),
            pltpu.SemaphoreType.DMA((n_sems,)),
            pltpu.SemaphoreType.DMA((n_sems,)),
            pltpu.SemaphoreType.DMA((13,)),
        ],
        compiler_params=pltpu.CompilerParams(collective_id=0, has_side_effects=True),
    )(
        residual,
        query_first,
        key_first,
        value_first,
        documents.reshape(1, tok_rows),
        bias_first,
        out_first,
        norm_gain.reshape(1, -1),
        query_w,
        key_w,
        value_w,
        bias_second,
        out_second,
    )


def solution(mesh):
    placed = (
        P("sp", "tp"),
        P("sp", "tp"),
        P("sp", "tp"),
        P("sp", "tp"),
        P("sp"),
        P("tp", None),
        P("tp", None),
        P(),
        P(None, "tp"),
        P(None, "tp"),
        P(None, "tp"),
        P("tp", None),
        P("tp", None),
    )
    return jax.shard_map(body, mesh=mesh, in_specs=placed, out_specs=P("sp", "tp"), check_vma=False)
```
